256 devices in a mesh: ep: 16 (over y, x), tp: 16 (over z, core).
Axes of the slice: x: 4, y: 4, z: 8, core: 2. Of those that a mesh axis runs over, the one named last changes fastest.
Arguments:
- tokens: bfloat16 [1024, 2048], P('ep'), may hold values from -7 to 7
- state: float32 [1024, 32, 64, 64], P('ep', 'tp'), may hold values from -6 to 6
- routes: int32 [1024, 2], P('ep'), may hold values from 0 to 15, all different within a row; in each aligned block of 64 rows (0 to 63, 64 to 127, ...) at most 12 rows name the same one
- route_logits: float32 [1024, 2], P('ep'), may hold values from -4 to 4
- mix_gain: float32 [2048], replicated, may hold values from 0.1 to 1.9
- w_recept: bfloat16 [2048, 2048], P(None, 'tp')
- w_key: bfloat16 [2048, 2048], P(None, 'tp'), may hold values from -0.125 to 0.125
- w_value: bfloat16 [2048, 2048], P(None, 'tp'), may hold values from -0.125 to 0.125
- w_decay: bfloat16 [2048, 2048], P(None, 'tp'), may hold values from -0.125 to 0.125
- w_rate: bfloat16 [2048, 2048], P(None, 'tp'), may hold values from -0.125 to 0.125
- decay_base: float32 [2048], P('tp'), may hold values from -3 to 1
- rate_base: float32 [2048], P('tp'), may hold values from -3 to 3
- key_gain: float32 [2048], P('tp'), may hold values from 0.1 to 1.9
- group_gain: float32 [2048], P('tp'), may hold values from 0.1 to 1.9
- w_output: bfloat16 [2048, 2048], P('tp'), may hold values from -0.125 to 0.125
- ffn_gain: float32 [2048], replicated, may hold values from 0.1 to 1.9
- w_gate: bfloat16 [16, 2048, 7168], P('ep', None, 'tp'), may hold values from -0.125 to 0.125
- w_up: bfloat16 [16, 2048, 7168], P('ep', None, 'tp'), may hold values from -0.125 to 0.125
- w_down: bfloat16 [16, 7168, 2048], P('ep', 'tp'), may hold values from -0.0625 to 0.0625
Outputs:
- output: bfloat16 [1024, 2048], P('ep', 'tp')
- new_state: float32 [1024, 32, 64, 64], P('ep', 'tp')
The draws below stay inside these ranges and needn't reach their ends.
Inputs may be any that keep to these rules, and one draw needn't show every extreme that they name: `routes`: for each expert, the 64 tokens of one device group's rows name it in at most 12 of their rows; the 2 experts of a row differ.
All inputs are finite; a program needn't handle non-finite values.
Results may differ from the reference program's by a relative error of at most 0.0091.
Values may be sent and summed in bfloat16 or wider, within the bound.
No kernel may reach another device: no remote copies, remote signals or barrier semaphores. Data moves between devices by JAX's collectives and lax.ppermute only.
A program may use at most 64 MiB of HBM per device.

```python
import math
from functools import partial
import jax
import jax.numpy as jnp
import numpy as np
from jax import lax

D = 2048
HEADS = 32
HEAD = 64
FF = 7168
TOPK = 2
SEQ_DEV = 64
SEQS = 1024
EXPERTS = 16
CAP = 12
N_EP = 16


def draw_tokens(key, part):
    noise_key = jax.random.fold_in(key, 11)
    columns = jnp.exp(jnp.linspace(jnp.log(0.25), 0.0, D)).astype(jnp.float32)
    values = jnp.clip(jax.random.normal(noise_key, (SEQS, D), jnp.float32), -5.0, 5.0) * columns[None, :]
    return values.astype(jnp.bfloat16)


def draw_w_recept(key, part):
    entry_key = jax.random.fold_in(key, 21)
    scale_key = jax.random.fold_in(key, 22)
    head_scale = jnp.exp(jax.random.uniform(scale_key, (HEADS,), jnp.float32, jnp.log(0.001), jnp.log(0.01)))
    column_scale = jnp.repeat(head_scale, HEAD) * jnp.sqrt(64.0 / HEAD) / jnp.sqrt(1.0 * D)
    entries = jnp.clip(jax.random.normal(entry_key, (D, D), jnp.float32), -4.0, 4.0)
    values = entries * column_scale[None, :]
    return values.astype(jnp.bfloat16)


def steps_of(stream_key, extent, split, smallest, high):
    def one(position, blocks):
        heights = jax.random.uniform(jax.random.fold_in(jax.random.fold_in(stream_key, 6), position), (blocks,), jnp.float32, smallest / len(split), high / len(split))
        return jnp.repeat(jnp.exp(heights), extent[position] // blocks).reshape((-1,) + (1,) * (len(extent) - position - 1))

    gain = one(*split[0])
    for cut in split[1:]:
        gain = gain * one(*cut)
    return gain


def deal_out(own_key, own, number, rows, amount, top, bound, lean):
    ranking = jax.random.permutation(own_key, amount)
    crowded, usual = shares(amount, rows * top, bound, lean, True), shares(amount, rows * top, bound, lean, False)
    places = jnp.arange(amount)

    def named(sizes, rotation):
        used = int((sizes > 0).sum())
        fixed = max(1, used // 4)
        moved = fixed + (places - fixed + rotation * (used - fixed)) % max(1, amount - fixed)
        return jnp.zeros((amount,), jnp.int32).at[ranking[jnp.where(places < fixed, places, moved)]].set(jnp.asarray(sizes, jnp.int32))

    sizes = jnp.where(number % 4 == 0, named(crowded, number // 4), named(usual, number - number // 4 - 1))
    mixed = jax.random.permutation(jax.random.fold_in(own, 3), amount)
    source_of, taker = mixed[0:amount // 2 * 2:2], mixed[1:amount // 2 * 2:2]
    room = jnp.minimum(sizes[source_of] - 1, bound - sizes[taker]) // 2
    room = jnp.where((source_of == ranking[0]) | (taker == ranking[0]) | (sizes[taker] == 0), 0, jnp.maximum(room, 0))
    moved = jax.random.randint(jax.random.fold_in(own, 4), (amount // 2,), 0, 1 << 20) % (room + 1)
    sizes = sizes.at[source_of].add(-moved).at[taker].add(moved)
    labels = jnp.searchsorted(jnp.cumsum(sizes), jnp.arange(rows * top), side="right").astype(jnp.int32)
    table = labels.reshape(top, rows).T
    table = table[jax.random.permutation(jax.random.fold_in(own, 1), rows)]
    rotation = jax.random.randint(jax.random.fold_in(own, 2), (rows, 1), 0, top)
    return jnp.take_along_axis(table, (jnp.arange(top)[None, :] + rotation) % top, axis=1)


def shares(amount, total, bound, lean, full):
    portions = [(1 << 20) // math.isqrt(rank ** lean) + 1 for rank in range(1, amount + 1)]
    largest = bound if full else min(bound, max(-(-total // amount), total * portions[0] // sum(portions)))
    least = 1 if total - largest >= amount - 1 else 0
    given, rest = [largest] + [least] * (amount - 1), total - largest - least * (amount - 1)
    while rest > 0:
        movable = [i for i in range(1, amount) if given[i] < largest] or [i for i in range(1, amount) if given[i] < bound]
        pool, budget = sum([portions[i] for i in movable]), rest
        for i in movable:
            more = min(bound - given[i], max(1, budget * portions[i] // pool), rest)
            given[i] = given[i] + more
            rest = rest - more
    return np.array(given)


def noise(key, dims, width, limit, cuts=(), kind=jnp.bfloat16):
    drawn = width * jax.random.normal(key, dims, jnp.float32)
    if cuts:
        drawn = drawn * steps_of(key, dims, cuts, -0.22, 0.18)
    return jnp.clip(drawn, -limit, limit).astype(kind)


def setup_inputs(seed: int = 0) -> dict:
    key_of = jax.random.split(jax.random.key(seed), 20)
    tokens = draw_tokens(jax.random.fold_in(key_of[19], 71), 0)
    state = noise(key_of[1], (SEQS, HEADS, HEAD, HEAD), 1.0, 6.0, ((0, 16), (1, 16)), jnp.float32)
    routes_keys = jax.random.split(jax.random.fold_in(key_of[2], 1), SEQS // SEQ_DEV)
    routes_turns = jax.random.permutation(jax.random.fold_in(key_of[2], 3), SEQS // SEQ_DEV)
    routes = jax.vmap(lambda own, number: deal_out(jax.random.fold_in(key_of[2], 2), own, number, SEQ_DEV, EXPERTS, TOPK, CAP, 2))(routes_keys, routes_turns).reshape((SEQS, TOPK))
    route_logits = noise(key_of[3], (SEQS, TOPK), 1.5, 4.0, ((0, 16),), jnp.float32)
    mix_gain = jnp.clip(1.0 + 0.18 * jax.random.normal(key_of[4], (D,), jnp.float32), 0.1, 1.9)
    w_recept = draw_w_recept(jax.random.fold_in(key_of[19], 71), 0)
    w_key = noise(key_of[6], (D, D), D ** -0.5, 0.125, ((1, 16),))
    w_value = noise(key_of[7], (D, D), D ** -0.5, 0.125, ((1, 16),))
    w_decay = noise(key_of[8], (D, D), D ** -0.5, 0.125, ((1, 16),))
    w_rate = noise(key_of[9], (D, D), D ** -0.5, 0.125, ((1, 16),))
    decay_base = jnp.clip(-3.0 + 4.0 * jax.random.uniform(key_of[10], (D,), jnp.float32) ** steps_of(key_of[10], (D,), ((0, 16),), -0.2, 0.2), -3.0, 1.0)
    rate_base = noise(key_of[11], (D,), 1.0, 3.0, ((0, 16),), jnp.float32)
    key_gain = jnp.clip(1.0 + 0.18 * jax.random.normal(key_of[12], (D,), jnp.float32), 0.1, 1.9)
    group_gain = jnp.clip(1.0 + 0.18 * jax.random.normal(key_of[13], (D,), jnp.float32), 0.1, 1.9)
    w_output = noise(key_of[14], (D, D), D ** -0.5, 0.125, ((0, 16),))
    ffn_gain = jnp.clip(1.0 + 0.18 * jax.random.normal(key_of[15], (D,), jnp.float32), 0.1, 1.9)
    w_gate = noise(key_of[16], (EXPERTS, D, FF), D ** -0.5, 0.125, ((0, 16), (2, 16)))
    w_up = noise(key_of[17], (EXPERTS, D, FF), D ** -0.5, 0.125, ((0, 16), (2, 16)))
    w_down = noise(key_of[18], (EXPERTS, FF, D), FF ** -0.5, 0.0625, ((0, 16), (1, 16)))
    return {"tokens": tokens, "state": state, "routes": routes, "route_logits": route_logits, "mix_gain": mix_gain, "w_recept": w_recept, "w_key": w_key, "w_value": w_value, "w_decay": w_decay, "w_rate": w_rate, "decay_base": decay_base, "rate_base": rate_base, "key_gain": key_gain, "group_gain": group_gain, "w_output": w_output, "ffn_gain": ffn_gain, "w_gate": w_gate, "w_up": w_up, "w_down": w_down}


RMS_EPS = 1e-06
GROUP_EPS = 0.00064
UNIT_EPS = 6.4e-05
HIGHEST = lax.Precision.HIGHEST

def rounded(values):
    return lax.optimization_barrier(values.astype(jnp.bfloat16)).astype(jnp.float32)

def mix_heads(normed, state, w_recept, w_key, w_value, w_decay, w_rate, decay_base, rate_base, key_gain, group_gain):
    seq_rows = state.shape[0]
    head_count = state.shape[1]

    def project(weight):
        return rounded(jnp.dot(normed, weight, preferred_element_type=jnp.float32))

    def split_heads(values):
        return values.reshape(seq_rows, head_count, -1)
    recept = split_heads(project(w_recept))
    keys_now = split_heads(project(w_key))
    values_now = split_heads(project(w_value))
    decay_pre = project(w_decay) + decay_base
    decay_now = split_heads(jnp.exp(-jnp.exp(-jax.nn.softplus(-decay_pre) - 0.5)))
    rate_now = split_heads(jax.nn.sigmoid(project(w_rate) + rate_base))
    scaled = keys_now * key_gain.reshape(head_count, -1)[None]
    unit_key = scaled * lax.rsqrt(lax.optimization_barrier(jnp.sum(scaled * scaled, axis=2, keepdims=True)) + UNIT_EPS)
    removed = jnp.einsum('bhvk,bhk->bhv', state, unit_key, precision=HIGHEST)
    new_state = state * decay_now[:, :, None, :] - removed[:, :, :, None] * (unit_key * rate_now)[:, :, None, :] + values_now[:, :, :, None] * keys_now[:, :, None, :]
    readout = jnp.einsum('bhvk,bhk->bhv', new_state, recept, precision=HIGHEST)
    centred = readout - lax.optimization_barrier(jnp.mean(readout, axis=2, keepdims=True))
    spread = lax.optimization_barrier(jnp.mean(centred * centred, axis=2, keepdims=True))
    normed_read = centred * lax.rsqrt(spread + GROUP_EPS) * group_gain.reshape(head_count, -1)[None]
    return (normed_read.reshape(seq_rows, -1).astype(jnp.bfloat16), new_state)

def slot_numbers(route_rows, expert_count, capacity):
    flat_routes = route_rows.reshape(-1)
    one_hot = (flat_routes[:, None] == jnp.arange(expert_count, dtype=jnp.int32)[None, :]).astype(jnp.int32)
    earlier = jnp.cumsum(one_hot, axis=0) - one_hot
    placed = lax.optimization_barrier(jnp.sum(earlier * one_hot, axis=1)).astype(jnp.int32)
    return (flat_routes * capacity + placed).reshape(route_rows.shape)

def expert_rows(slot_rows, gate_weight, up_weight, down_weight):
    gate_act = jnp.dot(slot_rows, gate_weight, preferred_element_type=jnp.float32)
    upward = jnp.dot(slot_rows, up_weight, preferred_element_type=jnp.float32)
    hidden = (jax.nn.silu(gate_act) * upward).astype(jnp.bfloat16)
    return jnp.dot(hidden, down_weight, preferred_element_type=jnp.float32)

def reference(tokens, state, routes, route_logits, mix_gain, w_recept, w_key, w_value, w_decay, w_rate, decay_base, rate_base, key_gain, group_gain, w_output, ffn_gain, w_gate, w_up, w_down):
    values = tokens.astype(jnp.float32)
    normed = (values * lax.rsqrt(lax.optimization_barrier(jnp.mean(values * values, axis=1, keepdims=True)) + RMS_EPS) * mix_gain).astype(jnp.bfloat16)
    mixed_rows, new_state = mix_heads(normed, state, w_recept, w_key, w_value, w_decay, w_rate, decay_base, rate_base, key_gain, group_gain)
    residual = (values + jnp.dot(mixed_rows, w_output, preferred_element_type=jnp.float32)).astype(jnp.bfloat16)
    resid_vals = residual.astype(jnp.float32)
    ffn_in = (resid_vals * lax.rsqrt(lax.optimization_barrier(jnp.mean(resid_vals * resid_vals, axis=1, keepdims=True)) + RMS_EPS) * ffn_gain).astype(jnp.bfloat16)
    route_exp = jnp.exp(route_logits)
    route_weight = route_exp / lax.optimization_barrier(jnp.sum(route_exp, axis=1, keepdims=True))
    group_routes = routes.reshape(N_EP, SEQ_DEV, TOPK)
    slot_ids = jax.vmap(partial(slot_numbers, expert_count=EXPERTS, capacity=CAP))(group_routes)
    group_index = jnp.arange(N_EP, dtype=jnp.int32)
    local_token = jnp.broadcast_to(jnp.arange(SEQ_DEV, dtype=jnp.int32)[None, :, None], slot_ids.shape)
    global_token = local_token + (group_index * SEQ_DEV)[:, None, None]
    slot_flat = (slot_ids + (group_index * (EXPERTS * CAP))[:, None, None]).reshape(-1)
    owners_table = jnp.full((N_EP * EXPERTS * CAP,), SEQS, jnp.int32).at[slot_flat].set(global_token.reshape(-1))
    owners_table = owners_table.reshape(N_EP, EXPERTS, CAP).transpose(1, 0, 2).reshape(EXPERTS, N_EP * CAP)
    padded_in = jnp.concatenate([ffn_in, jnp.zeros((1, D), ffn_in.dtype)], axis=0)

    def one_expert(inputs):
        owners, gate_weight, up_weight, down_weight = inputs
        return expert_rows(padded_in[owners], gate_weight, up_weight, down_weight)
    outputs = lax.map(one_expert, (owners_table, w_gate, w_up, w_down)).reshape(EXPERTS, N_EP, CAP, D)
    place_in = (slot_ids - group_routes * CAP).astype(jnp.int32)
    picked = outputs[group_routes, group_index[:, None, None], place_in]
    moe_sum = lax.optimization_barrier(jnp.sum(picked * route_weight.reshape(N_EP, SEQ_DEV, TOPK)[..., None], axis=2)).reshape(SEQS, D)
    output = (resid_vals + moe_sum).astype(jnp.bfloat16)
    return (output, new_state)
```

```python
import jax
import jax.numpy as jnp
from jax import lax
from jax.experimental import pallas as pl
from jax.experimental.pallas import tpu as pltpu
from jax.sharding import Mesh
from jax.sharding import PartitionSpec as P

TP = ("tp_0", "tp_1")

RMS_EPS = 1e-06
GROUP_EPS = 0.00064
UNIT_EPS = 6.4e-05
HIGHEST = lax.Precision.HIGHEST
F32 = jnp.float32
BF16 = jnp.bfloat16
VMEM = pltpu.VMEM
HEAD = 64
LANES = 128


def head_sums(values):
    rows = lax.broadcasted_iota(jnp.int32, (LANES, LANES), 0) // HEAD
    cols = lax.broadcasted_iota(jnp.int32, (LANES, LANES), 1) // HEAD
    ones = (rows == cols).astype(F32)
    return jnp.dot(values, ones, precision=HIGHEST, preferred_element_type=F32)


def mix_kernel(
    core_ref,
    tokens_hbm,
    state_hbm,
    w_recept_hbm,
    w_key_hbm,
    w_value_hbm,
    w_decay_hbm,
    w_rate_hbm,
    w_output_hbm,
    mix_gain_ref,
    decay_base_ref,
    rate_base_ref,
    key_gain_ref,
    group_gain_ref,
    keep_ref,
    send_ref,
    removed_ref,
    unit_rate_ref,
    decay_ref,
    key_ref,
    value_ref,
    tokens_ref,
    weights_ref,
    w_output_ref,
    state_ref,
    vectors_ref,
    products_ref,
    sems,
):
    seqs = tokens_ref.shape[0]
    chunks = state_ref.shape[0]
    chunk_rows = state_ref.shape[1]
    copies = [pltpu.make_async_copy(tokens_hbm, tokens_ref, sems.at[0])]
    sources = (w_key_hbm, w_value_hbm, w_recept_hbm, w_decay_hbm, w_rate_hbm)
    for place, source in enumerate(sources):
        target = weights_ref.at[:, pl.ds(place * LANES, LANES)]
        copies.append(pltpu.make_async_copy(source, target, sems.at[1 + place]))
    for chunk in range(chunks):
        source = state_hbm.at[pl.ds(chunk * chunk_rows, chunk_rows)]
        copies.append(pltpu.make_async_copy(source, state_ref.at[chunk], sems.at[6 + chunk]))
    copies.append(pltpu.make_async_copy(w_output_hbm, w_output_ref, sems.at[6 + chunks]))
    for copy in copies:
        copy.start()

    copies[0].wait()
    values = tokens_ref[...].astype(F32)
    mean_square = jnp.mean(values * values, axis=1, keepdims=True)
    normed = (values * lax.rsqrt(mean_square + RMS_EPS) * mix_gain_ref[...]).astype(BF16)

    def project(first, count):
        for place in range(first, first + count):
            copies[1 + place].wait()
        weight = weights_ref[:, first * LANES : (first + count) * LANES]
        return jnp.dot(normed, weight, preferred_element_type=F32).astype(BF16).astype(F32)

    key_value = project(0, 2)
    keys_now = key_value[:, :LANES]
    values_now = key_value[:, LANES:]
    recept_decay = project(2, 2)
    recept = recept_decay[:, :LANES]
    decay_pre = recept_decay[:, LANES:] + decay_base_ref[...]
    rate_pre = project(4, 1) + rate_base_ref[...]
    decay_now = jnp.exp(-jnp.exp(-jax.nn.softplus(-decay_pre) - 0.5))
    rate_now = jax.nn.sigmoid(rate_pre)
    scaled = keys_now * key_gain_ref[...]
    unit_key = scaled * lax.rsqrt(head_sums(scaled * scaled) + UNIT_EPS)
    unit_rate = unit_key * rate_now
    decayed_recept = decay_now * recept
    unit_rate_ref[...] = unit_rate
    decay_ref[...] = decay_now
    key_ref[...] = keys_now
    value_ref[...] = values_now

    vectors_ref[...] = jnp.zeros_like(vectors_ref)
    vectors_ref[pl.ds(0, seqs, stride=8), :] = unit_key
    vectors_ref[pl.ds(1, seqs, stride=8), :] = decayed_recept
    vectors_ref[pl.ds(2, seqs, stride=8), :] = pltpu.roll(unit_key, HEAD, 1)
    vectors_ref[pl.ds(3, seqs, stride=8), :] = pltpu.roll(decayed_recept, HEAD, 1)
    per_chunk = chunk_rows // LANES
    for chunk in range(chunks):
        copies[6 + chunk].wait()
        for inner in range(per_chunk):
            seq = chunk * per_chunk + inner
            left = vectors_ref[seq * 8 : seq * 8 + 8, :HEAD].astype(BF16)
            right = state_ref[chunk, inner * LANES : (inner + 1) * LANES, :].astype(BF16)
            products_ref[seq * 8 : seq * 8 + 8, :] = lax.dot_general(
                left, right, (((1,), (1,)), ((), ())), preferred_element_type=F32
            )
    first_head = lax.broadcasted_iota(jnp.int32, (seqs, LANES), 1) < HEAD
    removed = jnp.where(
        first_head,
        products_ref[pl.ds(0, seqs, stride=8), :],
        products_ref[pl.ds(2, seqs, stride=8), :],
    )
    faded = jnp.where(
        first_head,
        products_ref[pl.ds(1, seqs, stride=8), :],
        products_ref[pl.ds(3, seqs, stride=8), :],
    )
    removed_ref[...] = removed
    readout = (
        faded - removed * head_sums(unit_rate * recept) + values_now * head_sums(keys_now * recept)
    )
    centred = readout - head_sums(readout) * (1.0 / HEAD)
    spread = head_sums(centred * centred) * (1.0 / HEAD)
    mixed = (centred * lax.rsqrt(spread + GROUP_EPS) * group_gain_ref[...]).astype(BF16)
    copies[6 + chunks].wait()
    core = core_ref[0]
    for z in range(keep_ref.shape[0]):
        own = w_output_ref[:, pl.ds(pl.multiple_of((2 * z + core) * LANES, LANES), LANES)]
        keep_ref[z] = jnp.dot(mixed, own, preferred_element_type=F32)
        other = w_output_ref[:, pl.ds(pl.multiple_of((2 * z + 1 - core) * LANES, LANES), LANES)]
        send_ref[z] = jnp.dot(mixed, other, preferred_element_type=F32).astype(BF16)


def mix(core, tokens, state_rows, projections, w_output, mix_gain, vectors, z_count):
    seqs, full_width = tokens.shape
    chunks = 4
    chunk_rows = state_rows.shape[0] // chunks
    small = jax.ShapeDtypeStruct((seqs, LANES), F32)
    hbm = pl.BlockSpec(memory_space=pl.ANY)
    vmem = pl.BlockSpec(memory_space=VMEM)
    return pl.pallas_call(
        mix_kernel,
        out_shape=(
            jax.ShapeDtypeStruct((z_count, seqs, LANES), F32),
            jax.ShapeDtypeStruct((z_count, seqs, LANES), BF16),
            small,
            small,
            small,
            small,
            small,
        ),
        in_specs=[pl.BlockSpec(memory_space=pltpu.SMEM)] + [hbm] * 8 + [vmem] * 5,
        out_specs=(vmem,) * 7,
        scratch_shapes=[
            VMEM((seqs, full_width), BF16),
            VMEM((full_width, 5 * LANES), BF16),
            VMEM((LANES, full_width), BF16),
            VMEM((chunks, chunk_rows, HEAD), F32),
            VMEM((seqs * 8, LANES), F32),
            VMEM((seqs * 8, LANES), F32),
            pltpu.SemaphoreType.DMA((7 + chunks,)),
        ],
        compiler_params=pltpu.CompilerParams(vmem_limit_bytes=24 << 20),
        name="mix",
    )(core, tokens, state_rows, *projections, w_output, mix_gain, *vectors)


def update_kernel(
    state_ref,
    removed_ref,
    unit_rate_ref,
    decay_ref,
    key_ref,
    value_ref,
    out_ref,
    left_ref,
    right_ref,
):
    block = removed_ref.shape[0]
    first_head = lax.broadcasted_iota(jnp.int32, (block, LANES), 1) < HEAD
    removed = -removed_ref[...]
    removed_high = removed.astype(BF16).astype(F32)
    removed_low = removed - removed_high
    unit_rate = unit_rate_ref[...]
    unit_high = unit_rate.astype(BF16).astype(F32)
    unit_low = unit_rate - unit_high
    key = key_ref[...]
    lefts = (removed_high, removed_low, removed_high, value_ref[...])
    rights = (unit_high, unit_high, unit_low, key)
    for place in range(4):
        left_ref[pl.ds(place, block, stride=8), :] = jnp.where(first_head, lefts[place], 0.0)
        left_ref[pl.ds(place + 4, block, stride=8), :] = jnp.where(first_head, 0.0, lefts[place])
        right_ref[pl.ds(place, block, stride=8), :] = rights[place]
        right_ref[pl.ds(place + 4, block, stride=8), :] = pltpu.roll(rights[place], HEAD, 1)
    decay = decay_ref[...]
    decay_rolled = pltpu.roll(decay, HEAD, 1)
    for seq in range(block):
        left = left_ref[seq * 8 : seq * 8 + 8, :].astype(BF16)
        right = right_ref[seq * 8 : seq * 8 + 8, :HEAD].astype(BF16)
        change = lax.dot_general(
            left, right, (((0,), (0,)), ((), ())), preferred_element_type=F32
        )
        base = seq * LANES
        old = state_ref[base : base + HEAD, :]
        out_ref[base : base + HEAD, :] = old * decay[seq : seq + 1, :HEAD] + change[:HEAD]
        old = state_ref[base + HEAD : base + LANES, :]
        out_ref[base + HEAD : base + LANES, :] = (
            old * decay_rolled[seq : seq + 1, :HEAD] + change[HEAD:]
        )


def update_state(state_rows, removed, unit_rate, decay, key, value):
    seqs = removed.shape[0]
    steps = 8
    block = seqs // steps
    rows = pl.BlockSpec((block * LANES, HEAD), lambda i: (i, 0))
    small = pl.BlockSpec((block, LANES), lambda i: (i, 0))
    return pl.pallas_call(
        update_kernel,
        grid=(steps,),
        out_shape=jax.ShapeDtypeStruct(state_rows.shape, F32),
        in_specs=[rows] + [small] * 5,
        out_specs=rows,
        scratch_shapes=[VMEM((block * 8, LANES), F32), VMEM((block * 8, LANES), F32)],
        compiler_params=pltpu.CompilerParams(vmem_limit_bytes=8 << 20),
        cost_estimate=pl.CostEstimate(
            flops=2_000_000_000, bytes_accessed=8 << 20, transcendentals=0
        ),
        name="update_state",
    )(state_rows, removed, unit_rate, decay, key, value)


def pick_kernel(pick_ref, rows_ref, out_ref):
    for z in range(rows_ref.shape[0]):
        out_ref[:, z * LANES : (z + 1) * LANES] = jnp.dot(
            pick_ref[...], rows_ref[z], preferred_element_type=F32
        ).astype(BF16)


def pick_rows(pick, rows):
    return pl.pallas_call(
        pick_kernel,
        out_shape=jax.ShapeDtypeStruct((pick.shape[0], rows.shape[0] * LANES), BF16),
        compiler_params=pltpu.CompilerParams(vmem_limit_bytes=8 << 20),
        name="pick_rows",
    )(pick, rows)


def expert_kernel(
    core_ref,
    own_ref,
    other_ref,
    gain_ref,
    gate_ref,
    up_ref,
    down_ref,
    keep_ref,
    send_ref,
    x_ref,
    out_ref,
):
    core = core_ref[0]
    full_width = x_ref.shape[1]
    blocks = full_width // (2 * LANES)
    own = own_ref[...].astype(F32)
    other = other_ref[...].astype(F32)
    square_sum = jnp.sum(own * own, axis=1, keepdims=True) + jnp.sum(
        other * other, axis=1, keepdims=True
    )
    scale = lax.rsqrt(square_sum / full_width + RMS_EPS)
    for z in range(blocks):
        here = slice(z * LANES, (z + 1) * LANES)
        cols = pl.ds(pl.multiple_of((2 * z + core) * LANES, LANES), LANES)
        x_ref[:, cols] = (own[:, here] * scale * gain_ref[:, cols]).astype(BF16)
        cols = pl.ds(pl.multiple_of((2 * z + 1 - core) * LANES, LANES), LANES)
        x_ref[:, cols] = (other[:, here] * scale * gain_ref[:, cols]).astype(BF16)
    x = x_ref[...]
    across = (((1,), (1,)), ((), ()))
    gate_act = lax.dot_general(x, gate_ref[...], across, preferred_element_type=F32)
    upward = lax.dot_general(x, up_ref[...], across, preferred_element_type=F32)
    hidden = (jax.nn.silu(gate_act) * upward).astype(BF16)
    out_ref[...] = jnp.dot(hidden, down_ref[...], preferred_element_type=F32)
    for z in range(blocks):
        here = slice(z * LANES, (z + 1) * LANES)
        cols = pl.ds(pl.multiple_of((2 * z + core) * LANES, LANES), LANES)
        keep_ref[:, here] = out_ref[:, cols]
        cols = pl.ds(pl.multiple_of((2 * z + 1 - core) * LANES, LANES), LANES)
        send_ref[:, here] = out_ref[:, cols].astype(BF16)


def run_expert(core, own, other, gain, gate, up, down):
    rows, half = own.shape
    vmem = pl.BlockSpec(memory_space=VMEM)
    return pl.pallas_call(
        expert_kernel,
        out_shape=(
            jax.ShapeDtypeStruct((rows, half), F32),
            jax.ShapeDtypeStruct((rows, half), BF16),
        ),
        in_specs=[pl.BlockSpec(memory_space=pltpu.SMEM)] + [vmem] * 6,
        out_specs=(vmem, vmem),
        scratch_shapes=[VMEM((rows, 2 * half), BF16), VMEM((rows, 2 * half), F32)],
        compiler_params=pltpu.CompilerParams(vmem_limit_bytes=24 << 20),
        name="expert",
    )(core, own, other, gain, gate, up, down)


def combine_kernel(weight_ref, rows_ref, out_ref):
    weight = weight_ref[...]
    high = weight.astype(BF16)
    low = (weight - high.astype(F32)).astype(BF16)
    for z in range(out_ref.shape[0]):
        rows = rows_ref[:, z * LANES : (z + 1) * LANES]
        total = jnp.dot(high, rows, preferred_element_type=F32) + jnp.dot(
            low, rows, preferred_element_type=F32
        )
        out_ref[z] = total.astype(BF16)


def combine_rows(weight, rows):
    z_count = rows.shape[1] // LANES
    return pl.pallas_call(
        combine_kernel,
        out_shape=jax.ShapeDtypeStruct((z_count, weight.shape[0], LANES), BF16),
        compiler_params=pltpu.CompilerParams(vmem_limit_bytes=8 << 20),
        name="combine",
    )(weight, rows)


def slot_numbers(route_rows, expert_count, capacity):
    flat_routes = route_rows.reshape(-1)
    one_hot = (flat_routes[:, None] == jnp.arange(expert_count, dtype=jnp.int32)[None, :]).astype(
        jnp.int32
    )
    earlier = jnp.cumsum(one_hot, axis=0) - one_hot
    placed = jnp.sum(earlier * one_hot, axis=1)
    return (flat_routes * capacity + placed).reshape(route_rows.shape)


def swap(shard):
    return lax.ppermute(shard, "tp_1", [(0, 1), (1, 0)])


def exchange(shard, axis):
    return lax.all_to_all(shard, axis, split_axis=0, concat_axis=0, tiled=True)


def local(
    tokens,
    state,
    routes,
    route_logits,
    mix_gain,
    w_recept,
    w_key,
    w_value,
    w_decay,
    w_rate,
    decay_base,
    rate_base,
    key_gain,
    group_gain,
    w_output,
    ffn_gain,
    w_gate,
    w_up,
    w_down,
):
    seq_rows, full_width = tokens.shape
    z_count = lax.axis_size("tp_0")
    share_cols = full_width // lax.axis_size(TP)
    tp_index = lax.axis_index(TP)
    core = lax.axis_index("tp_1").astype(jnp.int32).reshape(1)
    group_count = lax.axis_size("ep")
    slot_rows = 16
    slot_count = group_count * slot_rows
    half = full_width // 2

    state_rows = state.reshape(-1, HEAD)
    keep, send, removed, unit_rate, decay, key, value = mix(
        core,
        tokens,
        state_rows,
        (w_recept, w_key, w_value, w_decay, w_rate),
        w_output,
        mix_gain.reshape(1, -1),
        [v.reshape(1, -1) for v in (decay_base, rate_base, key_gain, group_gain)],
        z_count,
    )
    pair_sum = (keep + swap(send).astype(F32)).astype(BF16)
    parts = exchange(pair_sum, "tp_0")
    new_state = update_state(state_rows, removed, unit_rate, decay, key, value)

    slot_ids = slot_numbers(routes, group_count, slot_rows)
    slot_range = jnp.arange(slot_count, dtype=jnp.int32)
    pick = jnp.any(slot_ids[None, :, :] == slot_range[:, None, None], axis=2).astype(BF16)
    route_exp = jnp.exp(route_logits)
    route_weight = route_exp / jnp.sum(route_exp, axis=1, keepdims=True)
    weight = jnp.sum(
        jnp.where(slot_ids[:, :, None] == slot_range[None, None, :], route_weight[:, :, None], 0.0),
        axis=1,
    )

    own_vals = lax.dynamic_slice_in_dim(tokens, tp_index * share_cols, share_cols, 1)
    resid_own = (own_vals.astype(F32) + parts.astype(F32).sum(axis=0)).astype(BF16)
    resid_half = exchange(jnp.broadcast_to(resid_own, (z_count, *resid_own.shape)), "tp_0")
    outgoing = pick_rows(pick, resid_half)
    arrived = exchange(outgoing.reshape(group_count, slot_rows, half), "ep")
    arrived = arrived.reshape(slot_count, half)
    keep, send = run_expert(
        core,
        arrived,
        swap(arrived),
        ffn_gain.reshape(1, -1),
        jnp.swapaxes(w_gate[0], 0, 1),
        jnp.swapaxes(w_up[0], 0, 1),
        w_down[0],
    )
    pair_sum = (keep + swap(send).astype(F32)).astype(BF16)
    returned = exchange(pair_sum.reshape(group_count, slot_rows, half), "ep")
    moe_parts = exchange(combine_rows(weight, returned.reshape(slot_count, half)), "tp_0")
    moe_own = moe_parts.astype(F32).sum(axis=0)
    output = (resid_own.astype(F32) + moe_own).astype(BF16)
    return (output, new_state.reshape(state.shape))


def solution(mesh):
    torus = Mesh(mesh.devices.reshape(mesh.shape["ep"], 8, 2), ("ep", "tp_0", "tp_1"))
    return jax.shard_map(
        local,
        mesh=torus,
        in_specs=(
            P("ep", None),
            P("ep", TP, None, None),
            P("ep", None),
            P("ep", None),
            P(),
            P(None, TP),
            P(None, TP),
            P(None, TP),
            P(None, TP),
            P(None, TP),
            P(TP),
            P(TP),
            P(TP),
            P(TP),
            P(TP, None),
            P(),
            P("ep", None, TP),
            P("ep", None, TP),
            P("ep", TP, None),
        ),
        out_specs=(P("ep", TP), P("ep", TP, None, None)),
        check_vma=False,
    )
```

```python
import jax
import jax.numpy as jnp
from jax import lax
from jax.experimental import pallas as pl
from jax.experimental.pallas import tpu as pltpu
from jax.sharding import Mesh
from jax.sharding import PartitionSpec as P

TP = ("tp_0", "tp_1")

RMS_EPS = 1e-06
GROUP_EPS = 0.00064
UNIT_EPS = 6.4e-05
HIGHEST = lax.Precision.HIGHEST
F32 = jnp.float32
BF16 = jnp.bfloat16
VMEM = pltpu.VMEM
HEAD = 64
LANES = 128


def in_hbm(array):
    return pltpu.with_memory_space_constraint(array, pltpu.HBM)


def head_sums(values):
    rows = lax.broadcasted_iota(jnp.int32, (LANES, LANES), 0) // HEAD
    cols = lax.broadcasted_iota(jnp.int32, (LANES, LANES), 1) // HEAD
    ones = (rows == cols).astype(F32)
    return jnp.dot(values, ones, precision=HIGHEST, preferred_element_type=F32)


def mix_kernel(
    core_ref,
    tokens_hbm,
    state_hbm,
    w_recept_hbm,
    w_key_hbm,
    w_value_hbm,
    w_decay_hbm,
    w_rate_hbm,
    w_output_hbm,
    mix_gain_hbm,
    decay_base_hbm,
    rate_base_hbm,
    key_gain_hbm,
    group_gain_hbm,
    keep_ref,
    send_ref,
    removed_ref,
    unit_rate_ref,
    decay_ref,
    key_ref,
    value_ref,
    tokens_ref,
    weights_ref,
    w_output_ref,
    state_ref,
    mix_gain_ref,
    decay_base_ref,
    rate_base_ref,
    key_gain_ref,
    group_gain_ref,
    vectors_ref,
    products_ref,
    sems,
    small_sems,
):
    seqs = tokens_ref.shape[0]
    chunks = state_ref.shape[0]
    chunk_rows = state_ref.shape[1]
    copies = [pltpu.make_async_copy(tokens_hbm, tokens_ref, sems.at[0])]
    smalls = [
        pltpu.make_async_copy(source, target, small_sems.at[place])
        for place, (source, target) in enumerate(
            (
                (mix_gain_hbm, mix_gain_ref),
                (key_gain_hbm, key_gain_ref),
                (decay_base_hbm, decay_base_ref),
                (rate_base_hbm, rate_base_ref),
                (group_gain_hbm, group_gain_ref),
            )
        )
    ]
    sources = (w_key_hbm, w_value_hbm, w_recept_hbm, w_decay_hbm, w_rate_hbm)
    for place, source in enumerate(sources):
        target = weights_ref.at[:, pl.ds(place * LANES, LANES)]
        copies.append(pltpu.make_async_copy(source, target, sems.at[1 + place]))
    for chunk in range(chunks):
        source = state_hbm.at[pl.ds(chunk * chunk_rows, chunk_rows)]
        copies.append(pltpu.make_async_copy(source, state_ref.at[chunk], sems.at[6 + chunk]))
    copies.append(pltpu.make_async_copy(w_output_hbm, w_output_ref, sems.at[6 + chunks]))
    copies[0].start()
    for copy in smalls:
        copy.start()
    for copy in copies[1:]:
        copy.start()

    copies[0].wait()
    for copy in smalls:
        copy.wait()
    values = tokens_ref[...].astype(F32)
    mean_square = jnp.mean(values * values, axis=1, keepdims=True)
    normed = (values * lax.rsqrt(mean_square + RMS_EPS) * mix_gain_ref[...]).astype(BF16)

    def project(first, count):
        for place in range(first, first + count):
            copies[1 + place].wait()
        weight = weights_ref[:, first * LANES : (first + count) * LANES]
        return jnp.dot(normed, weight, preferred_element_type=F32).astype(BF16).astype(F32)

    key_value = project(0, 2)
    keys_now = key_value[:, :LANES]
    values_now = key_value[:, LANES:]
    recept_decay = project(2, 2)
    recept = recept_decay[:, :LANES]
    decay_pre = recept_decay[:, LANES:] + decay_base_ref[...]
    rate_pre = project(4, 1) + rate_base_ref[...]
    decay_now = jnp.exp(-jnp.exp(-jax.nn.softplus(-decay_pre) - 0.5))
    rate_now = jax.nn.sigmoid(rate_pre)
    scaled = keys_now * key_gain_ref[...]
    unit_key = scaled * lax.rsqrt(head_sums(scaled * scaled) + UNIT_EPS)
    unit_rate = unit_key * rate_now
    decayed_recept = decay_now * recept
    unit_rate_ref[...] = unit_rate
    decay_ref[...] = decay_now
    key_ref[...] = keys_now
    value_ref[...] = values_now

    vectors_ref[...] = jnp.zeros_like(vectors_ref)
    vectors_ref[pl.ds(0, seqs, stride=8), :] = unit_key
    vectors_ref[pl.ds(1, seqs, stride=8), :] = decayed_recept
    vectors_ref[pl.ds(2, seqs, stride=8), :] = pltpu.roll(unit_key, HEAD, 1)
    vectors_ref[pl.ds(3, seqs, stride=8), :] = pltpu.roll(decayed_recept, HEAD, 1)
    per_chunk = chunk_rows // LANES
    for chunk in range(chunks):
        copies[6 + chunk].wait()
        for inner in range(per_chunk):
            seq = chunk * per_chunk + inner
            left = vectors_ref[seq * 8 : seq * 8 + 8, :HEAD].astype(BF16)
            right = state_ref[chunk, inner * LANES : (inner + 1) * LANES, :].astype(BF16)
            products_ref[seq * 8 : seq * 8 + 8, :] = lax.dot_general(
                left, right, (((1,), (1,)), ((), ())), preferred_element_type=F32
            )
    first_head = lax.broadcasted_iota(jnp.int32, (seqs, LANES), 1) < HEAD
    removed = jnp.where(
        first_head,
        products_ref[pl.ds(0, seqs, stride=8), :],
        products_ref[pl.ds(2, seqs, stride=8), :],
    )
    faded = jnp.where(
        first_head,
        products_ref[pl.ds(1, seqs, stride=8), :],
        products_ref[pl.ds(3, seqs, stride=8), :],
    )
    removed_ref[...] = removed
    readout = (
        faded - removed * head_sums(unit_rate * recept) + values_now * head_sums(keys_now * recept)
    )
    centred = readout - head_sums(readout) * (1.0 / HEAD)
    spread = head_sums(centred * centred) * (1.0 / HEAD)
    mixed = (centred * lax.rsqrt(spread + GROUP_EPS) * group_gain_ref[...]).astype(BF16)
    copies[6 + chunks].wait()
    core = core_ref[0]
    for z in range(keep_ref.shape[0]):
        own = w_output_ref[:, pl.ds(pl.multiple_of((2 * z + core) * LANES, LANES), LANES)]
        keep_ref[z] = jnp.dot(mixed, own, preferred_element_type=F32)
        other = w_output_ref[:, pl.ds(pl.multiple_of((2 * z + 1 - core) * LANES, LANES), LANES)]
        send_ref[z] = jnp.dot(mixed, other, preferred_element_type=F32).astype(BF16)


def mix(core, tokens, state_rows, projections, w_output, mix_gain, vectors, z_count):
    seqs, full_width = tokens.shape
    chunks = 4
    chunk_rows = state_rows.shape[0] // chunks
    small = jax.ShapeDtypeStruct((seqs, LANES), F32)
    hbm = pl.BlockSpec(memory_space=pl.ANY)
    vmem = pl.BlockSpec(memory_space=VMEM)
    return pl.pallas_call(
        mix_kernel,
        out_shape=(
            jax.ShapeDtypeStruct((z_count, seqs, LANES), F32),
            jax.ShapeDtypeStruct((z_count, seqs, LANES), BF16),
            small,
            small,
            small,
            small,
            small,
        ),
        in_specs=[pl.BlockSpec(memory_space=pltpu.SMEM)] + [hbm] * 13,
        out_specs=(vmem,) * 7,
        scratch_shapes=[
            VMEM((seqs, full_width), BF16),
            VMEM((full_width, 5 * LANES), BF16),
            VMEM((LANES, full_width), BF16),
            VMEM((chunks, chunk_rows, HEAD), F32),
            VMEM((1, full_width), F32),
            VMEM((1, LANES), F32),
            VMEM((1, LANES), F32),
            VMEM((1, LANES), F32),
            VMEM((1, LANES), F32),
            VMEM((seqs * 8, LANES), F32),
            VMEM((seqs * 8, LANES), F32),
            pltpu.SemaphoreType.DMA((7 + chunks,)),
            pltpu.SemaphoreType.DMA((5,)),
        ],
        compiler_params=pltpu.CompilerParams(vmem_limit_bytes=16 << 20),
        name="mix",
    )(core, *map(in_hbm, (tokens, state_rows, *projections, w_output, mix_gain, *vectors)))


def update_kernel(
    state_ref,
    removed_ref,
    unit_rate_ref,
    decay_ref,
    key_ref,
    value_ref,
    out_ref,
    left_ref,
    right_ref,
):
    block = removed_ref.shape[0]
    first_head = lax.broadcasted_iota(jnp.int32, (block, LANES), 1) < HEAD
    removed = -removed_ref[...]
    removed_high = removed.astype(BF16).astype(F32)
    removed_low = removed - removed_high
    unit_rate = unit_rate_ref[...]
    unit_high = unit_rate.astype(BF16).astype(F32)
    unit_low = unit_rate - unit_high
    key = key_ref[...]
    lefts = (removed_high, removed_low, removed_high, value_ref[...])
    rights = (unit_high, unit_high, unit_low, key)
    for place in range(4):
        left_ref[pl.ds(place, block, stride=8), :] = jnp.where(first_head, lefts[place], 0.0)
        left_ref[pl.ds(place + 4, block, stride=8), :] = jnp.where(first_head, 0.0, lefts[place])
        right_ref[pl.ds(place, block, stride=8), :] = rights[place]
        right_ref[pl.ds(place + 4, block, stride=8), :] = pltpu.roll(rights[place], HEAD, 1)
    decay = decay_ref[...]
    decay_rolled = pltpu.roll(decay, HEAD, 1)
    for seq in range(block):
        left = left_ref[seq * 8 : seq * 8 + 8, :].astype(BF16)
        right = right_ref[seq * 8 : seq * 8 + 8, :HEAD].astype(BF16)
        change = lax.dot_general(
            left, right, (((0,), (0,)), ((), ())), preferred_element_type=F32
        )
        base = seq * LANES
        old = state_ref[base : base + HEAD, :]
        out_ref[base : base + HEAD, :] = old * decay[seq : seq + 1, :HEAD] + change[:HEAD]
        old = state_ref[base + HEAD : base + LANES, :]
        out_ref[base + HEAD : base + LANES, :] = (
            old * decay_rolled[seq : seq + 1, :HEAD] + change[HEAD:]
        )


def update_state(state_rows, removed, unit_rate, decay, key, value):
    seqs = removed.shape[0]
    steps = 8
    block = seqs // steps
    rows = pl.BlockSpec((block * LANES, HEAD), lambda i: (i, 0))
    small = pl.BlockSpec((block, LANES), lambda i: (i, 0))
    return pl.pallas_call(
        update_kernel,
        grid=(steps,),
        out_shape=jax.ShapeDtypeStruct(state_rows.shape, F32),
        in_specs=[rows] + [small] * 5,
        out_specs=rows,
        scratch_shapes=[VMEM((block * 8, LANES), F32), VMEM((block * 8, LANES), F32)],
        compiler_params=pltpu.CompilerParams(vmem_limit_bytes=8 << 20),
        cost_estimate=pl.CostEstimate(
            flops=2_000_000_000, bytes_accessed=8 << 20, transcendentals=0
        ),
        name="update_state",
    )(in_hbm(state_rows), removed, unit_rate, decay, key, value)


def stage_kernel(after_ref, gate_hbm, up_hbm, down_hbm, gate_ref, up_ref, down_ref, sems):
    copies = [
        pltpu.make_async_copy(source, target, sems.at[place])
        for place, (source, target) in enumerate(
            ((gate_hbm, gate_ref), (up_hbm, up_ref), (down_hbm, down_ref))
        )
    ]
    for copy in copies:
        copy.start()
    for copy in copies:
        copy.wait()


def stage_weights(after, gate, up, down):
    weights = (gate, up, down)
    return pl.pallas_call(
        stage_kernel,
        out_shape=tuple(jax.ShapeDtypeStruct(w.shape, w.dtype) for w in weights),
        in_specs=[pl.BlockSpec(memory_space=pl.ANY)] * 4,
        out_specs=(pl.BlockSpec(memory_space=VMEM),) * 3,
        scratch_shapes=[pltpu.SemaphoreType.DMA((3,))],
        compiler_params=pltpu.CompilerParams(vmem_limit_bytes=1 << 20),
        name="stage_weights",
    )(after, *map(in_hbm, weights))


def dispatch_kernel(parts_ref, tokens_ref, pick_ref, resid_ref, out_ref):
    total = tokens_ref[...].astype(F32)
    mix = parts_ref[0].astype(F32)
    for z in range(1, parts_ref.shape[0]):
        mix = mix + parts_ref[z].astype(F32)
    resid = (total + mix).astype(BF16)
    resid_ref[...] = resid
    picked = jnp.dot(pick_ref[...], resid, preferred_element_type=F32).astype(BF16)
    for z in range(out_ref.shape[0]):
        out_ref[z] = picked


def dispatch_rows(parts, tokens, pick):
    return pl.pallas_call(
        dispatch_kernel,
        out_shape=(
            jax.ShapeDtypeStruct(tokens.shape, BF16),
            jax.ShapeDtypeStruct((parts.shape[0], pick.shape[0], LANES), BF16),
        ),
        compiler_params=pltpu.CompilerParams(vmem_limit_bytes=4 << 20),
        name="dispatch_rows",
    )(parts, tokens, pick)


def expert_kernel(
    core_ref,
    own_ref,
    other_ref,
    gain_ref,
    gate_ref,
    up_ref,
    down_ref,
    keep_ref,
    send_ref,
    x_ref,
    out_ref,
):
    core = core_ref[0]
    full_width = x_ref.shape[1]
    blocks = own_ref.shape[0]
    squares = jnp.zeros(own_ref.shape[1:], F32)
    for z in range(blocks):
        for part in (own_ref, other_ref):
            rows = part[z].astype(F32)
            squares = squares + rows * rows
    scale = lax.rsqrt(jnp.sum(squares, axis=1, keepdims=True) / full_width + RMS_EPS)
    for z in range(blocks):
        for part, place in ((own_ref, 2 * z + core), (other_ref, 2 * z + 1 - core)):
            cols = pl.ds(pl.multiple_of(place * LANES, LANES), LANES)
            x_ref[:, cols] = (part[z].astype(F32) * scale * gain_ref[:, cols]).astype(BF16)
    x = x_ref[...]
    across = (((1,), (1,)), ((), ()))
    gate_act = lax.dot_general(x, gate_ref[...], across, preferred_element_type=F32)
    upward = lax.dot_general(x, up_ref[...], across, preferred_element_type=F32)
    hidden = (jax.nn.silu(gate_act) * upward).astype(BF16)
    out_ref[...] = jnp.dot(hidden, down_ref[...], preferred_element_type=F32)
    for z in range(blocks):
        cols = pl.ds(pl.multiple_of((2 * z + core) * LANES, LANES), LANES)
        keep_ref[z] = out_ref[:, cols]
        cols = pl.ds(pl.multiple_of((2 * z + 1 - core) * LANES, LANES), LANES)
        send_ref[z] = out_ref[:, cols].astype(BF16)


def run_expert(core, own, other, gain, gate, up, down):
    rows = own.shape[1]
    full_width = gate.shape[1]
    vmem = pl.BlockSpec(memory_space=VMEM)
    return pl.pallas_call(
        expert_kernel,
        out_shape=(
            jax.ShapeDtypeStruct(own.shape, F32),
            jax.ShapeDtypeStruct(own.shape, BF16),
        ),
        in_specs=[pl.BlockSpec(memory_space=pltpu.SMEM)] + [vmem] * 6,
        out_specs=(vmem, vmem),
        scratch_shapes=[VMEM((rows, full_width), BF16), VMEM((rows, full_width), F32)],
        compiler_params=pltpu.CompilerParams(vmem_limit_bytes=10 << 20),
        name="expert",
    )(core, own, other, gain, gate, up, down)


def combine_kernel(weight_ref, rows_ref, resid_ref, out_ref):
    rows = rows_ref[0].astype(F32)
    for z in range(1, rows_ref.shape[0]):
        rows = rows + rows_ref[z].astype(F32)
    moe = jnp.dot(weight_ref[...], rows, precision=HIGHEST, preferred_element_type=F32)
    out_ref[...] = (resid_ref[...].astype(F32) + moe).astype(BF16)


def combine_rows(weight, rows, resid):
    return pl.pallas_call(
        combine_kernel,
        out_shape=jax.ShapeDtypeStruct(resid.shape, BF16),
        compiler_params=pltpu.CompilerParams(vmem_limit_bytes=4 << 20),
        name="combine",
    )(weight, rows, resid)


def slot_numbers(route_rows, expert_count, capacity):
    flat_routes = route_rows.reshape(-1)
    one_hot = (flat_routes[:, None] == jnp.arange(expert_count, dtype=jnp.int32)[None, :]).astype(
        jnp.int32
    )
    earlier = jnp.cumsum(one_hot, axis=0) - one_hot
    placed = jnp.sum(earlier * one_hot, axis=1)
    return (flat_routes * capacity + placed).reshape(route_rows.shape)


def swap(shard):
    return lax.ppermute(shard, "tp_1", [(0, 1), (1, 0)])


def exchange(shard, axis):
    return lax.all_to_all(shard, axis, split_axis=0, concat_axis=0, tiled=True)


def exchange_rows(shard):
    groups = lax.axis_size("ep") * lax.axis_size("tp_0")
    chunks = shard.reshape(groups, -1, 4, LANES)
    return exchange(chunks, ("tp_0", "ep")).reshape(shard.shape)


def local(
    tokens,
    state,
    routes,
    route_logits,
    mix_gain,
    w_recept,
    w_key,
    w_value,
    w_decay,
    w_rate,
    decay_base,
    rate_base,
    key_gain,
    group_gain,
    w_output,
    ffn_gain,
    w_gate,
    w_up,
    w_down,
):
    seq_rows, full_width = tokens.shape
    z_count = lax.axis_size("tp_0")
    share_cols = full_width // lax.axis_size(TP)
    tp_index = lax.axis_index(TP)
    core = lax.axis_index("tp_1").astype(jnp.int32).reshape(1)
    group_count = lax.axis_size("ep")
    slot_rows = max(2, 3 * routes.shape[1] * seq_rows // (2 * group_count))
    slot_count = group_count * slot_rows

    state_rows = state.reshape(-1, HEAD)
    keep, send, removed, unit_rate, decay, key, value = mix(
        core,
        tokens,
        state_rows,
        (w_recept, w_key, w_value, w_decay, w_rate),
        w_output,
        mix_gain.reshape(1, -1),
        [v.reshape(1, -1) for v in (decay_base, rate_base, key_gain, group_gain)],
        z_count,
    )
    pair_sum = (keep + swap(send).astype(F32)).astype(BF16)
    parts = exchange(pair_sum, "tp_0")
    new_state = update_state(state_rows, removed, unit_rate, decay, key, value)

    slot_ids = slot_numbers(routes, group_count, slot_rows)
    slot_range = jnp.arange(slot_count, dtype=jnp.int32)
    pick = jnp.any(slot_ids[None, :, :] == slot_range[:, None, None], axis=2).astype(BF16)
    route_exp = jnp.exp(route_logits)
    route_weight = route_exp / jnp.sum(route_exp, axis=1, keepdims=True)
    weight = jnp.sum(
        jnp.where(slot_ids[:, :, None] == slot_range[None, None, :], route_weight[:, :, None], 0.0),
        axis=1,
    )

    own_tokens = lax.dynamic_slice_in_dim(tokens, tp_index * share_cols, share_cols, 1)
    gain = ffn_gain.reshape(1, -1)
    parts, new_state, pick, weight, own_tokens, gain = lax.optimization_barrier(
        (parts, new_state, pick, weight, own_tokens, gain)
    )
    resid_own, outgoing = dispatch_rows(parts, own_tokens, pick)
    arrived = exchange_rows(outgoing)
    weights = stage_weights(
        arrived, jnp.swapaxes(w_gate[0], 0, 1), jnp.swapaxes(w_up[0], 0, 1), w_down[0]
    )
    keep, send = run_expert(core, arrived, swap(arrived), gain, *weights)
    pair_sum = (keep + swap(send).astype(F32)).astype(BF16)
    output = combine_rows(weight, exchange_rows(pair_sum), resid_own)
    return (output, new_state.reshape(state.shape))


def solution(mesh):
    torus = Mesh(mesh.devices.reshape(mesh.shape["ep"], 8, 2), ("ep", "tp_0", "tp_1"))
    return jax.shard_map(
        local,
        mesh=torus,
        in_specs=(
            P("ep", None),
            P("ep", TP, None, None),
            P("ep", None),
            P("ep", None),
            P(),
            P(None, TP),
            P(None, TP),
            P(None, TP),
            P(None, TP),
            P(None, TP),
            P(TP),
            P(TP),
            P(TP),
            P(TP),
            P(TP, None),
            P(),
            P("ep", None, TP),
            P("ep", None, TP),
            P("ep", TP, None),
        ),
        out_specs=(P("ep", TP), P("ep", TP, None, None)),
        check_vma=False,
    )
```

```python
import jax
import jax.numpy as jnp
from jax import lax
from jax.experimental import pallas as pl
from jax.experimental.pallas import tpu as pltpu
from jax.sharding import Mesh
from jax.sharding import PartitionSpec as P

TP = ("tp_0", "tp_1")

RMS_EPS = 1e-06
GROUP_EPS = 0.00064
UNIT_EPS = 6.4e-05
HIGHEST = lax.Precision.HIGHEST
F32 = jnp.float32
BF16 = jnp.bfloat16
VMEM = pltpu.VMEM
HEAD = 64
LANES = 128


def in_hbm(array):
    return pltpu.with_memory_space_constraint(array, pltpu.HBM)


def head_sums(values):
    rows = lax.broadcasted_iota(jnp.int32, (LANES, LANES), 0) // HEAD
    cols = lax.broadcasted_iota(jnp.int32, (LANES, LANES), 1) // HEAD
    ones = (rows == cols).astype(F32)
    return jnp.dot(values, ones, precision=HIGHEST, preferred_element_type=F32)


def route_slots(routes, logits, pick_ref, share_ref):
    slots, seqs = pick_ref.shape
    experts = lax.axis_size("ep")
    first, second = routes[0:1, :], routes[1:2, :]
    expert = lax.broadcasted_iota(jnp.int32, (experts, seqs), 0)
    named = [(expert == choice).astype(F32) for choice in (first, second)]
    earlier = lax.broadcasted_iota(jnp.int32, (seqs, seqs), 0) < lax.broadcasted_iota(
        jnp.int32, (seqs, seqs), 1
    )
    counts = jnp.dot(
        (named[0] + named[1]).astype(BF16),
        earlier.astype(F32).astype(BF16),
        preferred_element_type=F32,
    )
    exps = jnp.exp(logits)
    total = exps[0:1, :] + exps[1:2, :]
    slot = lax.broadcasted_iota(jnp.int32, (slots, seqs), 0)
    picked = jnp.zeros((slots, seqs), F32)
    shares = jnp.zeros((slots, seqs), F32)
    for k, choice in enumerate((first, second)):
        placed = jnp.sum(named[k] * counts, axis=0, keepdims=True).astype(jnp.int32)
        here = slot == choice * (slots // experts) + placed
        picked = jnp.where(here, 1.0, picked)
        shares = jnp.where(here, exps[k : k + 1, :] / total, shares)
    pick_ref[...] = picked.astype(BF16)
    share_ref[...] = shares


def project_kernel(
    tokens_hbm,
    w_recept_hbm,
    w_key_hbm,
    w_value_hbm,
    w_decay_hbm,
    w_rate_hbm,
    mix_gain_hbm,
    decay_base_hbm,
    rate_base_hbm,
    key_gain_hbm,
    routes_hbm,
    logits_hbm,
    vectors_ref,
    recept_ref,
    unit_rate_ref,
    decay_ref,
    key_ref,
    value_ref,
    own_ref,
    pick_ref,
    share_ref,
    tokens_ref,
    weights_ref,
    mix_gain_ref,
    decay_base_ref,
    rate_base_ref,
    key_gain_ref,
    routes_ref,
    logits_ref,
    sems,
    small_sems,
):
    seqs = tokens_ref.shape[0]
    copies = [pltpu.make_async_copy(tokens_hbm, tokens_ref, sems.at[0])]
    smalls = [
        pltpu.make_async_copy(source, target, small_sems.at[place])
        for place, (source, target) in enumerate(
            (
                (mix_gain_hbm, mix_gain_ref),
                (key_gain_hbm, key_gain_ref),
                (decay_base_hbm, decay_base_ref),
                (rate_base_hbm, rate_base_ref),
                (routes_hbm, routes_ref),
                (logits_hbm, logits_ref),
            )
        )
    ]
    sources = (w_key_hbm, w_value_hbm, w_recept_hbm, w_decay_hbm, w_rate_hbm)
    for place, source in enumerate(sources):
        target = weights_ref.at[:, pl.ds(place * LANES, LANES)]
        copies.append(pltpu.make_async_copy(source, target, sems.at[1 + place]))
    copies[0].start()
    for copy in smalls:
        copy.start()
    for copy in copies[1:]:
        copy.start()

    for copy in smalls:
        copy.wait()
    route_slots(routes_ref[...], logits_ref[...], pick_ref, share_ref)
    copies[0].wait()
    own_ref[...] = tokens_ref[:, pl.ds(pl.multiple_of(lax.axis_index(TP) * LANES, LANES), LANES)]
    values = tokens_ref[...].astype(F32)
    mean_square = jnp.mean(values * values, axis=1, keepdims=True)
    normed = (values * lax.rsqrt(mean_square + RMS_EPS) * mix_gain_ref[...]).astype(BF16)

    def project(first, count):
        for place in range(first, first + count):
            copies[1 + place].wait()
        weight = weights_ref[:, first * LANES : (first + count) * LANES]
        return jnp.dot(normed, weight, preferred_element_type=F32).astype(BF16).astype(F32)

    key_value = project(0, 2)
    keys_now = key_value[:, :LANES]
    key_ref[...] = keys_now
    value_ref[...] = key_value[:, LANES:]
    scaled = keys_now * key_gain_ref[...]
    unit_key = scaled * lax.rsqrt(head_sums(scaled * scaled) + UNIT_EPS)
    vectors_ref[...] = jnp.zeros_like(vectors_ref)
    vectors_ref[pl.ds(0, seqs, stride=8), :] = unit_key
    vectors_ref[pl.ds(2, seqs, stride=8), :] = pltpu.roll(unit_key, HEAD, 1)
    recept_decay = project(2, 2)
    recept = recept_decay[:, :LANES]
    recept_ref[...] = recept
    decay_pre = recept_decay[:, LANES:] + decay_base_ref[...]
    decay_now = jnp.exp(-jnp.exp(-jax.nn.softplus(-decay_pre) - 0.5))
    decay_ref[...] = decay_now
    decayed_recept = decay_now * recept
    vectors_ref[pl.ds(1, seqs, stride=8), :] = decayed_recept
    vectors_ref[pl.ds(3, seqs, stride=8), :] = pltpu.roll(decayed_recept, HEAD, 1)
    rate_pre = project(4, 1) + rate_base_ref[...]
    unit_rate_ref[...] = unit_key * jax.nn.sigmoid(rate_pre)


def project_heads(tokens, projections, mix_gain, vectors, routes, logits, slots):
    seqs, full_width = tokens.shape
    small = jax.ShapeDtypeStruct((seqs, LANES), F32)
    hbm = pl.BlockSpec(memory_space=pl.ANY)
    vmem = pl.BlockSpec(memory_space=VMEM)
    return pl.pallas_call(
        project_kernel,
        out_shape=(jax.ShapeDtypeStruct((seqs * 8, LANES), F32),)
        + (small,) * 5
        + (
            jax.ShapeDtypeStruct((seqs, LANES), BF16),
            jax.ShapeDtypeStruct((slots, seqs), BF16),
            jax.ShapeDtypeStruct((slots, seqs), F32),
        ),
        in_specs=[hbm] * 12,
        out_specs=(vmem,) * 9,
        scratch_shapes=[
            VMEM((seqs, full_width), BF16),
            VMEM((full_width, 5 * LANES), BF16),
            VMEM((1, full_width), F32),
            VMEM((1, LANES), F32),
            VMEM((1, LANES), F32),
            VMEM((1, LANES), F32),
            VMEM(routes.shape, jnp.int32),
            VMEM(logits.shape, F32),
            pltpu.SemaphoreType.DMA((6,)),
            pltpu.SemaphoreType.DMA((6,)),
        ],
        compiler_params=pltpu.CompilerParams(vmem_limit_bytes=12 << 20),
        cost_estimate=pl.CostEstimate(
            flops=3_000_000_000, bytes_accessed=6 << 20, transcendentals=0
        ),
        name="project_heads",
    )(*map(in_hbm, (tokens, *projections, mix_gain, *vectors, routes, logits)))


def mix_kernel(
    state_ref,
    vectors_ref,
    recept_ref,
    unit_rate_ref,
    key_ref,
    value_ref,
    w_output_ref,
    group_gain_ref,
    keep_ref,
    send_ref,
    removed_ref,
    products_ref,
):
    seqs = recept_ref.shape[0]
    for seq in range(seqs):
        left = vectors_ref[seq * 8 : seq * 8 + 8, :HEAD].astype(BF16)
        right = state_ref[seq * LANES : (seq + 1) * LANES, :].astype(BF16)
        products_ref[seq * 8 : seq * 8 + 8, :] = lax.dot_general(
            left, right, (((1,), (1,)), ((), ())), preferred_element_type=F32
        )
    first_head = lax.broadcasted_iota(jnp.int32, (seqs, LANES), 1) < HEAD
    removed = jnp.where(
        first_head,
        products_ref[pl.ds(0, seqs, stride=8), :],
        products_ref[pl.ds(2, seqs, stride=8), :],
    )
    faded = jnp.where(
        first_head,
        products_ref[pl.ds(1, seqs, stride=8), :],
        products_ref[pl.ds(3, seqs, stride=8), :],
    )
    removed_ref[...] = removed
    recept = recept_ref[...]
    readout = (
        faded
        - removed * head_sums(unit_rate_ref[...] * recept)
        + value_ref[...] * head_sums(key_ref[...] * recept)
    )
    centred = readout - head_sums(readout) * (1.0 / HEAD)
    spread = head_sums(centred * centred) * (1.0 / HEAD)
    mixed = (centred * lax.rsqrt(spread + GROUP_EPS) * group_gain_ref[...]).astype(BF16)
    core = lax.axis_index("tp_1")
    for z in range(keep_ref.shape[0]):
        own = w_output_ref[:, pl.ds(pl.multiple_of((2 * z + core) * LANES, LANES), LANES)]
        keep_ref[z] = jnp.dot(mixed, own, preferred_element_type=F32)
        other = w_output_ref[:, pl.ds(pl.multiple_of((2 * z + 1 - core) * LANES, LANES), LANES)]
        send_ref[z] = jnp.dot(mixed, other, preferred_element_type=F32).astype(BF16)


def mix(state_rows, vectors, recept, unit_rate, key, value, w_output, group_gain, z_count):
    seqs = recept.shape[0]
    vmem = pl.BlockSpec(memory_space=VMEM)
    return pl.pallas_call(
        mix_kernel,
        out_shape=(
            jax.ShapeDtypeStruct((z_count, seqs, LANES), F32),
            jax.ShapeDtypeStruct((z_count, seqs, LANES), BF16),
            jax.ShapeDtypeStruct((seqs, LANES), F32),
        ),
        in_specs=[vmem] * 8,
        out_specs=(vmem,) * 3,
        scratch_shapes=[VMEM((seqs * 8, LANES), F32)],
        compiler_params=pltpu.CompilerParams(vmem_limit_bytes=12 << 20),
        name="mix",
    )(state_rows, vectors, recept, unit_rate, key, value, w_output, group_gain)


def update_kernel(
    state_ref,
    removed_ref,
    unit_rate_ref,
    decay_ref,
    key_ref,
    value_ref,
    out_ref,
    left_ref,
    right_ref,
):
    block = removed_ref.shape[0]
    first_head = lax.broadcasted_iota(jnp.int32, (block, LANES), 1) < HEAD
    removed = -removed_ref[...]
    removed_high = removed.astype(BF16).astype(F32)
    removed_low = removed - removed_high
    unit_rate = unit_rate_ref[...]
    unit_high = unit_rate.astype(BF16).astype(F32)
    unit_low = unit_rate - unit_high
    key = key_ref[...]
    lefts = (removed_high, removed_low, removed_high, value_ref[...])
    rights = (unit_high, unit_high, unit_low, key)
    for place in range(4):
        left_ref[pl.ds(place, block, stride=8), :] = jnp.where(first_head, lefts[place], 0.0)
        left_ref[pl.ds(place + 4, block, stride=8), :] = jnp.where(first_head, 0.0, lefts[place])
        right_ref[pl.ds(place, block, stride=8), :] = rights[place]
        right_ref[pl.ds(place + 4, block, stride=8), :] = pltpu.roll(rights[place], HEAD, 1)
    decay = decay_ref[...]
    decay_rolled = pltpu.roll(decay, HEAD, 1)
    for seq in range(block):
        left = left_ref[seq * 8 : seq * 8 + 8, :].astype(BF16)
        right = right_ref[seq * 8 : seq * 8 + 8, :HEAD].astype(BF16)
        change = lax.dot_general(
            left, right, (((0,), (0,)), ((), ())), preferred_element_type=F32
        )
        base = seq * LANES
        old = state_ref[base : base + HEAD, :]
        out_ref[base : base + HEAD, :] = old * decay[seq : seq + 1, :HEAD] + change[:HEAD]
        old = state_ref[base + HEAD : base + LANES, :]
        out_ref[base + HEAD : base + LANES, :] = (
            old * decay_rolled[seq : seq + 1, :HEAD] + change[HEAD:]
        )


def update_state(state_rows, removed, unit_rate, decay, key, value):
    seqs = removed.shape[0]
    steps = 8
    block = seqs // steps
    rows = pl.BlockSpec((block * LANES, HEAD), lambda i: (i, 0))
    small = pl.BlockSpec((block, LANES), lambda i: (i, 0))
    return pl.pallas_call(
        update_kernel,
        grid=(steps,),
        out_shape=jax.ShapeDtypeStruct(state_rows.shape, F32),
        in_specs=[rows] + [small] * 5,
        out_specs=rows,
        scratch_shapes=[VMEM((block * 8, LANES), F32), VMEM((block * 8, LANES), F32)],
        compiler_params=pltpu.CompilerParams(vmem_limit_bytes=8 << 20),
        cost_estimate=pl.CostEstimate(
            flops=2_000_000_000, bytes_accessed=8 << 20, transcendentals=0
        ),
        name="update_state",
    )(in_hbm(state_rows), removed, unit_rate, decay, key, value)


def stage_kernel(after_ref, gate_hbm, up_hbm, gate_ref, up_ref, sems):
    copies = [
        pltpu.make_async_copy(source, target, sems.at[place])
        for place, (source, target) in enumerate(
            ((gate_hbm, gate_ref), (up_hbm, up_ref))
        )
    ]
    for copy in copies:
        copy.start()
    for copy in copies:
        copy.wait()


def stage_weights(after, gate, up):
    weights = (gate, up)
    return pl.pallas_call(
        stage_kernel,
        out_shape=tuple(jax.ShapeDtypeStruct(w.shape, w.dtype) for w in weights),
        in_specs=[pl.BlockSpec(memory_space=pl.ANY)] * 3,
        out_specs=(pl.BlockSpec(memory_space=VMEM),) * 2,
        scratch_shapes=[pltpu.SemaphoreType.DMA((2,))],
        compiler_params=pltpu.CompilerParams(vmem_limit_bytes=1 << 20),
        name="stage_weights",
    )(after, *map(in_hbm, weights))


def dispatch_kernel(parts_ref, tokens_ref, pick_ref, resid_ref, out_ref):
    total = tokens_ref[...].astype(F32)
    mix = parts_ref[0].astype(F32)
    for z in range(1, parts_ref.shape[0]):
        mix = mix + parts_ref[z].astype(F32)
    resid = (total + mix).astype(BF16)
    resid_ref[...] = resid
    picked = jnp.dot(pick_ref[...], resid, preferred_element_type=F32).astype(BF16)
    for z in range(out_ref.shape[0]):
        out_ref[z] = picked


def dispatch_rows(parts, tokens, pick):
    return pl.pallas_call(
        dispatch_kernel,
        out_shape=(
            jax.ShapeDtypeStruct(tokens.shape, BF16),
            jax.ShapeDtypeStruct((parts.shape[0], pick.shape[0], LANES), BF16),
        ),
        compiler_params=pltpu.CompilerParams(vmem_limit_bytes=4 << 20),
        name="dispatch_rows",
    )(parts, tokens, pick)


def expert_kernel(
    own_ref,
    other_ref,
    gain_ref,
    gate_ref,
    up_ref,
    down_hbm,
    keep_ref,
    send_ref,
    x_ref,
    out_ref,
    down_ref,
    sem,
):
    down_copy = pltpu.make_async_copy(down_hbm, down_ref, sem)
    down_copy.start()
    core = lax.axis_index("tp_1")
    full_width = x_ref.shape[1]
    blocks = own_ref.shape[0]
    squares = jnp.zeros(own_ref.shape[1:], F32)
    for z in range(blocks):
        for part in (own_ref, other_ref):
            rows = part[z].astype(F32)
            squares = squares + rows * rows
    scale = lax.rsqrt(jnp.sum(squares, axis=1, keepdims=True) / full_width + RMS_EPS)
    for z in range(blocks):
        for part, place in ((own_ref, 2 * z + core), (other_ref, 2 * z + 1 - core)):
            cols = pl.ds(pl.multiple_of(place * LANES, LANES), LANES)
            x_ref[:, cols] = (part[z].astype(F32) * scale * gain_ref[:, cols]).astype(BF16)
    x = x_ref[...]
    across = (((1,), (1,)), ((), ()))
    gate_act = lax.dot_general(x, gate_ref[...], across, preferred_element_type=F32)
    upward = lax.dot_general(x, up_ref[...], across, preferred_element_type=F32)
    hidden = (jax.nn.silu(gate_act) * upward).astype(BF16)
    down_copy.wait()
    out_ref[...] = jnp.dot(hidden, down_ref[...], preferred_element_type=F32)
    for z in range(blocks):
        cols = pl.ds(pl.multiple_of((2 * z + core) * LANES, LANES), LANES)
        keep_ref[z] = out_ref[:, cols]
        cols = pl.ds(pl.multiple_of((2 * z + 1 - core) * LANES, LANES), LANES)
        send_ref[z] = out_ref[:, cols].astype(BF16)


def run_expert(own, other, gain, gate, up, down):
    rows = own.shape[1]
    full_width = gate.shape[1]
    vmem = pl.BlockSpec(memory_space=VMEM)
    return pl.pallas_call(
        expert_kernel,
        out_shape=(
            jax.ShapeDtypeStruct(own.shape, F32),
            jax.ShapeDtypeStruct(own.shape, BF16),
        ),
        in_specs=[vmem] * 5 + [pl.BlockSpec(memory_space=pl.ANY)],
        out_specs=(vmem, vmem),
        scratch_shapes=[
            VMEM((rows, full_width), BF16),
            VMEM((rows, full_width), F32),
            VMEM(down.shape, BF16),
            pltpu.SemaphoreType.DMA(()),
        ],
        compiler_params=pltpu.CompilerParams(vmem_limit_bytes=10 << 20),
        name="expert",
    )(own, other, gain, gate, up, in_hbm(down))


def combine_kernel(share_ref, rows_ref, resid_ref, out_ref):
    rows = rows_ref[0].astype(F32)
    for z in range(1, rows_ref.shape[0]):
        rows = rows + rows_ref[z].astype(F32)
    moe = lax.dot_general(
        share_ref[...],
        rows,
        (((0,), (0,)), ((), ())),
        precision=HIGHEST,
        preferred_element_type=F32,
    )
    out_ref[...] = (resid_ref[...].astype(F32) + moe).astype(BF16)


def combine_rows(share, rows, resid):
    return pl.pallas_call(
        combine_kernel,
        out_shape=jax.ShapeDtypeStruct(resid.shape, BF16),
        compiler_params=pltpu.CompilerParams(vmem_limit_bytes=4 << 20),
        name="combine",
    )(share, rows, resid)


def swap(shard):
    return lax.ppermute(shard, "tp_1", [(0, 1), (1, 0)])


def exchange(shard, axis):
    return lax.all_to_all(shard, axis, split_axis=0, concat_axis=0, tiled=True)


def exchange_rows(shard):
    groups = lax.axis_size("ep") * lax.axis_size("tp_0")
    chunks = shard.reshape(groups, -1, 4, LANES)
    return exchange(chunks, ("tp_0", "ep")).reshape(shard.shape)


def local(
    tokens,
    state,
    routes,
    route_logits,
    mix_gain,
    w_recept,
    w_key,
    w_value,
    w_decay,
    w_rate,
    decay_base,
    rate_base,
    key_gain,
    group_gain,
    w_output,
    ffn_gain,
    w_gate,
    w_up,
    w_down,
):
    seq_rows = tokens.shape[0]
    z_count = lax.axis_size("tp_0")
    group_count = lax.axis_size("ep")
    slot_rows = max(2, 3 * routes.shape[1] * seq_rows // (2 * group_count))
    slot_count = group_count * slot_rows

    state_rows = state.reshape(-1, HEAD)
    vectors, recept, unit_rate, decay, key, value, own_tokens, pick, share = project_heads(
        tokens,
        (w_recept, w_key, w_value, w_decay, w_rate),
        mix_gain.reshape(1, -1),
        [v.reshape(1, -1) for v in (decay_base, rate_base, key_gain)],
        routes.T,
        route_logits.T,
        slot_count,
    )
    keep, send, removed = mix(
        state_rows,
        vectors,
        recept,
        unit_rate,
        key,
        value,
        w_output,
        group_gain.reshape(1, -1),
        z_count,
    )
    pair_sum = (keep + swap(send).astype(F32)).astype(BF16)
    parts = exchange(pair_sum, "tp_0")
    new_state = update_state(state_rows, removed, unit_rate, decay, key, value)

    resid_own, outgoing = dispatch_rows(parts, own_tokens, pick)
    arrived = exchange_rows(outgoing)
    weights = stage_weights(
        arrived, jnp.swapaxes(w_gate[0], 0, 1), jnp.swapaxes(w_up[0], 0, 1)
    )
    gain = ffn_gain.reshape(1, -1)
    keep, send = run_expert(arrived, swap(arrived), gain, *weights, w_down[0])
    pair_sum = (keep + swap(send).astype(F32)).astype(BF16)
    output = combine_rows(share, exchange_rows(pair_sum), resid_own)
    return (output, new_state.reshape(state.shape))


def solution(mesh):
    torus = Mesh(mesh.devices.reshape(mesh.shape["ep"], 8, 2), ("ep", "tp_0", "tp_1"))
    return jax.shard_map(
        local,
        mesh=torus,
        in_specs=(
            P("ep", None),
            P("ep", TP, None, None),
            P("ep", None),
            P("ep", None),
            P(),
            P(None, TP),
            P(None, TP),
            P(None, TP),
            P(None, TP),
            P(None, TP),
            P(TP),
            P(TP),
            P(TP),
            P(TP),
            P(TP, None),
            P(),
            P("ep", None, TP),
            P("ep", None, TP),
            P("ep", TP, None),
        ),
        out_specs=(P("ep", TP), P("ep", TP, None, None)),
        check_vma=False,
    )
```

```python
import jax
import jax.numpy as jnp
from jax import lax
from jax.experimental import pallas as pl
from jax.experimental.pallas import tpu as pltpu
from jax.sharding import Mesh
from jax.sharding import PartitionSpec as P

TP = ("tp_0", "tp_1")

RMS_EPS = 1e-06
GROUP_EPS = 0.00064
UNIT_EPS = 6.4e-05
HIGHEST = lax.Precision.HIGHEST
F32 = jnp.float32
BF16 = jnp.bfloat16
VMEM = pltpu.VMEM
HEAD = 64
LANES = 128


def in_hbm(array):
    return pltpu.with_memory_space_constraint(array, pltpu.HBM)


def head_sums(values):
    rows = lax.broadcasted_iota(jnp.int32, (LANES, LANES), 0) // HEAD
    cols = lax.broadcasted_iota(jnp.int32, (LANES, LANES), 1) // HEAD
    ones = (rows == cols).astype(F32)
    return jnp.dot(values, ones, precision=HIGHEST, preferred_element_type=F32)


def route_slots(routes, logits, pick_ref, share_ref):
    slots, seqs = pick_ref.shape
    experts = lax.axis_size("ep")
    first, second = routes[0:1, :], routes[1:2, :]
    expert = lax.broadcasted_iota(jnp.int32, (experts, seqs), 0)
    named = [(expert == choice).astype(F32) for choice in (first, second)]
    earlier = lax.broadcasted_iota(jnp.int32, (seqs, seqs), 0) < lax.broadcasted_iota(
        jnp.int32, (seqs, seqs), 1
    )
    counts = jnp.dot(
        (named[0] + named[1]).astype(BF16),
        earlier.astype(F32).astype(BF16),
        preferred_element_type=F32,
    )
    exps = jnp.exp(logits)
    total = exps[0:1, :] + exps[1:2, :]
    slot = lax.broadcasted_iota(jnp.int32, (slots, seqs), 0)
    picked = jnp.zeros((slots, seqs), F32)
    shares = jnp.zeros((slots, seqs), F32)
    for k, choice in enumerate((first, second)):
        placed = jnp.sum(named[k] * counts, axis=0, keepdims=True).astype(jnp.int32)
        here = slot == choice * (slots // experts) + placed
        picked = jnp.where(here, 1.0, picked)
        shares = jnp.where(here, exps[k : k + 1, :] / total, shares)
    pick_ref[...] = picked.astype(BF16)
    share_ref[...] = shares


def project_kernel(
    tokens_hbm,
    w_recept_hbm,
    w_key_hbm,
    w_value_hbm,
    w_decay_hbm,
    w_rate_hbm,
    mix_gain_hbm,
    decay_base_hbm,
    rate_base_hbm,
    key_gain_hbm,
    routes_hbm,
    logits_hbm,
    vectors_ref,
    recept_ref,
    unit_rate_ref,
    decay_ref,
    key_ref,
    value_ref,
    own_ref,
    pick_ref,
    share_ref,
    tokens_ref,
    weights_ref,
    mix_gain_ref,
    decay_base_ref,
    rate_base_ref,
    key_gain_ref,
    routes_ref,
    logits_ref,
    sems,
    small_sems,
):
    seqs = tokens_ref.shape[0]
    copies = [pltpu.make_async_copy(tokens_hbm, tokens_ref, sems.at[0])]
    smalls = [
        pltpu.make_async_copy(source, target, small_sems.at[place])
        for place, (source, target) in enumerate(
            (
                (mix_gain_hbm, mix_gain_ref),
                (key_gain_hbm, key_gain_ref),
                (decay_base_hbm, decay_base_ref),
                (rate_base_hbm, rate_base_ref),
                (routes_hbm, routes_ref),
                (logits_hbm, logits_ref),
            )
        )
    ]
    sources = (w_key_hbm, w_value_hbm, w_recept_hbm, w_decay_hbm, w_rate_hbm)
    for place, source in enumerate(sources):
        target = weights_ref.at[:, pl.ds(place * LANES, LANES)]
        copies.append(pltpu.make_async_copy(source, target, sems.at[1 + place]))
    copies[0].start()
    for copy in smalls:
        copy.start()
    for copy in copies[1:]:
        copy.start()

    for copy in smalls:
        copy.wait()
    route_slots(routes_ref[...], logits_ref[...], pick_ref, share_ref)
    copies[0].wait()
    own_ref[...] = tokens_ref[:, pl.ds(pl.multiple_of(lax.axis_index(TP) * LANES, LANES), LANES)]
    values = tokens_ref[...].astype(F32)
    mean_square = jnp.mean(values * values, axis=1, keepdims=True)
    normed = (values * lax.rsqrt(mean_square + RMS_EPS) * mix_gain_ref[...]).astype(BF16)

    def project(first, count):
        for place in range(first, first + count):
            copies[1 + place].wait()
        weight = weights_ref[:, first * LANES : (first + count) * LANES]
        return jnp.dot(normed, weight, preferred_element_type=F32).astype(BF16).astype(F32)

    key_value = project(0, 2)
    keys_now = key_value[:, :LANES]
    key_ref[...] = keys_now
    value_ref[...] = key_value[:, LANES:]
    scaled = keys_now * key_gain_ref[...]
    unit_key = scaled * lax.rsqrt(head_sums(scaled * scaled) + UNIT_EPS)
    vectors_ref[...] = jnp.zeros_like(vectors_ref)
    vectors_ref[pl.ds(0, seqs, stride=8), :] = unit_key
    vectors_ref[pl.ds(2, seqs, stride=8), :] = pltpu.roll(unit_key, HEAD, 1)
    recept_decay = project(2, 2)
    recept = recept_decay[:, :LANES]
    recept_ref[...] = recept
    decay_pre = recept_decay[:, LANES:] + decay_base_ref[...]
    decay_now = jnp.exp(-jnp.exp(-jax.nn.softplus(-decay_pre) - 0.5))
    decay_ref[...] = decay_now
    decayed_recept = decay_now * recept
    vectors_ref[pl.ds(1, seqs, stride=8), :] = decayed_recept
    vectors_ref[pl.ds(3, seqs, stride=8), :] = pltpu.roll(decayed_recept, HEAD, 1)
    rate_pre = project(4, 1) + rate_base_ref[...]
    unit_rate_ref[...] = unit_key * jax.nn.sigmoid(rate_pre)


def project_heads(tokens, projections, mix_gain, vectors, routes, logits, slots):
    seqs, full_width = tokens.shape
    small = jax.ShapeDtypeStruct((seqs, LANES), F32)
    hbm = pl.BlockSpec(memory_space=pl.ANY)
    vmem = pl.BlockSpec(memory_space=VMEM)
    return pl.pallas_call(
        project_kernel,
        out_shape=(jax.ShapeDtypeStruct((seqs * 8, LANES), F32),)
        + (small,) * 5
        + (
            jax.ShapeDtypeStruct((seqs, LANES), BF16),
            jax.ShapeDtypeStruct((slots, seqs), BF16),
            jax.ShapeDtypeStruct((slots, seqs), F32),
        ),
        in_specs=[hbm] * 12,
        out_specs=(vmem,) * 9,
        scratch_shapes=[
            VMEM((seqs, full_width), BF16),
            VMEM((full_width, 5 * LANES), BF16),
            VMEM((1, full_width), F32),
            VMEM((1, LANES), F32),
            VMEM((1, LANES), F32),
            VMEM((1, LANES), F32),
            VMEM(routes.shape, jnp.int32),
            VMEM(logits.shape, F32),
            pltpu.SemaphoreType.DMA((6,)),
            pltpu.SemaphoreType.DMA((6,)),
        ],
        compiler_params=pltpu.CompilerParams(vmem_limit_bytes=12 << 20),
        cost_estimate=pl.CostEstimate(
            flops=3_000_000_000, bytes_accessed=6 << 20, transcendentals=0
        ),
        name="project_heads",
    )(*map(in_hbm, (tokens, *projections, mix_gain, *vectors, routes, logits)))


def mix_kernel(
    state_ref,
    vectors_ref,
    recept_ref,
    unit_rate_ref,
    key_ref,
    value_ref,
    w_output_ref,
    group_gain_ref,
    keep_ref,
    send_ref,
    removed_ref,
    products_ref,
):
    seqs = recept_ref.shape[0]
    for seq in range(seqs):
        left = vectors_ref[seq * 8 : seq * 8 + 8, :HEAD].astype(BF16)
        right = state_ref[seq * LANES : (seq + 1) * LANES, :].astype(BF16)
        products_ref[seq * 8 : seq * 8 + 8, :] = lax.dot_general(
            left, right, (((1,), (1,)), ((), ())), preferred_element_type=F32
        )
    first_head = lax.broadcasted_iota(jnp.int32, (seqs, LANES), 1) < HEAD
    removed = jnp.where(
        first_head,
        products_ref[pl.ds(0, seqs, stride=8), :],
        products_ref[pl.ds(2, seqs, stride=8), :],
    )
    faded = jnp.where(
        first_head,
        products_ref[pl.ds(1, seqs, stride=8), :],
        products_ref[pl.ds(3, seqs, stride=8), :],
    )
    removed_ref[...] = removed
    recept = recept_ref[...]
    readout = (
        faded
        - removed * head_sums(unit_rate_ref[...] * recept)
        + value_ref[...] * head_sums(key_ref[...] * recept)
    )
    centred = readout - head_sums(readout) * (1.0 / HEAD)
    spread = head_sums(centred * centred) * (1.0 / HEAD)
    mixed = (centred * lax.rsqrt(spread + GROUP_EPS) * group_gain_ref[...]).astype(BF16)
    core = lax.axis_index("tp_1")
    for z in range(keep_ref.shape[0]):
        own = w_output_ref[:, pl.ds(pl.multiple_of((2 * z + core) * LANES, LANES), LANES)]
        keep_ref[z] = jnp.dot(mixed, own, preferred_element_type=F32)
        other = w_output_ref[:, pl.ds(pl.multiple_of((2 * z + 1 - core) * LANES, LANES), LANES)]
        send_ref[z] = jnp.dot(mixed, other, preferred_element_type=F32).astype(BF16)


def mix(state_rows, vectors, recept, unit_rate, key, value, w_output, group_gain, z_count):
    seqs = recept.shape[0]
    vmem = pl.BlockSpec(memory_space=VMEM)
    return pl.pallas_call(
        mix_kernel,
        out_shape=(
            jax.ShapeDtypeStruct((z_count, seqs, LANES), F32),
            jax.ShapeDtypeStruct((z_count, seqs, LANES), BF16),
            jax.ShapeDtypeStruct((seqs, LANES), F32),
        ),
        in_specs=[vmem] * 8,
        out_specs=(vmem,) * 3,
        scratch_shapes=[VMEM((seqs * 8, LANES), F32)],
        compiler_params=pltpu.CompilerParams(vmem_limit_bytes=12 << 20),
        name="mix",
    )(state_rows, vectors, recept, unit_rate, key, value, w_output, group_gain)


def update_kernel(
    state_ref,
    removed_ref,
    unit_rate_ref,
    decay_ref,
    key_ref,
    value_ref,
    out_ref,
    left_ref,
    right_ref,
):
    block = removed_ref.shape[0]
    first_head = lax.broadcasted_iota(jnp.int32, (block, LANES), 1) < HEAD
    removed = -removed_ref[...]
    removed_high = removed.astype(BF16).astype(F32)
    removed_low = removed - removed_high
    unit_rate = unit_rate_ref[...]
    unit_high = unit_rate.astype(BF16).astype(F32)
    unit_low = unit_rate - unit_high
    key = key_ref[...]
    lefts = (removed_high, removed_low, removed_high, value_ref[...])
    rights = (unit_high, unit_high, unit_low, key)
    for place in range(4):
        left_ref[pl.ds(place, block, stride=8), :] = jnp.where(first_head, lefts[place], 0.0)
        left_ref[pl.ds(place + 4, block, stride=8), :] = jnp.where(first_head, 0.0, lefts[place])
        right_ref[pl.ds(place, block, stride=8), :] = rights[place]
        right_ref[pl.ds(place + 4, block, stride=8), :] = pltpu.roll(rights[place], HEAD, 1)
    decay = decay_ref[...]
    decay_rolled = pltpu.roll(decay, HEAD, 1)
    for seq in range(block):
        left = left_ref[seq * 8 : seq * 8 + 8, :].astype(BF16)
        right = right_ref[seq * 8 : seq * 8 + 8, :HEAD].astype(BF16)
        change = lax.dot_general(
            left, right, (((0,), (0,)), ((), ())), preferred_element_type=F32
        )
        base = seq * LANES
        old = state_ref[base : base + HEAD, :]
        out_ref[base : base + HEAD, :] = old * decay[seq : seq + 1, :HEAD] + change[:HEAD]
        old = state_ref[base + HEAD : base + LANES, :]
        out_ref[base + HEAD : base + LANES, :] = (
            old * decay_rolled[seq : seq + 1, :HEAD] + change[HEAD:]
        )


def update_state(state_rows, removed, unit_rate, decay, key, value):
    seqs = removed.shape[0]
    steps = 8
    block = seqs // steps
    rows = pl.BlockSpec((block * LANES, HEAD), lambda i: (i, 0))
    small = pl.BlockSpec((block, LANES), lambda i: (i, 0))
    return pl.pallas_call(
        update_kernel,
        grid=(steps,),
        out_shape=jax.ShapeDtypeStruct(state_rows.shape, F32),
        in_specs=[rows] + [small] * 5,
        out_specs=rows,
        scratch_shapes=[VMEM((block * 8, LANES), F32), VMEM((block * 8, LANES), F32)],
        compiler_params=pltpu.CompilerParams(vmem_limit_bytes=8 << 20),
        cost_estimate=pl.CostEstimate(
            flops=2_000_000_000, bytes_accessed=8 << 20, transcendentals=0
        ),
        name="update_state",
    )(in_hbm(state_rows), removed, unit_rate, decay, key, value)


def dispatch_kernel(parts_ref, tokens_ref, pick_ref, resid_ref, out_ref):
    total = tokens_ref[...].astype(F32)
    mix = parts_ref[0].astype(F32)
    for z in range(1, parts_ref.shape[0]):
        mix = mix + parts_ref[z].astype(F32)
    resid = (total + mix).astype(BF16)
    resid_ref[...] = resid
    picked = jnp.dot(pick_ref[...], resid, preferred_element_type=F32).astype(BF16)
    for z in range(out_ref.shape[0]):
        out_ref[z] = picked


def dispatch_rows(parts, tokens, pick):
    return pl.pallas_call(
        dispatch_kernel,
        out_shape=(
            jax.ShapeDtypeStruct(tokens.shape, BF16),
            jax.ShapeDtypeStruct((parts.shape[0], pick.shape[0], LANES), BF16),
        ),
        compiler_params=pltpu.CompilerParams(vmem_limit_bytes=4 << 20),
        name="dispatch_rows",
    )(parts, tokens, pick)


def expert_kernel(
    own_ref,
    other_ref,
    gain_ref,
    gate_ref,
    up_ref,
    down_ref,
    keep_ref,
    send_ref,
    x_ref,
    out_ref,
):
    core = lax.axis_index("tp_1")
    full_width = x_ref.shape[1]
    blocks = own_ref.shape[0]
    squares = jnp.zeros(own_ref.shape[1:], F32)
    for z in range(blocks):
        for part in (own_ref, other_ref):
            rows = part[z].astype(F32)
            squares = squares + rows * rows
    scale = lax.rsqrt(jnp.sum(squares, axis=1, keepdims=True) / full_width + RMS_EPS)
    for z in range(blocks):
        for part, place in ((own_ref, 2 * z + core), (other_ref, 2 * z + 1 - core)):
            cols = pl.ds(pl.multiple_of(place * LANES, LANES), LANES)
            x_ref[:, cols] = (part[z].astype(F32) * scale * gain_ref[:, cols]).astype(BF16)
    x = x_ref[...]
    across = (((1,), (1,)), ((), ()))
    gate_act = lax.dot_general(x, gate_ref[...], across, preferred_element_type=F32)
    upward = lax.dot_general(x, up_ref[...], across, preferred_element_type=F32)
    hidden = (jax.nn.silu(gate_act) * upward).astype(BF16)
    out_ref[...] = jnp.dot(hidden, down_ref[...], preferred_element_type=F32)
    for z in range(blocks):
        cols = pl.ds(pl.multiple_of((2 * z + core) * LANES, LANES), LANES)
        keep_ref[z] = out_ref[:, cols]
        cols = pl.ds(pl.multiple_of((2 * z + 1 - core) * LANES, LANES), LANES)
        send_ref[z] = out_ref[:, cols].astype(BF16)


def run_expert(own, other, gain, gate, up, down):
    rows = own.shape[1]
    full_width = gate.shape[1]
    vmem = pl.BlockSpec(memory_space=VMEM)
    return pl.pallas_call(
        expert_kernel,
        out_shape=(
            jax.ShapeDtypeStruct(own.shape, F32),
            jax.ShapeDtypeStruct(own.shape, BF16),
        ),
        in_specs=[vmem] * 6,
        out_specs=(vmem, vmem),
        scratch_shapes=[VMEM((rows, full_width), BF16), VMEM((rows, full_width), F32)],
        compiler_params=pltpu.CompilerParams(vmem_limit_bytes=10 << 20),
        name="expert",
    )(own, other, gain, gate, up, down)


def combine_kernel(share_ref, rows_ref, resid_ref, out_ref):
    rows = rows_ref[0].astype(F32)
    for z in range(1, rows_ref.shape[0]):
        rows = rows + rows_ref[z].astype(F32)
    moe = lax.dot_general(
        share_ref[...],
        rows,
        (((0,), (0,)), ((), ())),
        precision=HIGHEST,
        preferred_element_type=F32,
    )
    out_ref[...] = (resid_ref[...].astype(F32) + moe).astype(BF16)


def combine_rows(share, rows, resid):
    return pl.pallas_call(
        combine_kernel,
        out_shape=jax.ShapeDtypeStruct(resid.shape, BF16),
        compiler_params=pltpu.CompilerParams(vmem_limit_bytes=4 << 20),
        name="combine",
    )(share, rows, resid)


def swap(shard):
    return lax.ppermute(shard, "tp_1", [(0, 1), (1, 0)])


def exchange(shard, axis):
    return lax.all_to_all(shard, axis, split_axis=0, concat_axis=0, tiled=True)


def exchange_rows(shard):
    groups = lax.axis_size("ep") * lax.axis_size("tp_0")
    chunks = shard.reshape(groups, -1, 4, LANES)
    return exchange(chunks, ("tp_0", "ep")).reshape(shard.shape)


def local(
    tokens,
    state,
    routes,
    route_logits,
    mix_gain,
    w_recept,
    w_key,
    w_value,
    w_decay,
    w_rate,
    decay_base,
    rate_base,
    key_gain,
    group_gain,
    w_output,
    ffn_gain,
    w_gate,
    w_up,
    w_down,
):
    seq_rows = tokens.shape[0]
    z_count = lax.axis_size("tp_0")
    group_count = lax.axis_size("ep")
    slot_rows = max(2, 3 * routes.shape[1] * seq_rows // (2 * group_count))
    slot_count = group_count * slot_rows

    state_rows = state.reshape(-1, HEAD)
    vectors, recept, unit_rate, decay, key, value, own_tokens, pick, share = project_heads(
        tokens,
        (w_recept, w_key, w_value, w_decay, w_rate),
        mix_gain.reshape(1, -1),
        [v.reshape(1, -1) for v in (decay_base, rate_base, key_gain)],
        routes.T,
        route_logits.T,
        slot_count,
    )
    keep, send, removed = mix(
        state_rows,
        vectors,
        recept,
        unit_rate,
        key,
        value,
        w_output,
        group_gain.reshape(1, -1),
        z_count,
    )
    pair_sum = (keep + swap(send).astype(F32)).astype(BF16)
    parts = exchange(pair_sum, "tp_0")
    new_state = update_state(state_rows, removed, unit_rate, decay, key, value)

    resid_own, outgoing = dispatch_rows(parts, own_tokens, pick)
    arrived = exchange_rows(outgoing)
    gain = ffn_gain.reshape(1, -1)
    keep, send = run_expert(
        arrived,
        swap(arrived),
        gain,
        jnp.swapaxes(w_gate[0], 0, 1),
        jnp.swapaxes(w_up[0], 0, 1),
        w_down[0],
    )
    pair_sum = (keep + swap(send).astype(F32)).astype(BF16)
    output = combine_rows(share, exchange_rows(pair_sum), resid_own)
    return (output, new_state.reshape(state.shape))


def solution(mesh):
    torus = Mesh(mesh.devices.reshape(mesh.shape["ep"], 8, 2), ("ep", "tp_0", "tp_1"))
    return jax.shard_map(
        local,
        mesh=torus,
        in_specs=(
            P("ep", None),
            P("ep", TP, None, None),
            P("ep", None),
            P("ep", None),
            P(),
            P(None, TP),
            P(None, TP),
            P(None, TP),
            P(None, TP),
            P(None, TP),
            P(TP),
            P(TP),
            P(TP),
            P(TP),
            P(TP, None),
            P(),
            P("ep", None, TP),
            P("ep", None, TP),
            P("ep", TP, None),
        ),
        out_specs=(P("ep", TP), P("ep", TP, None, None)),
        check_vma=False,
    )
```

```python
import jax
import jax.numpy as jnp
from jax import lax
from jax.experimental import pallas as pl
from jax.experimental.pallas import tpu as pltpu
from jax.sharding import Mesh
from jax.sharding import PartitionSpec as P

TP = ("tp_0", "tp_1")

RMS_EPS = 1e-06
GROUP_EPS = 0.00064
UNIT_EPS = 6.4e-05
HIGHEST = lax.Precision.HIGHEST
F32 = jnp.float32
BF16 = jnp.bfloat16
VMEM = pltpu.VMEM
HEAD = 64
LANES = 128


def in_hbm(array):
    return pltpu.with_memory_space_constraint(array, pltpu.HBM)


def head_sums(values):
    rows = lax.broadcasted_iota(jnp.int32, (LANES, LANES), 0) // HEAD
    cols = lax.broadcasted_iota(jnp.int32, (LANES, LANES), 1) // HEAD
    ones = (rows == cols).astype(F32)
    return jnp.dot(values, ones, precision=HIGHEST, preferred_element_type=F32)


def route_slots(routes, logits, pick_ref, share_ref):
    slots, seqs = pick_ref.shape
    experts = lax.axis_size("ep")
    first, second = routes[0:1, :], routes[1:2, :]
    expert = lax.broadcasted_iota(jnp.int32, (experts, seqs), 0)
    named = [(expert == choice).astype(F32) for choice in (first, second)]
    earlier = lax.broadcasted_iota(jnp.int32, (seqs, seqs), 0) < lax.broadcasted_iota(
        jnp.int32, (seqs, seqs), 1
    )
    counts = jnp.dot(
        (named[0] + named[1]).astype(BF16),
        earlier.astype(F32).astype(BF16),
        preferred_element_type=F32,
    )
    exps = jnp.exp(logits)
    total = exps[0:1, :] + exps[1:2, :]
    slot = lax.broadcasted_iota(jnp.int32, (slots, seqs), 0)
    picked = jnp.zeros((slots, seqs), F32)
    shares = jnp.zeros((slots, seqs), F32)
    for k, choice in enumerate((first, second)):
        placed = jnp.sum(named[k] * counts, axis=0, keepdims=True).astype(jnp.int32)
        here = slot == choice * (slots // experts) + placed
        picked = jnp.where(here, 1.0, picked)
        shares = jnp.where(here, exps[k : k + 1, :] / total, shares)
    pick_ref[...] = picked.astype(BF16)
    share_ref[...] = shares


def project_kernel(
    tokens_hbm,
    w_recept_hbm,
    w_key_hbm,
    w_value_hbm,
    w_decay_hbm,
    w_rate_hbm,
    mix_gain_hbm,
    decay_base_hbm,
    rate_base_hbm,
    key_gain_hbm,
    routes_hbm,
    logits_hbm,
    vectors_ref,
    recept_ref,
    unit_rate_ref,
    decay_ref,
    key_ref,
    value_ref,
    own_ref,
    pick_ref,
    share_ref,
    tokens_ref,
    weights_ref,
    mix_gain_ref,
    decay_base_ref,
    rate_base_ref,
    key_gain_ref,
    routes_ref,
    logits_ref,
    sems,
    small_sems,
):
    seqs = tokens_ref.shape[0]
    copies = [pltpu.make_async_copy(tokens_hbm, tokens_ref, sems.at[0])]
    smalls = [
        pltpu.make_async_copy(source, target, small_sems.at[place])
        for place, (source, target) in enumerate(
            (
                (mix_gain_hbm, mix_gain_ref),
                (key_gain_hbm, key_gain_ref),
                (decay_base_hbm, decay_base_ref),
                (rate_base_hbm, rate_base_ref),
                (routes_hbm, routes_ref),
                (logits_hbm, logits_ref),
            )
        )
    ]
    sources = (w_key_hbm, w_value_hbm, w_recept_hbm, w_decay_hbm, w_rate_hbm)
    for place, source in enumerate(sources):
        target = weights_ref.at[:, pl.ds(place * LANES, LANES)]
        copies.append(pltpu.make_async_copy(source, target, sems.at[1 + place]))
    copies[0].start()
    for copy in smalls:
        copy.start()
    for copy in copies[1:]:
        copy.start()

    for copy in smalls:
        copy.wait()
    route_slots(routes_ref[...], logits_ref[...], pick_ref, share_ref)
    copies[0].wait()
    own_ref[...] = tokens_ref[:, pl.ds(pl.multiple_of(lax.axis_index(TP) * LANES, LANES), LANES)]
    values = tokens_ref[...].astype(F32)
    mean_square = jnp.mean(values * values, axis=1, keepdims=True)
    normed = (values * lax.rsqrt(mean_square + RMS_EPS) * mix_gain_ref[...]).astype(BF16)

    def project(first, count):
        for place in range(first, first + count):
            copies[1 + place].wait()
        weight = weights_ref[:, first * LANES : (first + count) * LANES]
        return jnp.dot(normed, weight, preferred_element_type=F32).astype(BF16).astype(F32)

    key_value = project(0, 2)
    keys_now = key_value[:, :LANES]
    key_ref[...] = keys_now
    value_ref[...] = key_value[:, LANES:]
    scaled = keys_now * key_gain_ref[...]
    unit_key = scaled * lax.rsqrt(head_sums(scaled * scaled) + UNIT_EPS)
    vectors_ref[...] = jnp.zeros_like(vectors_ref)
    vectors_ref[pl.ds(0, seqs, stride=8), :] = unit_key
    vectors_ref[pl.ds(2, seqs, stride=8), :] = pltpu.roll(unit_key, HEAD, 1)
    recept_decay = project(2, 2)
    recept = recept_decay[:, :LANES]
    recept_ref[...] = recept
    decay_pre = recept_decay[:, LANES:] + decay_base_ref[...]
    decay_now = jnp.exp(-jnp.exp(-jax.nn.softplus(-decay_pre) - 0.5))
    decay_ref[...] = decay_now
    decayed_recept = decay_now * recept
    vectors_ref[pl.ds(1, seqs, stride=8), :] = decayed_recept
    vectors_ref[pl.ds(3, seqs, stride=8), :] = pltpu.roll(decayed_recept, HEAD, 1)
    rate_pre = project(4, 1) + rate_base_ref[...]
    unit_rate_ref[...] = unit_key * jax.nn.sigmoid(rate_pre)


def project_heads(tokens, projections, mix_gain, vectors, routes, logits, slots):
    seqs, full_width = tokens.shape
    small = jax.ShapeDtypeStruct((seqs, LANES), F32)
    hbm = pl.BlockSpec(memory_space=pl.ANY)
    vmem = pl.BlockSpec(memory_space=VMEM)
    return pl.pallas_call(
        project_kernel,
        out_shape=(jax.ShapeDtypeStruct((seqs * 8, LANES), F32),)
        + (small,) * 5
        + (
            jax.ShapeDtypeStruct((seqs, LANES), BF16),
            jax.ShapeDtypeStruct((slots, seqs), BF16),
            jax.ShapeDtypeStruct((slots, seqs), F32),
        ),
        in_specs=[hbm] * 12,
        out_specs=(vmem,) * 9,
        scratch_shapes=[
            VMEM((seqs, full_width), BF16),
            VMEM((full_width, 5 * LANES), BF16),
            VMEM((1, full_width), F32),
            VMEM((1, LANES), F32),
            VMEM((1, LANES), F32),
            VMEM((1, LANES), F32),
            VMEM(routes.shape, jnp.int32),
            VMEM(logits.shape, F32),
            pltpu.SemaphoreType.DMA((6,)),
            pltpu.SemaphoreType.DMA((6,)),
        ],
        compiler_params=pltpu.CompilerParams(vmem_limit_bytes=12 << 20),
        cost_estimate=pl.CostEstimate(
            flops=3_000_000_000, bytes_accessed=6 << 20, transcendentals=0
        ),
        name="project_heads",
    )(*map(in_hbm, (tokens, *projections, mix_gain, *vectors, routes, logits)))


def mix_kernel(
    state_ref,
    vectors_ref,
    recept_ref,
    unit_rate_ref,
    key_ref,
    value_ref,
    w_output_ref,
    group_gain_ref,
    keep_ref,
    send_ref,
    removed_ref,
    products_ref,
):
    seqs = recept_ref.shape[0]
    for seq in range(seqs):
        left = vectors_ref[seq * 8 : seq * 8 + 8, :HEAD].astype(BF16)
        right = state_ref[seq * LANES : (seq + 1) * LANES, :].astype(BF16)
        products_ref[seq * 8 : seq * 8 + 8, :] = lax.dot_general(
            left, right, (((1,), (1,)), ((), ())), preferred_element_type=F32
        )
    first_head = lax.broadcasted_iota(jnp.int32, (seqs, LANES), 1) < HEAD
    removed = jnp.where(
        first_head,
        products_ref[pl.ds(0, seqs, stride=8), :],
        products_ref[pl.ds(2, seqs, stride=8), :],
    )
    faded = jnp.where(
        first_head,
        products_ref[pl.ds(1, seqs, stride=8), :],
        products_ref[pl.ds(3, seqs, stride=8), :],
    )
    removed_ref[...] = removed
    recept = recept_ref[...]
    readout = (
        faded
        - removed * head_sums(unit_rate_ref[...] * recept)
        + value_ref[...] * head_sums(key_ref[...] * recept)
    )
    centred = readout - head_sums(readout) * (1.0 / HEAD)
    spread = head_sums(centred * centred) * (1.0 / HEAD)
    mixed = (centred * lax.rsqrt(spread + GROUP_EPS) * group_gain_ref[...]).astype(BF16)
    core = lax.axis_index("tp_1")
    for z in range(keep_ref.shape[0]):
        own = w_output_ref[:, pl.ds(pl.multiple_of((2 * z + core) * LANES, LANES), LANES)]
        keep_ref[z] = jnp.dot(mixed, own, preferred_element_type=F32)
        other = w_output_ref[:, pl.ds(pl.multiple_of((2 * z + 1 - core) * LANES, LANES), LANES)]
        send_ref[z] = jnp.dot(mixed, other, preferred_element_type=F32).astype(BF16)


def mix(state_rows, vectors, recept, unit_rate, key, value, w_output, group_gain, z_count):
    seqs = recept.shape[0]
    vmem = pl.BlockSpec(memory_space=VMEM)
    return pl.pallas_call(
        mix_kernel,
        out_shape=(
            jax.ShapeDtypeStruct((z_count, seqs, LANES), F32),
            jax.ShapeDtypeStruct((z_count, seqs, LANES), BF16),
            jax.ShapeDtypeStruct((seqs, LANES), F32),
        ),
        in_specs=[vmem] * 8,
        out_specs=(vmem,) * 3,
        scratch_shapes=[VMEM((seqs * 8, LANES), F32)],
        compiler_params=pltpu.CompilerParams(vmem_limit_bytes=12 << 20),
        name="mix",
    )(state_rows, vectors, recept, unit_rate, key, value, w_output, group_gain)


def update_kernel(
    state_ref,
    removed_ref,
    unit_rate_ref,
    decay_ref,
    key_ref,
    value_ref,
    out_ref,
    left_ref,
    right_ref,
):
    block = removed_ref.shape[0]
    first_head = lax.broadcasted_iota(jnp.int32, (block, LANES), 1) < HEAD
    removed = -removed_ref[...]
    removed_high = removed.astype(BF16).astype(F32)
    removed_low = removed - removed_high
    unit_rate = unit_rate_ref[...]
    unit_high = unit_rate.astype(BF16).astype(F32)
    unit_low = unit_rate - unit_high
    key = key_ref[...]
    lefts = (removed_high, removed_low, removed_high, value_ref[...])
    rights = (unit_high, unit_high, unit_low, key)
    for place in range(4):
        left_ref[pl.ds(place, block, stride=8), :] = jnp.where(first_head, lefts[place], 0.0)
        left_ref[pl.ds(place + 4, block, stride=8), :] = jnp.where(first_head, 0.0, lefts[place])
        right_ref[pl.ds(place, block, stride=8), :] = rights[place]
        right_ref[pl.ds(place + 4, block, stride=8), :] = pltpu.roll(rights[place], HEAD, 1)
    decay = decay_ref[...]
    decay_rolled = pltpu.roll(decay, HEAD, 1)
    for seq in range(block):
        left = left_ref[seq * 8 : seq * 8 + 8, :].astype(BF16)
        right = right_ref[seq * 8 : seq * 8 + 8, :HEAD].astype(BF16)
        change = lax.dot_general(
            left, right, (((0,), (0,)), ((), ())), preferred_element_type=F32
        )
        base = seq * LANES
        old = state_ref[base : base + HEAD, :]
        out_ref[base : base + HEAD, :] = old * decay[seq : seq + 1, :HEAD] + change[:HEAD]
        old = state_ref[base + HEAD : base + LANES, :]
        out_ref[base + HEAD : base + LANES, :] = (
            old * decay_rolled[seq : seq + 1, :HEAD] + change[HEAD:]
        )


def update_state(state_rows, removed, unit_rate, decay, key, value):
    seqs = removed.shape[0]
    steps = 8
    block = seqs // steps
    rows = pl.BlockSpec((block * LANES, HEAD), lambda i: (i, 0))
    small = pl.BlockSpec((block, LANES), lambda i: (i, 0))
    return pl.pallas_call(
        update_kernel,
        grid=(steps,),
        out_shape=jax.ShapeDtypeStruct(state_rows.shape, F32),
        in_specs=[rows] + [small] * 5,
        out_specs=rows,
        scratch_shapes=[VMEM((block * 8, LANES), F32), VMEM((block * 8, LANES), F32)],
        compiler_params=pltpu.CompilerParams(vmem_limit_bytes=8 << 20),
        cost_estimate=pl.CostEstimate(
            flops=2_000_000_000, bytes_accessed=8 << 20, transcendentals=0
        ),
        name="update_state",
    )(in_hbm(state_rows), removed, unit_rate, decay, key, value)


def dispatch_kernel(parts_ref, tokens_ref, pick_ref, resid_ref, out_ref):
    total = tokens_ref[...].astype(F32)
    mix = parts_ref[0].astype(F32)
    for z in range(1, parts_ref.shape[0]):
        mix = mix + parts_ref[z].astype(F32)
    resid = (total + mix).astype(BF16)
    resid_ref[...] = resid
    picked = jnp.dot(pick_ref[...], resid, preferred_element_type=F32).astype(BF16)
    for z in range(out_ref.shape[0]):
        out_ref[z] = picked


def dispatch_rows(parts, tokens, pick):
    return pl.pallas_call(
        dispatch_kernel,
        out_shape=(
            jax.ShapeDtypeStruct(tokens.shape, BF16),
            jax.ShapeDtypeStruct((parts.shape[0], pick.shape[0], LANES), BF16),
        ),
        compiler_params=pltpu.CompilerParams(vmem_limit_bytes=4 << 20),
        name="dispatch_rows",
    )(parts, tokens, pick)


ACROSS = (((1,), (1,)), ((), ()))


def core_columns(ref, core):
    blocks = ref.shape[1] // (2 * LANES)
    return jnp.concatenate(
        [
            ref[:, pl.ds(pl.multiple_of((2 * z + core) * LANES, LANES), LANES)]
            for z in range(blocks)
        ],
        axis=1,
    )


def half_products(rows_ref, gain_ref, gate_ref, up_ref, core):
    gain = core_columns(gain_ref, core)
    squares = jnp.zeros(rows_ref.shape[1:], F32)
    parts = []
    for z in range(rows_ref.shape[0]):
        rows = rows_ref[z].astype(F32)
        squares = squares + rows * rows
        parts.append((rows * gain[:, z * LANES : (z + 1) * LANES]).astype(BF16))
    x = jnp.concatenate(parts, axis=1)
    gate = lax.dot_general(
        x, core_columns(gate_ref, core), ACROSS, preferred_element_type=F32
    )
    upward = lax.dot_general(
        x, core_columns(up_ref, core), ACROSS, preferred_element_type=F32
    )
    return squares, gate, upward


def own_half_kernel(rows_ref, gain_ref, gate_ref, up_ref, squares_ref, gate_out, up_out):
    core = lax.axis_index("tp_1")
    squares_ref[...], gate_out[...], up_out[...] = half_products(
        rows_ref, gain_ref, gate_ref, up_ref, core
    )


def other_half_kernel(
    rows_ref,
    gain_ref,
    gate_ref,
    up_ref,
    down_ref,
    squares_ref,
    gate_part_ref,
    up_part_ref,
    hidden_ref,
    send_ref,
):
    other = 1 - lax.axis_index("tp_1")
    squares, gate, upward = half_products(rows_ref, gain_ref, gate_ref, up_ref, other)
    square_sum = jnp.sum(squares + squares_ref[...], axis=1, keepdims=True)
    scale = lax.rsqrt(square_sum / gate_ref.shape[1] + RMS_EPS)
    gate = (gate + gate_part_ref[...]) * scale
    upward = (upward + up_part_ref[...]) * scale
    hidden = (jax.nn.silu(gate) * upward).astype(BF16)
    hidden_ref[...] = hidden
    out = jnp.dot(hidden, core_columns(down_ref, other), preferred_element_type=F32)
    for z in range(send_ref.shape[0]):
        send_ref[z] = out[:, z * LANES : (z + 1) * LANES].astype(BF16)


def keep_kernel(hidden_ref, down_ref, keep_ref):
    core = lax.axis_index("tp_1")
    out = jnp.dot(hidden_ref[...], core_columns(down_ref, core), preferred_element_type=F32)
    for z in range(keep_ref.shape[0]):
        keep_ref[z] = out[:, z * LANES : (z + 1) * LANES]


def run_expert(own, gain, gate, up, down):
    rows = own.shape[1]
    vmem = pl.BlockSpec(memory_space=VMEM)
    part = jax.ShapeDtypeStruct((rows, gate.shape[0]), F32)

    def call(body, name, *operands, out_shape):
        return pl.pallas_call(
            body,
            out_shape=out_shape,
            in_specs=[vmem] * len(operands),
            out_specs=jax.tree.map(lambda _: vmem, out_shape),
            compiler_params=pltpu.CompilerParams(vmem_limit_bytes=10 << 20),
            name=name,
        )(*operands)

    other = swap(own)
    partial = call(
        own_half_kernel,
        "own_half",
        own,
        gain,
        gate,
        up,
        out_shape=(jax.ShapeDtypeStruct((rows, LANES), F32), part, part),
    )
    other, partial = lax.optimization_barrier((other, partial))
    hidden, send = call(
        other_half_kernel,
        "other_half",
        other,
        gain,
        gate,
        up,
        down,
        *partial,
        out_shape=(
            jax.ShapeDtypeStruct((rows, gate.shape[0]), BF16),
            jax.ShapeDtypeStruct(own.shape, BF16),
        ),
    )
    received = swap(send)
    keep = call(
        keep_kernel, "keep_half", hidden, down, out_shape=jax.ShapeDtypeStruct(own.shape, F32)
    )
    return (keep + received.astype(F32)).astype(BF16)


def combine_kernel(share_ref, rows_ref, resid_ref, out_ref):
    rows = rows_ref[0].astype(F32)
    for z in range(1, rows_ref.shape[0]):
        rows = rows + rows_ref[z].astype(F32)
    moe = lax.dot_general(
        share_ref[...],
        rows,
        (((0,), (0,)), ((), ())),
        precision=HIGHEST,
        preferred_element_type=F32,
    )
    out_ref[...] = (resid_ref[...].astype(F32) + moe).astype(BF16)


def combine_rows(share, rows, resid):
    return pl.pallas_call(
        combine_kernel,
        out_shape=jax.ShapeDtypeStruct(resid.shape, BF16),
        compiler_params=pltpu.CompilerParams(vmem_limit_bytes=4 << 20),
        name="combine",
    )(share, rows, resid)


def swap(shard):
    return lax.ppermute(shard, "tp_1", [(0, 1), (1, 0)])


def exchange(shard, axis):
    return lax.all_to_all(shard, axis, split_axis=0, concat_axis=0, tiled=True)


def exchange_rows(shard):
    groups = lax.axis_size("ep") * lax.axis_size("tp_0")
    chunks = shard.reshape(groups, -1, 4, LANES)
    return exchange(chunks, ("tp_0", "ep")).reshape(shard.shape)


def local(
    tokens,
    state,
    routes,
    route_logits,
    mix_gain,
    w_recept,
    w_key,
    w_value,
    w_decay,
    w_rate,
    decay_base,
    rate_base,
    key_gain,
    group_gain,
    w_output,
    ffn_gain,
    w_gate,
    w_up,
    w_down,
):
    seq_rows = tokens.shape[0]
    z_count = lax.axis_size("tp_0")
    group_count = lax.axis_size("ep")
    slot_rows = max(2, 3 * routes.shape[1] * seq_rows // (2 * group_count))
    slot_count = group_count * slot_rows

    state_rows = state.reshape(-1, HEAD)
    vectors, recept, unit_rate, decay, key, value, own_tokens, pick, share = project_heads(
        tokens,
        (w_recept, w_key, w_value, w_decay, w_rate),
        mix_gain.reshape(1, -1),
        [v.reshape(1, -1) for v in (decay_base, rate_base, key_gain)],
        routes.T,
        route_logits.T,
        slot_count,
    )
    keep, send, removed = mix(
        state_rows,
        vectors,
        recept,
        unit_rate,
        key,
        value,
        w_output,
        group_gain.reshape(1, -1),
        z_count,
    )
    pair_sum = (keep + swap(send).astype(F32)).astype(BF16)
    parts = exchange(pair_sum, "tp_0")
    new_state = update_state(state_rows, removed, unit_rate, decay, key, value)

    resid_own, outgoing = dispatch_rows(parts, own_tokens, pick)
    arrived = exchange_rows(outgoing)
    gain = ffn_gain.reshape(1, -1)
    pair_sum = run_expert(
        arrived,
        gain,
        jnp.swapaxes(w_gate[0], 0, 1),
        jnp.swapaxes(w_up[0], 0, 1),
        w_down[0],
    )
    output = combine_rows(share, exchange_rows(pair_sum), resid_own)
    return (output, new_state.reshape(state.shape))


def solution(mesh):
    torus = Mesh(mesh.devices.reshape(mesh.shape["ep"], 8, 2), ("ep", "tp_0", "tp_1"))
    return jax.shard_map(
        local,
        mesh=torus,
        in_specs=(
            P("ep", None),
            P("ep", TP, None, None),
            P("ep", None),
            P("ep", None),
            P(),
            P(None, TP),
            P(None, TP),
            P(None, TP),
            P(None, TP),
            P(None, TP),
            P(TP),
            P(TP),
            P(TP),
            P(TP),
            P(TP, None),
            P(),
            P("ep", None, TP),
            P("ep", None, TP),
            P("ep", TP, None),
        ),
        out_specs=(P("ep", TP), P("ep", TP, None, None)),
        check_vma=False,
    )
```

```python
import jax
import jax.numpy as jnp
from jax import lax
from jax.experimental import pallas as pl
from jax.experimental.pallas import tpu as pltpu
from jax.sharding import Mesh
from jax.sharding import PartitionSpec as P

TP = ("tp_0", "tp_1")

RMS_EPS = 1e-06
GROUP_EPS = 0.00064
UNIT_EPS = 6.4e-05
HIGHEST = lax.Precision.HIGHEST
F32 = jnp.float32
BF16 = jnp.bfloat16
VMEM = pltpu.VMEM
HEAD = 64
LANES = 128
FIRST_Z = 5
FIRST_EP = 10


def z_order(count):
    return [(FIRST_Z + step) % count for step in range(count)]


def ep_order(count):
    return [(FIRST_EP + step) % count for step in range(count)]


def in_hbm(array):
    return pltpu.with_memory_space_constraint(array, pltpu.HBM)


def head_sums(values):
    rows = lax.broadcasted_iota(jnp.int32, (LANES, LANES), 0) // HEAD
    cols = lax.broadcasted_iota(jnp.int32, (LANES, LANES), 1) // HEAD
    ones = (rows == cols).astype(F32)
    return jnp.dot(values, ones, precision=HIGHEST, preferred_element_type=F32)


def route_slots(routes, logits, pick_ref, share_ref):
    slots, seqs = pick_ref.shape
    experts = lax.axis_size("ep")
    first, second = routes[0:1, :], routes[1:2, :]
    expert = lax.broadcasted_iota(jnp.int32, (experts, seqs), 0)
    named = [(expert == choice).astype(F32) for choice in (first, second)]
    earlier = lax.broadcasted_iota(jnp.int32, (seqs, seqs), 0) < lax.broadcasted_iota(
        jnp.int32, (seqs, seqs), 1
    )
    counts = jnp.dot(
        (named[0] + named[1]).astype(BF16),
        earlier.astype(F32).astype(BF16),
        preferred_element_type=F32,
    )
    exps = jnp.exp(logits)
    total = exps[0:1, :] + exps[1:2, :]
    slot = lax.broadcasted_iota(jnp.int32, (slots, seqs), 0)
    picked = jnp.zeros((slots, seqs), F32)
    shares = jnp.zeros((slots, seqs), F32)
    for k, choice in enumerate((first, second)):
        placed = jnp.sum(named[k] * counts, axis=0, keepdims=True).astype(jnp.int32)
        chunk = lax.rem(choice + (experts - FIRST_EP), experts)
        here = slot == chunk * (slots // experts) + placed
        picked = jnp.where(here, 1.0, picked)
        shares = jnp.where(here, exps[k : k + 1, :] / total, shares)
    pick_ref[...] = picked.astype(BF16)
    share_ref[...] = shares


def project_kernel(
    tokens_hbm,
    w_recept_hbm,
    w_key_hbm,
    w_value_hbm,
    w_decay_hbm,
    w_rate_hbm,
    mix_gain_hbm,
    decay_base_hbm,
    rate_base_hbm,
    key_gain_hbm,
    routes_hbm,
    logits_hbm,
    vectors_ref,
    recept_ref,
    unit_rate_ref,
    decay_ref,
    key_ref,
    value_ref,
    own_ref,
    pick_ref,
    share_ref,
    tokens_ref,
    weights_ref,
    mix_gain_ref,
    decay_base_ref,
    rate_base_ref,
    key_gain_ref,
    routes_ref,
    logits_ref,
    sems,
    small_sems,
):
    seqs = tokens_ref.shape[0]
    copies = [pltpu.make_async_copy(tokens_hbm, tokens_ref, sems.at[0])]
    smalls = [
        pltpu.make_async_copy(source, target, small_sems.at[place])
        for place, (source, target) in enumerate(
            (
                (mix_gain_hbm, mix_gain_ref),
                (key_gain_hbm, key_gain_ref),
                (decay_base_hbm, decay_base_ref),
                (rate_base_hbm, rate_base_ref),
                (routes_hbm, routes_ref),
                (logits_hbm, logits_ref),
            )
        )
    ]
    sources = (w_key_hbm, w_value_hbm, w_recept_hbm, w_decay_hbm, w_rate_hbm)
    for place, source in enumerate(sources):
        target = weights_ref.at[:, pl.ds(place * LANES, LANES)]
        copies.append(pltpu.make_async_copy(source, target, sems.at[1 + place]))
    copies[0].start()
    for copy in smalls:
        copy.start()
    for copy in copies[1:]:
        copy.start()

    for copy in smalls:
        copy.wait()
    route_slots(routes_ref[...], logits_ref[...], pick_ref, share_ref)
    copies[0].wait()
    own_ref[...] = tokens_ref[:, pl.ds(pl.multiple_of(lax.axis_index(TP) * LANES, LANES), LANES)]
    values = tokens_ref[...].astype(F32)
    mean_square = jnp.mean(values * values, axis=1, keepdims=True)
    normed = (values * lax.rsqrt(mean_square + RMS_EPS) * mix_gain_ref[...]).astype(BF16)

    def project(first, count):
        for place in range(first, first + count):
            copies[1 + place].wait()
        weight = weights_ref[:, first * LANES : (first + count) * LANES]
        return jnp.dot(normed, weight, preferred_element_type=F32).astype(BF16).astype(F32)

    key_value = project(0, 2)
    keys_now = key_value[:, :LANES]
    key_ref[...] = keys_now
    value_ref[...] = key_value[:, LANES:]
    scaled = keys_now * key_gain_ref[...]
    unit_key = scaled * lax.rsqrt(head_sums(scaled * scaled) + UNIT_EPS)
    vectors_ref[...] = jnp.zeros_like(vectors_ref)
    vectors_ref[pl.ds(0, seqs, stride=8), :] = unit_key
    vectors_ref[pl.ds(2, seqs, stride=8), :] = pltpu.roll(unit_key, HEAD, 1)
    recept_decay = project(2, 2)
    recept = recept_decay[:, :LANES]
    recept_ref[...] = recept
    decay_pre = recept_decay[:, LANES:] + decay_base_ref[...]
    decay_now = jnp.exp(-jnp.exp(-jax.nn.softplus(-decay_pre) - 0.5))
    decay_ref[...] = decay_now
    decayed_recept = decay_now * recept
    vectors_ref[pl.ds(1, seqs, stride=8), :] = decayed_recept
    vectors_ref[pl.ds(3, seqs, stride=8), :] = pltpu.roll(decayed_recept, HEAD, 1)
    rate_pre = project(4, 1) + rate_base_ref[...]
    unit_rate_ref[...] = unit_key * jax.nn.sigmoid(rate_pre)


def project_heads(tokens, projections, mix_gain, vectors, routes, logits, slots):
    seqs, full_width = tokens.shape
    small = jax.ShapeDtypeStruct((seqs, LANES), F32)
    hbm = pl.BlockSpec(memory_space=pl.ANY)
    vmem = pl.BlockSpec(memory_space=VMEM)
    return pl.pallas_call(
        project_kernel,
        out_shape=(jax.ShapeDtypeStruct((seqs * 8, LANES), F32),)
        + (small,) * 5
        + (
            jax.ShapeDtypeStruct((seqs, LANES), BF16),
            jax.ShapeDtypeStruct((slots, seqs), BF16),
            jax.ShapeDtypeStruct((slots, seqs), F32),
        ),
        in_specs=[hbm] * 12,
        out_specs=(vmem,) * 9,
        scratch_shapes=[
            VMEM((seqs, full_width), BF16),
            VMEM((full_width, 5 * LANES), BF16),
            VMEM((1, full_width), F32),
            VMEM((1, LANES), F32),
            VMEM((1, LANES), F32),
            VMEM((1, LANES), F32),
            VMEM(routes.shape, jnp.int32),
            VMEM(logits.shape, F32),
            pltpu.SemaphoreType.DMA((6,)),
            pltpu.SemaphoreType.DMA((6,)),
        ],
        compiler_params=pltpu.CompilerParams(vmem_limit_bytes=12 << 20),
        cost_estimate=pl.CostEstimate(
            flops=3_000_000_000, bytes_accessed=6 << 20, transcendentals=0
        ),
        name="project_heads",
    )(*map(in_hbm, (tokens, *projections, mix_gain, *vectors, routes, logits)))


def mix_kernel(
    state_ref,
    vectors_ref,
    recept_ref,
    unit_rate_ref,
    key_ref,
    value_ref,
    w_output_ref,
    group_gain_ref,
    keep_ref,
    send_ref,
    removed_ref,
    products_ref,
):
    seqs = recept_ref.shape[0]
    for seq in range(seqs):
        left = vectors_ref[seq * 8 : seq * 8 + 8, :HEAD].astype(BF16)
        right = state_ref[seq * LANES : (seq + 1) * LANES, :].astype(BF16)
        products_ref[seq * 8 : seq * 8 + 8, :] = lax.dot_general(
            left, right, (((1,), (1,)), ((), ())), preferred_element_type=F32
        )
    first_head = lax.broadcasted_iota(jnp.int32, (seqs, LANES), 1) < HEAD
    removed = jnp.where(
        first_head,
        products_ref[pl.ds(0, seqs, stride=8), :],
        products_ref[pl.ds(2, seqs, stride=8), :],
    )
    faded = jnp.where(
        first_head,
        products_ref[pl.ds(1, seqs, stride=8), :],
        products_ref[pl.ds(3, seqs, stride=8), :],
    )
    removed_ref[...] = removed
    recept = recept_ref[...]
    readout = (
        faded
        - removed * head_sums(unit_rate_ref[...] * recept)
        + value_ref[...] * head_sums(key_ref[...] * recept)
    )
    centred = readout - head_sums(readout) * (1.0 / HEAD)
    spread = head_sums(centred * centred) * (1.0 / HEAD)
    mixed = (centred * lax.rsqrt(spread + GROUP_EPS) * group_gain_ref[...]).astype(BF16)
    core = lax.axis_index("tp_1")
    for place, z in enumerate(z_order(keep_ref.shape[0])):
        own = w_output_ref[:, pl.ds(pl.multiple_of((2 * z + core) * LANES, LANES), LANES)]
        keep_ref[place] = jnp.dot(mixed, own, preferred_element_type=F32)
        other = w_output_ref[:, pl.ds(pl.multiple_of((2 * z + 1 - core) * LANES, LANES), LANES)]
        send_ref[place] = jnp.dot(mixed, other, preferred_element_type=F32).astype(BF16)


def mix(state_rows, vectors, recept, unit_rate, key, value, w_output, group_gain, z_count):
    seqs = recept.shape[0]
    vmem = pl.BlockSpec(memory_space=VMEM)
    return pl.pallas_call(
        mix_kernel,
        out_shape=(
            jax.ShapeDtypeStruct((z_count, seqs, LANES), F32),
            jax.ShapeDtypeStruct((z_count, seqs, LANES), BF16),
            jax.ShapeDtypeStruct((seqs, LANES), F32),
        ),
        in_specs=[vmem] * 8,
        out_specs=(vmem,) * 3,
        scratch_shapes=[VMEM((seqs * 8, LANES), F32)],
        compiler_params=pltpu.CompilerParams(vmem_limit_bytes=12 << 20),
        name="mix",
    )(state_rows, vectors, recept, unit_rate, key, value, w_output, group_gain)


def update_kernel(
    state_ref,
    removed_ref,
    unit_rate_ref,
    decay_ref,
    key_ref,
    value_ref,
    out_ref,
    left_ref,
    right_ref,
):
    block = removed_ref.shape[0]
    first_head = lax.broadcasted_iota(jnp.int32, (block, LANES), 1) < HEAD
    removed = -removed_ref[...]
    removed_high = removed.astype(BF16).astype(F32)
    removed_low = removed - removed_high
    unit_rate = unit_rate_ref[...]
    unit_high = unit_rate.astype(BF16).astype(F32)
    unit_low = unit_rate - unit_high
    key = key_ref[...]
    lefts = (removed_high, removed_low, removed_high, value_ref[...])
    rights = (unit_high, unit_high, unit_low, key)
    for place in range(4):
        left_ref[pl.ds(place, block, stride=8), :] = jnp.where(first_head, lefts[place], 0.0)
        left_ref[pl.ds(place + 4, block, stride=8), :] = jnp.where(first_head, 0.0, lefts[place])
        right_ref[pl.ds(place, block, stride=8), :] = rights[place]
        right_ref[pl.ds(place + 4, block, stride=8), :] = pltpu.roll(rights[place], HEAD, 1)
    decay = decay_ref[...]
    decay_rolled = pltpu.roll(decay, HEAD, 1)
    for seq in range(block):
        left = left_ref[seq * 8 : seq * 8 + 8, :].astype(BF16)
        right = right_ref[seq * 8 : seq * 8 + 8, :HEAD].astype(BF16)
        change = lax.dot_general(
            left, right, (((0,), (0,)), ((), ())), preferred_element_type=F32
        )
        base = seq * LANES
        old = state_ref[base : base + HEAD, :]
        out_ref[base : base + HEAD, :] = old * decay[seq : seq + 1, :HEAD] + change[:HEAD]
        old = state_ref[base + HEAD : base + LANES, :]
        out_ref[base + HEAD : base + LANES, :] = (
            old * decay_rolled[seq : seq + 1, :HEAD] + change[HEAD:]
        )


def update_state(state_rows, removed, unit_rate, decay, key, value):
    seqs = removed.shape[0]
    steps = 8
    block = seqs // steps
    rows = pl.BlockSpec((block * LANES, HEAD), lambda i: (i, 0))
    small = pl.BlockSpec((block, LANES), lambda i: (i, 0))
    return pl.pallas_call(
        update_kernel,
        grid=(steps,),
        out_shape=jax.ShapeDtypeStruct(state_rows.shape, F32),
        in_specs=[rows] + [small] * 5,
        out_specs=rows,
        scratch_shapes=[VMEM((block * 8, LANES), F32), VMEM((block * 8, LANES), F32)],
        compiler_params=pltpu.CompilerParams(vmem_limit_bytes=8 << 20),
        cost_estimate=pl.CostEstimate(
            flops=2_000_000_000, bytes_accessed=8 << 20, transcendentals=0
        ),
        name="update_state",
    )(in_hbm(state_rows), removed, unit_rate, decay, key, value)


def dispatch_kernel(parts_ref, tokens_ref, pick_ref, resid_ref, out_ref):
    total = tokens_ref[...].astype(F32)
    mix = parts_ref[0].astype(F32)
    for z in range(1, parts_ref.shape[0]):
        mix = mix + parts_ref[z].astype(F32)
    resid = (total + mix).astype(BF16)
    resid_ref[...] = resid
    picked = jnp.dot(pick_ref[...], resid, preferred_element_type=F32).astype(BF16)
    for z in range(out_ref.shape[0]):
        out_ref[z] = picked


def dispatch_rows(parts, tokens, pick):
    return pl.pallas_call(
        dispatch_kernel,
        out_shape=(
            jax.ShapeDtypeStruct(tokens.shape, BF16),
            jax.ShapeDtypeStruct((parts.shape[0], pick.shape[0], LANES), BF16),
        ),
        compiler_params=pltpu.CompilerParams(vmem_limit_bytes=4 << 20),
        name="dispatch_rows",
    )(parts, tokens, pick)


ACROSS = (((1,), (1,)), ((), ()))


def core_columns(ref, core):
    blocks = ref.shape[1] // (2 * LANES)
    return jnp.concatenate(
        [
            ref[:, pl.ds(pl.multiple_of((2 * z + core) * LANES, LANES), LANES)]
            for z in z_order(blocks)
        ],
        axis=1,
    )


def half_products(rows_ref, gain_ref, gate_ref, up_ref, core):
    gain = core_columns(gain_ref, core)
    squares = jnp.zeros(rows_ref.shape[1:], F32)
    parts = []
    for z in range(rows_ref.shape[0]):
        rows = rows_ref[z].astype(F32)
        squares = squares + rows * rows
        parts.append((rows * gain[:, z * LANES : (z + 1) * LANES]).astype(BF16))
    x = jnp.concatenate(parts, axis=1)
    gate = lax.dot_general(
        x, core_columns(gate_ref, core), ACROSS, preferred_element_type=F32
    )
    upward = lax.dot_general(
        x, core_columns(up_ref, core), ACROSS, preferred_element_type=F32
    )
    return squares, gate, upward


def own_half_kernel(rows_ref, gain_ref, gate_ref, up_ref, squares_ref, gate_out, up_out):
    core = lax.axis_index("tp_1")
    squares_ref[...], gate_out[...], up_out[...] = half_products(
        rows_ref, gain_ref, gate_ref, up_ref, core
    )


def other_half_kernel(
    rows_ref,
    gain_ref,
    gate_ref,
    up_ref,
    down_ref,
    squares_ref,
    gate_part_ref,
    up_part_ref,
    hidden_ref,
    send_ref,
):
    other = 1 - lax.axis_index("tp_1")
    squares, gate, upward = half_products(rows_ref, gain_ref, gate_ref, up_ref, other)
    square_sum = jnp.sum(squares + squares_ref[...], axis=1, keepdims=True)
    scale = lax.rsqrt(square_sum / gate_ref.shape[1] + RMS_EPS)
    gate = (gate + gate_part_ref[...]) * scale
    upward = (upward + up_part_ref[...]) * scale
    hidden = (jax.nn.silu(gate) * upward).astype(BF16)
    hidden_ref[...] = hidden
    out = jnp.dot(hidden, core_columns(down_ref, other), preferred_element_type=F32)
    for z in range(send_ref.shape[0]):
        send_ref[z] = out[:, z * LANES : (z + 1) * LANES].astype(BF16)


def keep_kernel(hidden_ref, down_ref, keep_ref):
    core = lax.axis_index("tp_1")
    out = jnp.dot(hidden_ref[...], core_columns(down_ref, core), preferred_element_type=F32)
    for z in range(keep_ref.shape[0]):
        keep_ref[z] = out[:, z * LANES : (z + 1) * LANES]


def run_expert(own, gain, gate, up, down):
    rows = own.shape[1]
    vmem = pl.BlockSpec(memory_space=VMEM)
    part = jax.ShapeDtypeStruct((rows, gate.shape[0]), F32)

    def call(body, name, *operands, out_shape):
        return pl.pallas_call(
            body,
            out_shape=out_shape,
            in_specs=[vmem] * len(operands),
            out_specs=jax.tree.map(lambda _: vmem, out_shape),
            compiler_params=pltpu.CompilerParams(vmem_limit_bytes=10 << 20),
            name=name,
        )(*operands)

    other = swap(own)
    partial = call(
        own_half_kernel,
        "own_half",
        own,
        gain,
        gate,
        up,
        out_shape=(jax.ShapeDtypeStruct((rows, LANES), F32), part, part),
    )
    other, partial = lax.optimization_barrier((other, partial))
    hidden, send = call(
        other_half_kernel,
        "other_half",
        other,
        gain,
        gate,
        up,
        down,
        *partial,
        out_shape=(
            jax.ShapeDtypeStruct((rows, gate.shape[0]), BF16),
            jax.ShapeDtypeStruct(own.shape, BF16),
        ),
    )
    received = swap(send)
    keep = call(
        keep_kernel, "keep_half", hidden, down, out_shape=jax.ShapeDtypeStruct(own.shape, F32)
    )
    return (keep + received.astype(F32)).astype(BF16)


def combine_kernel(share_ref, rows_ref, resid_ref, out_ref):
    rows = rows_ref[0].astype(F32)
    for z in range(1, rows_ref.shape[0]):
        rows = rows + rows_ref[z].astype(F32)
    moe = lax.dot_general(
        share_ref[...],
        rows,
        (((0,), (0,)), ((), ())),
        precision=HIGHEST,
        preferred_element_type=F32,
    )
    out_ref[...] = (resid_ref[...].astype(F32) + moe).astype(BF16)


def combine_rows(share, rows, resid):
    return pl.pallas_call(
        combine_kernel,
        out_shape=jax.ShapeDtypeStruct(resid.shape, BF16),
        compiler_params=pltpu.CompilerParams(vmem_limit_bytes=4 << 20),
        name="combine",
    )(share, rows, resid)


def swap(shard):
    return lax.ppermute(shard, "tp_1", [(0, 1), (1, 0)])


def exchange(shard, axis, order):
    return lax.all_to_all(
        shard, axis, split_axis=0, concat_axis=0, axis_index_groups=[order], tiled=True
    )


def exchange_rows(shard):
    ep_count, z_count = lax.axis_size("ep"), lax.axis_size("tp_0")
    order = [z * ep_count + e for z in z_order(z_count) for e in ep_order(ep_count)]
    chunks = shard.reshape(len(order), -1, 4, LANES)
    return exchange(chunks, ("tp_0", "ep"), order).reshape(shard.shape)


def local(
    tokens,
    state,
    routes,
    route_logits,
    mix_gain,
    w_recept,
    w_key,
    w_value,
    w_decay,
    w_rate,
    decay_base,
    rate_base,
    key_gain,
    group_gain,
    w_output,
    ffn_gain,
    w_gate,
    w_up,
    w_down,
):
    seq_rows = tokens.shape[0]
    z_count = lax.axis_size("tp_0")
    group_count = lax.axis_size("ep")
    slot_rows = max(2, 3 * routes.shape[1] * seq_rows // (2 * group_count))
    slot_count = group_count * slot_rows

    state_rows = state.reshape(-1, HEAD)
    vectors, recept, unit_rate, decay, key, value, own_tokens, pick, share = project_heads(
        tokens,
        (w_recept, w_key, w_value, w_decay, w_rate),
        mix_gain.reshape(1, -1),
        [v.reshape(1, -1) for v in (decay_base, rate_base, key_gain)],
        routes.T,
        route_logits.T,
        slot_count,
    )
    keep, send, removed = mix(
        state_rows,
        vectors,
        recept,
        unit_rate,
        key,
        value,
        w_output,
        group_gain.reshape(1, -1),
        z_count,
    )
    pair_sum = (keep + swap(send).astype(F32)).astype(BF16)
    parts = exchange(pair_sum, "tp_0", z_order(z_count))
    new_state = update_state(state_rows, removed, unit_rate, decay, key, value)

    resid_own, outgoing = dispatch_rows(parts, own_tokens, pick)
    arrived = exchange_rows(outgoing)
    gain = ffn_gain.reshape(1, -1)
    pair_sum = run_expert(
        arrived,
        gain,
        jnp.swapaxes(w_gate[0], 0, 1),
        jnp.swapaxes(w_up[0], 0, 1),
        w_down[0],
    )
    output = combine_rows(share, exchange_rows(pair_sum), resid_own)
    return (output, new_state.reshape(state.shape))


def solution(mesh):
    torus = Mesh(mesh.devices.reshape(mesh.shape["ep"], 8, 2), ("ep", "tp_0", "tp_1"))
    return jax.shard_map(
        local,
        mesh=torus,
        in_specs=(
            P("ep", None),
            P("ep", TP, None, None),
            P("ep", None),
            P("ep", None),
            P(),
            P(None, TP),
            P(None, TP),
            P(None, TP),
            P(None, TP),
            P(None, TP),
            P(TP),
            P(TP),
            P(TP),
            P(TP),
            P(TP, None),
            P(),
            P("ep", None, TP),
            P("ep", None, TP),
            P("ep", TP, None),
        ),
        out_specs=(P("ep", TP), P("ep", TP, None, None)),
        check_vma=False,
    )
```

```python
import jax
import jax.numpy as jnp
from jax import lax
from jax.experimental import pallas as pl
from jax.experimental.pallas import tpu as pltpu
from jax.sharding import Mesh
from jax.sharding import PartitionSpec as P

TP = ("tp_0", "tp_1")

RMS_EPS = 1e-06
GROUP_EPS = 0.00064
UNIT_EPS = 6.4e-05
HIGHEST = lax.Precision.HIGHEST
F32 = jnp.float32
BF16 = jnp.bfloat16
VMEM = pltpu.VMEM
HEAD = 64
LANES = 128
FIRST_Z = 5
FIRST_EP = 10


def z_order(count):
    return [(FIRST_Z + step) % count for step in range(count)]


def ep_order(count):
    return [(FIRST_EP + step) % count for step in range(count)]


def in_hbm(array):
    return pltpu.with_memory_space_constraint(array, pltpu.HBM)


def head_sums(values):
    rows = lax.broadcasted_iota(jnp.int32, (LANES, LANES), 0) // HEAD
    cols = lax.broadcasted_iota(jnp.int32, (LANES, LANES), 1) // HEAD
    ones = (rows == cols).astype(F32)
    return jnp.dot(values, ones, precision=HIGHEST, preferred_element_type=F32)


def route_slots(routes, logits, pick_ref, share_ref):
    slots, seqs = pick_ref.shape
    experts = lax.axis_size("ep")
    first, second = routes[0:1, :], routes[1:2, :]
    expert = lax.broadcasted_iota(jnp.int32, (experts, seqs), 0)
    named = [(expert == choice).astype(F32) for choice in (first, second)]
    earlier = lax.broadcasted_iota(jnp.int32, (seqs, seqs), 0) < lax.broadcasted_iota(
        jnp.int32, (seqs, seqs), 1
    )
    counts = jnp.dot(
        (named[0] + named[1]).astype(BF16),
        earlier.astype(F32).astype(BF16),
        preferred_element_type=F32,
    )
    exps = jnp.exp(logits)
    total = exps[0:1, :] + exps[1:2, :]
    slot = lax.broadcasted_iota(jnp.int32, (slots, seqs), 0)
    picked = jnp.zeros((slots, seqs), F32)
    shares = jnp.zeros((slots, seqs), F32)
    for k, choice in enumerate((first, second)):
        placed = jnp.sum(named[k] * counts, axis=0, keepdims=True).astype(jnp.int32)
        chunk = lax.rem(choice + (experts - FIRST_EP), experts)
        here = slot == chunk * (slots // experts) + placed
        picked = jnp.where(here, 1.0, picked)
        shares = jnp.where(here, exps[k : k + 1, :] / total, shares)
    pick_ref[...] = picked.astype(BF16)
    share_ref[...] = shares


def project_kernel(
    tokens_hbm,
    w_recept_hbm,
    w_key_hbm,
    w_value_hbm,
    w_decay_hbm,
    w_rate_hbm,
    mix_gain_hbm,
    decay_base_hbm,
    rate_base_hbm,
    key_gain_hbm,
    routes_hbm,
    logits_hbm,
    vectors_ref,
    recept_ref,
    unit_rate_ref,
    decay_ref,
    key_ref,
    value_ref,
    own_ref,
    pick_ref,
    share_ref,
    tokens_ref,
    weights_ref,
    mix_gain_ref,
    decay_base_ref,
    rate_base_ref,
    key_gain_ref,
    routes_ref,
    logits_ref,
    sems,
    small_sems,
):
    seqs = tokens_ref.shape[0]
    copies = [pltpu.make_async_copy(tokens_hbm, tokens_ref, sems.at[0])]
    smalls = [
        pltpu.make_async_copy(source, target, small_sems.at[place])
        for place, (source, target) in enumerate(
            (
                (mix_gain_hbm, mix_gain_ref),
                (key_gain_hbm, key_gain_ref),
                (decay_base_hbm, decay_base_ref),
                (rate_base_hbm, rate_base_ref),
                (routes_hbm, routes_ref),
                (logits_hbm, logits_ref),
            )
        )
    ]
    sources = (w_key_hbm, w_value_hbm, w_recept_hbm, w_decay_hbm, w_rate_hbm)
    for place, source in enumerate(sources):
        target = weights_ref.at[:, pl.ds(place * LANES, LANES)]
        copies.append(pltpu.make_async_copy(source, target, sems.at[1 + place]))
    copies[0].start()
    for copy in smalls:
        copy.start()
    for copy in copies[1:]:
        copy.start()

    for copy in smalls:
        copy.wait()
    route_slots(routes_ref[...], logits_ref[...], pick_ref, share_ref)
    copies[0].wait()
    own_ref[...] = tokens_ref[:, pl.ds(pl.multiple_of(lax.axis_index(TP) * LANES, LANES), LANES)]
    values = tokens_ref[...].astype(F32)
    mean_square = jnp.mean(values * values, axis=1, keepdims=True)
    normed = (values * lax.rsqrt(mean_square + RMS_EPS) * mix_gain_ref[...]).astype(BF16)

    def project(first, count):
        for place in range(first, first + count):
            copies[1 + place].wait()
        weight = weights_ref[:, first * LANES : (first + count) * LANES]
        return jnp.dot(normed, weight, preferred_element_type=F32).astype(BF16).astype(F32)

    key_value = project(0, 2)
    keys_now = key_value[:, :LANES]
    key_ref[...] = keys_now
    value_ref[...] = key_value[:, LANES:]
    scaled = keys_now * key_gain_ref[...]
    unit_key = scaled * lax.rsqrt(head_sums(scaled * scaled) + UNIT_EPS)
    vectors_ref[...] = jnp.zeros_like(vectors_ref)
    vectors_ref[pl.ds(0, seqs, stride=8), :] = unit_key
    vectors_ref[pl.ds(2, seqs, stride=8), :] = pltpu.roll(unit_key, HEAD, 1)
    recept_decay = project(2, 2)
    recept = recept_decay[:, :LANES]
    recept_ref[...] = recept
    decay_pre = recept_decay[:, LANES:] + decay_base_ref[...]
    decay_now = jnp.exp(-jnp.exp(-jax.nn.softplus(-decay_pre) - 0.5))
    decay_ref[...] = decay_now
    decayed_recept = decay_now * recept
    vectors_ref[pl.ds(1, seqs, stride=8), :] = decayed_recept
    vectors_ref[pl.ds(3, seqs, stride=8), :] = pltpu.roll(decayed_recept, HEAD, 1)
    rate_pre = project(4, 1) + rate_base_ref[...]
    unit_rate_ref[...] = unit_key * jax.nn.sigmoid(rate_pre)


def project_heads(tokens, projections, mix_gain, vectors, routes, logits, slots):
    seqs, full_width = tokens.shape
    small = jax.ShapeDtypeStruct((seqs, LANES), F32)
    hbm = pl.BlockSpec(memory_space=pl.ANY)
    vmem = pl.BlockSpec(memory_space=VMEM)
    return pl.pallas_call(
        project_kernel,
        out_shape=(jax.ShapeDtypeStruct((seqs * 8, LANES), F32),)
        + (small,) * 5
        + (
            jax.ShapeDtypeStruct((seqs, LANES), BF16),
            jax.ShapeDtypeStruct((slots, seqs), BF16),
            jax.ShapeDtypeStruct((slots, seqs), F32),
        ),
        in_specs=[hbm] * 12,
        out_specs=(vmem,) * 9,
        scratch_shapes=[
            VMEM((seqs, full_width), BF16),
            VMEM((full_width, 5 * LANES), BF16),
            VMEM((1, full_width), F32),
            VMEM((1, LANES), F32),
            VMEM((1, LANES), F32),
            VMEM((1, LANES), F32),
            VMEM(routes.shape, jnp.int32),
            VMEM(logits.shape, F32),
            pltpu.SemaphoreType.DMA((6,)),
            pltpu.SemaphoreType.DMA((6,)),
        ],
        compiler_params=pltpu.CompilerParams(vmem_limit_bytes=12 << 20),
        cost_estimate=pl.CostEstimate(
            flops=3_000_000_000, bytes_accessed=6 << 20, transcendentals=0
        ),
        name="project_heads",
    )(*map(in_hbm, (tokens, *projections, mix_gain, *vectors, routes, logits)))


def mix_kernel(
    state_ref,
    vectors_ref,
    recept_ref,
    unit_rate_ref,
    key_ref,
    value_ref,
    w_output_hbm,
    group_gain_ref,
    send_ref,
    removed_ref,
    mixed_ref,
    w_output_ref,
    products_ref,
    sem,
):
    w_output_copy = pltpu.make_async_copy(w_output_hbm, w_output_ref, sem)
    w_output_copy.start()
    seqs = recept_ref.shape[0]
    group = 2
    for seq in range(0, seqs, group):
        left = vectors_ref[seq * 8 : (seq + group) * 8, :HEAD].astype(BF16)
        right = state_ref[seq * LANES : (seq + group) * LANES, :].astype(BF16)
        out = lax.dot_general(left, right, ACROSS, preferred_element_type=F32)
        for one in range(group):
            products_ref[(seq + one) * 8 : (seq + one + 1) * 8, :] = out[
                one * 8 : (one + 1) * 8, one * LANES : (one + 1) * LANES
            ]
    first_head = lax.broadcasted_iota(jnp.int32, (seqs, LANES), 1) < HEAD
    removed = jnp.where(
        first_head,
        products_ref[pl.ds(0, seqs, stride=8), :],
        products_ref[pl.ds(2, seqs, stride=8), :],
    )
    faded = jnp.where(
        first_head,
        products_ref[pl.ds(1, seqs, stride=8), :],
        products_ref[pl.ds(3, seqs, stride=8), :],
    )
    removed_ref[...] = removed
    recept = recept_ref[...]
    readout = (
        faded
        - removed * head_sums(unit_rate_ref[...] * recept)
        + value_ref[...] * head_sums(key_ref[...] * recept)
    )
    centred = readout - head_sums(readout) * (1.0 / HEAD)
    spread = head_sums(centred * centred) * (1.0 / HEAD)
    mixed = (centred * lax.rsqrt(spread + GROUP_EPS) * group_gain_ref[...]).astype(BF16)
    mixed_ref[...] = mixed
    w_output_copy.wait()
    out_columns(mixed, w_output_ref, send_ref, 1 - lax.axis_index("tp_1"))


def out_columns(mixed, w_output_ref, out_ref, core):
    for place, z in enumerate(z_order(out_ref.shape[0])):
        cols = pl.ds(pl.multiple_of((2 * z + core) * LANES, LANES), LANES)
        out_ref[place] = jnp.dot(
            mixed, w_output_ref[:, cols], preferred_element_type=F32
        ).astype(out_ref.dtype)


def mix(state_rows, vectors, recept, unit_rate, key, value, w_output, group_gain, z_count):
    seqs = recept.shape[0]
    vmem = pl.BlockSpec(memory_space=VMEM)
    return pl.pallas_call(
        mix_kernel,
        out_shape=(
            jax.ShapeDtypeStruct((z_count, seqs, LANES), BF16),
            jax.ShapeDtypeStruct((seqs, LANES), F32),
            jax.ShapeDtypeStruct((seqs, LANES), BF16),
            jax.ShapeDtypeStruct(w_output.shape, BF16),
        ),
        in_specs=[vmem] * 6 + [pl.BlockSpec(memory_space=pl.ANY), vmem],
        out_specs=(vmem,) * 4,
        scratch_shapes=[VMEM((seqs * 8, LANES), F32), pltpu.SemaphoreType.DMA(())],
        compiler_params=pltpu.CompilerParams(vmem_limit_bytes=12 << 20),
        name="mix",
    )(state_rows, vectors, recept, unit_rate, key, value, in_hbm(w_output), group_gain)


def keep_out_kernel(mixed_ref, w_output_ref, keep_ref):
    out_columns(mixed_ref[...], w_output_ref, keep_ref, lax.axis_index("tp_1"))


def keep_out(mixed, w_output, z_count):
    return pl.pallas_call(
        keep_out_kernel,
        out_shape=jax.ShapeDtypeStruct((z_count, *mixed.shape), F32),
        compiler_params=pltpu.CompilerParams(vmem_limit_bytes=2 << 20),
        name="keep_out",
    )(mixed, w_output)


def update_kernel(
    state_ref,
    removed_ref,
    unit_rate_ref,
    decay_ref,
    key_ref,
    value_ref,
    out_ref,
    left_ref,
    right_ref,
):
    block = removed_ref.shape[0]
    first_head = lax.broadcasted_iota(jnp.int32, (block, LANES), 1) < HEAD
    removed = -removed_ref[...]
    removed_high = removed.astype(BF16).astype(F32)
    removed_low = removed - removed_high
    unit_rate = unit_rate_ref[...]
    unit_high = unit_rate.astype(BF16).astype(F32)
    unit_low = unit_rate - unit_high
    key = key_ref[...]
    lefts = (removed_high, removed_low, removed_high, value_ref[...])
    rights = (unit_high, unit_high, unit_low, key)
    for place in range(4):
        left_ref[pl.ds(place, block, stride=8), :] = jnp.where(first_head, lefts[place], 0.0)
        left_ref[pl.ds(place + 4, block, stride=8), :] = jnp.where(first_head, 0.0, lefts[place])
        right_ref[pl.ds(place, block, stride=8), :] = rights[place]
        right_ref[pl.ds(place + 4, block, stride=8), :] = pltpu.roll(rights[place], HEAD, 1)
    decay = decay_ref[...]
    decay_rolled = pltpu.roll(decay, HEAD, 1)
    for seq in range(block):
        left = left_ref[seq * 8 : seq * 8 + 8, :].astype(BF16)
        right = right_ref[seq * 8 : seq * 8 + 8, :HEAD].astype(BF16)
        change = lax.dot_general(
            left, right, (((0,), (0,)), ((), ())), preferred_element_type=F32
        )
        base = seq * LANES
        old = state_ref[base : base + HEAD, :]
        out_ref[base : base + HEAD, :] = old * decay[seq : seq + 1, :HEAD] + change[:HEAD]
        old = state_ref[base + HEAD : base + LANES, :]
        out_ref[base + HEAD : base + LANES, :] = (
            old * decay_rolled[seq : seq + 1, :HEAD] + change[HEAD:]
        )


def update_state(state_rows, removed, unit_rate, decay, key, value):
    seqs = removed.shape[0]
    steps = 8
    block = seqs // steps
    rows = pl.BlockSpec((block * LANES, HEAD), lambda i: (i, 0))
    small = pl.BlockSpec((block, LANES), lambda i: (i, 0))
    return pl.pallas_call(
        update_kernel,
        grid=(steps,),
        out_shape=jax.ShapeDtypeStruct(state_rows.shape, F32),
        in_specs=[rows] + [small] * 5,
        out_specs=rows,
        scratch_shapes=[VMEM((block * 8, LANES), F32), VMEM((block * 8, LANES), F32)],
        compiler_params=pltpu.CompilerParams(vmem_limit_bytes=8 << 20),
        cost_estimate=pl.CostEstimate(
            flops=2_000_000_000, bytes_accessed=8 << 20, transcendentals=0
        ),
        name="update_state",
    )(in_hbm(state_rows), removed, unit_rate, decay, key, value)


def dispatch_kernel(parts_ref, tokens_ref, pick_ref, resid_ref, out_ref):
    total = tokens_ref[...].astype(F32)
    mix = parts_ref[0].astype(F32)
    for z in range(1, parts_ref.shape[0]):
        mix = mix + parts_ref[z].astype(F32)
    resid = (total + mix).astype(BF16)
    resid_ref[...] = resid
    picked = jnp.dot(pick_ref[...], resid, preferred_element_type=F32).astype(BF16)
    for z in range(out_ref.shape[0]):
        out_ref[z] = picked


def dispatch_rows(parts, tokens, pick):
    return pl.pallas_call(
        dispatch_kernel,
        out_shape=(
            jax.ShapeDtypeStruct(tokens.shape, BF16),
            jax.ShapeDtypeStruct((parts.shape[0], pick.shape[0], LANES), BF16),
        ),
        compiler_params=pltpu.CompilerParams(vmem_limit_bytes=4 << 20),
        name="dispatch_rows",
    )(parts, tokens, pick)


ACROSS = (((1,), (1,)), ((), ()))


def core_columns(ref, core):
    blocks = ref.shape[1] // (2 * LANES)
    return jnp.concatenate(
        [
            ref[:, pl.ds(pl.multiple_of((2 * z + core) * LANES, LANES), LANES)]
            for z in z_order(blocks)
        ],
        axis=1,
    )


def half_products(rows_ref, gain_ref, gate_ref, up_ref, core):
    gain = core_columns(gain_ref, core)
    squares = jnp.zeros(rows_ref.shape[1:], F32)
    parts = []
    for z in range(rows_ref.shape[0]):
        rows = rows_ref[z].astype(F32)
        squares = squares + rows * rows
        parts.append((rows * gain[:, z * LANES : (z + 1) * LANES]).astype(BF16))
    x = jnp.concatenate(parts, axis=1)
    gate = lax.dot_general(
        x, core_columns(gate_ref, core), ACROSS, preferred_element_type=F32
    )
    upward = lax.dot_general(
        x, core_columns(up_ref, core), ACROSS, preferred_element_type=F32
    )
    return squares, gate, upward


def own_half_kernel(rows_ref, gain_ref, gate_ref, up_ref, squares_ref, gate_out, up_out):
    core = lax.axis_index("tp_1")
    squares_ref[...], gate_out[...], up_out[...] = half_products(
        rows_ref, gain_ref, gate_ref, up_ref, core
    )


def other_half_kernel(
    rows_ref,
    gain_ref,
    gate_ref,
    up_ref,
    down_ref,
    squares_ref,
    gate_part_ref,
    up_part_ref,
    hidden_ref,
    send_ref,
):
    other = 1 - lax.axis_index("tp_1")
    squares, gate, upward = half_products(rows_ref, gain_ref, gate_ref, up_ref, other)
    square_sum = jnp.sum(squares + squares_ref[...], axis=1, keepdims=True)
    scale = lax.rsqrt(square_sum / gate_ref.shape[1] + RMS_EPS)
    gate = (gate + gate_part_ref[...]) * scale
    upward = (upward + up_part_ref[...]) * scale
    hidden = (jax.nn.silu(gate) * upward).astype(BF16)
    hidden_ref[...] = hidden
    out = jnp.dot(hidden, core_columns(down_ref, other), preferred_element_type=F32)
    for z in range(send_ref.shape[0]):
        send_ref[z] = out[:, z * LANES : (z + 1) * LANES].astype(BF16)


def keep_kernel(hidden_ref, down_ref, keep_ref):
    core = lax.axis_index("tp_1")
    out = jnp.dot(hidden_ref[...], core_columns(down_ref, core), preferred_element_type=F32)
    for z in range(keep_ref.shape[0]):
        keep_ref[z] = out[:, z * LANES : (z + 1) * LANES]


def run_expert(own, gain, gate, up, down):
    rows = own.shape[1]
    vmem = pl.BlockSpec(memory_space=VMEM)
    part = jax.ShapeDtypeStruct((rows, gate.shape[0]), F32)

    def call(body, name, *operands, out_shape):
        return pl.pallas_call(
            body,
            out_shape=out_shape,
            in_specs=[vmem] * len(operands),
            out_specs=jax.tree.map(lambda _: vmem, out_shape),
            compiler_params=pltpu.CompilerParams(vmem_limit_bytes=10 << 20),
            name=name,
        )(*operands)

    other = swap(own)
    partial = call(
        own_half_kernel,
        "own_half",
        own,
        gain,
        gate,
        up,
        out_shape=(jax.ShapeDtypeStruct((rows, LANES), F32), part, part),
    )
    other, partial = lax.optimization_barrier((other, partial))
    hidden, send = call(
        other_half_kernel,
        "other_half",
        other,
        gain,
        gate,
        up,
        down,
        *partial,
        out_shape=(
            jax.ShapeDtypeStruct((rows, gate.shape[0]), BF16),
            jax.ShapeDtypeStruct(own.shape, BF16),
        ),
    )
    received = swap(send)
    keep = call(
        keep_kernel, "keep_half", hidden, down, out_shape=jax.ShapeDtypeStruct(own.shape, F32)
    )
    return (keep + received.astype(F32)).astype(BF16)


def combine_kernel(share_ref, rows_ref, resid_ref, out_ref):
    rows = rows_ref[0].astype(F32)
    for z in range(1, rows_ref.shape[0]):
        rows = rows + rows_ref[z].astype(F32)
    moe = lax.dot_general(
        share_ref[...],
        rows,
        (((0,), (0,)), ((), ())),
        precision=HIGHEST,
        preferred_element_type=F32,
    )
    out_ref[...] = (resid_ref[...].astype(F32) + moe).astype(BF16)


def combine_rows(share, rows, resid):
    return pl.pallas_call(
        combine_kernel,
        out_shape=jax.ShapeDtypeStruct(resid.shape, BF16),
        compiler_params=pltpu.CompilerParams(vmem_limit_bytes=4 << 20),
        name="combine",
    )(share, rows, resid)


def swap(shard):
    return lax.ppermute(shard, "tp_1", [(0, 1), (1, 0)])


def exchange(shard, axis, order):
    return lax.all_to_all(
        shard, axis, split_axis=0, concat_axis=0, axis_index_groups=[order], tiled=True
    )


def exchange_rows(shard):
    ep_count, z_count = lax.axis_size("ep"), lax.axis_size("tp_0")
    order = [z * ep_count + e for z in z_order(z_count) for e in ep_order(ep_count)]
    chunks = shard.reshape(len(order), -1, 4, LANES)
    return exchange(chunks, ("tp_0", "ep"), order).reshape(shard.shape)


def local(
    tokens,
    state,
    routes,
    route_logits,
    mix_gain,
    w_recept,
    w_key,
    w_value,
    w_decay,
    w_rate,
    decay_base,
    rate_base,
    key_gain,
    group_gain,
    w_output,
    ffn_gain,
    w_gate,
    w_up,
    w_down,
):
    seq_rows = tokens.shape[0]
    z_count = lax.axis_size("tp_0")
    group_count = lax.axis_size("ep")
    slot_rows = max(2, 3 * routes.shape[1] * seq_rows // (2 * group_count))
    slot_count = group_count * slot_rows

    state_rows = state.reshape(-1, HEAD)
    vectors, recept, unit_rate, decay, key, value, own_tokens, pick, share = project_heads(
        tokens,
        (w_recept, w_key, w_value, w_decay, w_rate),
        mix_gain.reshape(1, -1),
        [v.reshape(1, -1) for v in (decay_base, rate_base, key_gain)],
        routes.T,
        route_logits.T,
        slot_count,
    )
    send, removed, mixed, w_output_near = mix(
        state_rows,
        vectors,
        recept,
        unit_rate,
        key,
        value,
        w_output,
        group_gain.reshape(1, -1),
        z_count,
    )
    keep = keep_out(mixed, w_output_near, z_count)
    pair_sum = (keep + swap(send).astype(F32)).astype(BF16)
    parts = exchange(pair_sum, "tp_0", z_order(z_count))
    new_state = update_state(state_rows, removed, unit_rate, decay, key, value)

    resid_own, outgoing = dispatch_rows(parts, own_tokens, pick)
    arrived = exchange_rows(outgoing)
    gain = ffn_gain.reshape(1, -1)
    pair_sum = run_expert(
        arrived,
        gain,
        jnp.swapaxes(w_gate[0], 0, 1),
        jnp.swapaxes(w_up[0], 0, 1),
        w_down[0],
    )
    output = combine_rows(share, exchange_rows(pair_sum), resid_own)
    return (output, new_state.reshape(state.shape))


def solution(mesh):
    torus = Mesh(mesh.devices.reshape(mesh.shape["ep"], 8, 2), ("ep", "tp_0", "tp_1"))
    return jax.shard_map(
        local,
        mesh=torus,
        in_specs=(
            P("ep", None),
            P("ep", TP, None, None),
            P("ep", None),
            P("ep", None),
            P(),
            P(None, TP),
            P(None, TP),
            P(None, TP),
            P(None, TP),
            P(None, TP),
            P(TP),
            P(TP),
            P(TP),
            P(TP),
            P(TP, None),
            P(),
            P("ep", None, TP),
            P("ep", None, TP),
            P("ep", TP, None),
        ),
        out_specs=(P("ep", TP), P("ep", TP, None, None)),
        check_vma=False,
    )
```

```python
import jax
import jax.numpy as jnp
from jax import lax
from jax.experimental import pallas as pl
from jax.experimental.pallas import tpu as pltpu
from jax.sharding import Mesh
from jax.sharding import PartitionSpec as P

TP = ("tp_0", "tp_1")

RMS_EPS = 1e-06
GROUP_EPS = 0.00064
UNIT_EPS = 6.4e-05
HIGHEST = lax.Precision.HIGHEST
F32 = jnp.float32
BF16 = jnp.bfloat16
VMEM = pltpu.VMEM
HEAD = 64
LANES = 128
FIRST_Z = 5
FIRST_EP = 10


def z_order(count):
    return [(FIRST_Z + step) % count for step in range(count)]


def ep_order(count):
    return [(FIRST_EP + step) % count for step in range(count)]


def in_hbm(array):
    return pltpu.with_memory_space_constraint(array, pltpu.HBM)


def head_sums(values):
    rows = lax.broadcasted_iota(jnp.int32, (LANES, LANES), 0) // HEAD
    cols = lax.broadcasted_iota(jnp.int32, (LANES, LANES), 1) // HEAD
    ones = (rows == cols).astype(F32)
    return jnp.dot(values, ones, precision=HIGHEST, preferred_element_type=F32)


def route_slots(routes, logits, pick_ref, share_ref):
    slots, seqs = pick_ref.shape
    experts = lax.axis_size("ep")
    first, second = routes[0:1, :], routes[1:2, :]
    expert = lax.broadcasted_iota(jnp.int32, (experts, seqs), 0)
    named = [(expert == choice).astype(F32) for choice in (first, second)]
    earlier = lax.broadcasted_iota(jnp.int32, (seqs, seqs), 0) < lax.broadcasted_iota(
        jnp.int32, (seqs, seqs), 1
    )
    counts = jnp.dot(
        (named[0] + named[1]).astype(BF16),
        earlier.astype(F32).astype(BF16),
        preferred_element_type=F32,
    )
    exps = jnp.exp(logits)
    total = exps[0:1, :] + exps[1:2, :]
    slot = lax.broadcasted_iota(jnp.int32, (slots, seqs), 0)
    picked = jnp.zeros((slots, seqs), F32)
    shares = jnp.zeros((slots, seqs), F32)
    for k, choice in enumerate((first, second)):
        placed = jnp.sum(named[k] * counts, axis=0, keepdims=True).astype(jnp.int32)
        chunk = lax.rem(choice + (experts - FIRST_EP), experts)
        here = slot == chunk * (slots // experts) + placed
        picked = jnp.where(here, 1.0, picked)
        shares = jnp.where(here, exps[k : k + 1, :] / total, shares)
    pick_ref[...] = picked.astype(BF16)
    share_ref[...] = shares


def project_kernel(
    tokens_hbm,
    w_recept_hbm,
    w_key_hbm,
    w_value_hbm,
    w_decay_hbm,
    w_rate_hbm,
    mix_gain_hbm,
    decay_base_hbm,
    rate_base_hbm,
    key_gain_hbm,
    routes_hbm,
    logits_hbm,
    vectors_ref,
    recept_ref,
    unit_rate_ref,
    decay_ref,
    key_ref,
    value_ref,
    own_ref,
    pick_ref,
    share_ref,
    tokens_ref,
    weights_ref,
    mix_gain_ref,
    decay_base_ref,
    rate_base_ref,
    key_gain_ref,
    routes_ref,
    logits_ref,
    sems,
    small_sems,
):
    seqs = tokens_ref.shape[0]
    copies = [pltpu.make_async_copy(tokens_hbm, tokens_ref, sems.at[0])]
    smalls = [
        pltpu.make_async_copy(source, target, small_sems.at[place])
        for place, (source, target) in enumerate(
            (
                (mix_gain_hbm, mix_gain_ref),
                (key_gain_hbm, key_gain_ref),
                (decay_base_hbm, decay_base_ref),
                (rate_base_hbm, rate_base_ref),
                (routes_hbm, routes_ref),
                (logits_hbm, logits_ref),
            )
        )
    ]
    sources = (w_key_hbm, w_value_hbm, w_recept_hbm, w_decay_hbm, w_rate_hbm)
    for place, source in enumerate(sources):
        target = weights_ref.at[:, pl.ds(place * LANES, LANES)]
        copies.append(pltpu.make_async_copy(source, target, sems.at[1 + place]))
    copies[0].start()
    for copy in smalls:
        copy.start()
    for copy in copies[1:]:
        copy.start()

    for copy in smalls:
        copy.wait()
    route_slots(routes_ref[...], logits_ref[...], pick_ref, share_ref)
    copies[0].wait()
    own_ref[...] = tokens_ref[:, pl.ds(pl.multiple_of(lax.axis_index(TP) * LANES, LANES), LANES)]
    values = tokens_ref[...].astype(F32)
    mean_square = jnp.mean(values * values, axis=1, keepdims=True)
    normed = (values * lax.rsqrt(mean_square + RMS_EPS) * mix_gain_ref[...]).astype(BF16)

    def project(first, count):
        for place in range(first, first + count):
            copies[1 + place].wait()
        weight = weights_ref[:, first * LANES : (first + count) * LANES]
        return jnp.dot(normed, weight, preferred_element_type=F32).astype(BF16).astype(F32)

    key_value = project(0, 2)
    keys_now = key_value[:, :LANES]
    key_ref[...] = keys_now
    value_ref[...] = key_value[:, LANES:]
    scaled = keys_now * key_gain_ref[...]
    unit_key = scaled * lax.rsqrt(head_sums(scaled * scaled) + UNIT_EPS)
    vectors_ref[...] = jnp.zeros_like(vectors_ref)
    vectors_ref[pl.ds(0, seqs, stride=8), :] = unit_key
    vectors_ref[pl.ds(2, seqs, stride=8), :] = pltpu.roll(unit_key, HEAD, 1)
    recept_decay = project(2, 2)
    recept = recept_decay[:, :LANES]
    recept_ref[...] = recept
    decay_pre = recept_decay[:, LANES:] + decay_base_ref[...]
    decay_now = jnp.exp(-jnp.exp(-jax.nn.softplus(-decay_pre) - 0.5))
    decay_ref[...] = decay_now
    decayed_recept = decay_now * recept
    vectors_ref[pl.ds(1, seqs, stride=8), :] = decayed_recept
    vectors_ref[pl.ds(3, seqs, stride=8), :] = pltpu.roll(decayed_recept, HEAD, 1)
    rate_pre = project(4, 1) + rate_base_ref[...]
    unit_rate_ref[...] = unit_key * jax.nn.sigmoid(rate_pre)


def project_heads(tokens, projections, mix_gain, vectors, routes, logits, slots):
    seqs, full_width = tokens.shape
    small = jax.ShapeDtypeStruct((seqs, LANES), F32)
    hbm = pl.BlockSpec(memory_space=pl.ANY)
    vmem = pl.BlockSpec(memory_space=VMEM)
    return pl.pallas_call(
        project_kernel,
        out_shape=(jax.ShapeDtypeStruct((seqs * 8, LANES), F32),)
        + (small,) * 5
        + (
            jax.ShapeDtypeStruct((seqs, LANES), BF16),
            jax.ShapeDtypeStruct((slots, seqs), BF16),
            jax.ShapeDtypeStruct((slots, seqs), F32),
        ),
        in_specs=[hbm] * 12,
        out_specs=(vmem,) * 9,
        scratch_shapes=[
            VMEM((seqs, full_width), BF16),
            VMEM((full_width, 5 * LANES), BF16),
            VMEM((1, full_width), F32),
            VMEM((1, LANES), F32),
            VMEM((1, LANES), F32),
            VMEM((1, LANES), F32),
            VMEM(routes.shape, jnp.int32),
            VMEM(logits.shape, F32),
            pltpu.SemaphoreType.DMA((6,)),
            pltpu.SemaphoreType.DMA((6,)),
        ],
        compiler_params=pltpu.CompilerParams(vmem_limit_bytes=12 << 20),
        cost_estimate=pl.CostEstimate(
            flops=3_000_000_000, bytes_accessed=6 << 20, transcendentals=0
        ),
        name="project_heads",
    )(*map(in_hbm, (tokens, *projections, mix_gain, *vectors, routes, logits)))


def mix_kernel(
    state_ref,
    vectors_ref,
    recept_ref,
    unit_rate_ref,
    key_ref,
    value_ref,
    w_output_hbm,
    group_gain_ref,
    send_ref,
    removed_ref,
    mixed_ref,
    w_output_ref,
    products_ref,
    sem,
):
    w_output_copy = pltpu.make_async_copy(w_output_hbm, w_output_ref, sem)
    w_output_copy.start()
    seqs = recept_ref.shape[0]
    group = 2
    for seq in range(0, seqs, group):
        left = vectors_ref[seq * 8 : (seq + group) * 8, :HEAD].astype(BF16)
        right = state_ref[seq * LANES : (seq + group) * LANES, :].astype(BF16)
        out = lax.dot_general(left, right, ACROSS, preferred_element_type=F32)
        for one in range(group):
            products_ref[(seq + one) * 8 : (seq + one + 1) * 8, :] = out[
                one * 8 : (one + 1) * 8, one * LANES : (one + 1) * LANES
            ]
    first_head = lax.broadcasted_iota(jnp.int32, (seqs, LANES), 1) < HEAD
    removed = jnp.where(
        first_head,
        products_ref[pl.ds(0, seqs, stride=8), :],
        products_ref[pl.ds(2, seqs, stride=8), :],
    )
    faded = jnp.where(
        first_head,
        products_ref[pl.ds(1, seqs, stride=8), :],
        products_ref[pl.ds(3, seqs, stride=8), :],
    )
    removed_ref[...] = removed
    recept = recept_ref[...]
    readout = (
        faded
        - removed * head_sums(unit_rate_ref[...] * recept)
        + value_ref[...] * head_sums(key_ref[...] * recept)
    )
    centred = readout - head_sums(readout) * (1.0 / HEAD)
    spread = head_sums(centred * centred) * (1.0 / HEAD)
    mixed = (centred * lax.rsqrt(spread + GROUP_EPS) * group_gain_ref[...]).astype(BF16)
    mixed_ref[...] = mixed
    w_output_copy.wait()
    out_columns(mixed, w_output_ref, send_ref, 1 - lax.axis_index("tp_1"))


def out_columns(mixed, w_output_ref, out_ref, core):
    for place, z in enumerate(z_order(out_ref.shape[0])):
        cols = pl.ds(pl.multiple_of((2 * z + core) * LANES, LANES), LANES)
        out_ref[place] = jnp.dot(
            mixed, w_output_ref[:, cols], preferred_element_type=F32
        ).astype(out_ref.dtype)


def mix(state_rows, vectors, recept, unit_rate, key, value, w_output, group_gain, z_count):
    seqs = recept.shape[0]
    vmem = pl.BlockSpec(memory_space=VMEM)
    return pl.pallas_call(
        mix_kernel,
        out_shape=(
            jax.ShapeDtypeStruct((z_count, seqs, LANES), BF16),
            jax.ShapeDtypeStruct((seqs, LANES), F32),
            jax.ShapeDtypeStruct((seqs, LANES), BF16),
            jax.ShapeDtypeStruct(w_output.shape, BF16),
        ),
        in_specs=[vmem] * 6 + [pl.BlockSpec(memory_space=pl.ANY), vmem],
        out_specs=(vmem,) * 4,
        scratch_shapes=[VMEM((seqs * 8, LANES), F32), pltpu.SemaphoreType.DMA(())],
        compiler_params=pltpu.CompilerParams(vmem_limit_bytes=12 << 20),
        name="mix",
    )(state_rows, vectors, recept, unit_rate, key, value, in_hbm(w_output), group_gain)


def keep_out_kernel(mixed_ref, w_output_ref, keep_ref):
    out_columns(mixed_ref[...], w_output_ref, keep_ref, lax.axis_index("tp_1"))


def keep_out(mixed, w_output, z_count):
    return pl.pallas_call(
        keep_out_kernel,
        out_shape=jax.ShapeDtypeStruct((z_count, *mixed.shape), F32),
        compiler_params=pltpu.CompilerParams(vmem_limit_bytes=2 << 20),
        name="keep_out",
    )(mixed, w_output)


def update_kernel(
    state_ref,
    removed_ref,
    unit_rate_ref,
    decay_ref,
    key_ref,
    value_ref,
    out_ref,
    left_ref,
    right_ref,
):
    block = removed_ref.shape[0]
    first_head = lax.broadcasted_iota(jnp.int32, (block, LANES), 1) < HEAD
    removed = -removed_ref[...]
    removed_high = removed.astype(BF16).astype(F32)
    removed_low = removed - removed_high
    unit_rate = unit_rate_ref[...]
    unit_high = unit_rate.astype(BF16).astype(F32)
    unit_low = unit_rate - unit_high
    key = key_ref[...]
    lefts = (removed_high, removed_low, removed_high, value_ref[...])
    rights = (unit_high, unit_high, unit_low, key)
    for place in range(4):
        left_ref[pl.ds(place, block, stride=8), :] = jnp.where(first_head, lefts[place], 0.0)
        left_ref[pl.ds(place + 4, block, stride=8), :] = jnp.where(first_head, 0.0, lefts[place])
        right_ref[pl.ds(place, block, stride=8), :] = rights[place]
        right_ref[pl.ds(place + 4, block, stride=8), :] = pltpu.roll(rights[place], HEAD, 1)
    decay = decay_ref[...]
    decay_rolled = pltpu.roll(decay, HEAD, 1)
    for seq in range(block):
        left = left_ref[seq * 8 : seq * 8 + 8, :].astype(BF16)
        right = right_ref[seq * 8 : seq * 8 + 8, :HEAD].astype(BF16)
        change = lax.dot_general(
            left, right, (((0,), (0,)), ((), ())), preferred_element_type=F32
        )
        base = seq * LANES
        old = state_ref[base : base + HEAD, :]
        out_ref[base : base + HEAD, :] = old * decay[seq : seq + 1, :HEAD] + change[:HEAD]
        old = state_ref[base + HEAD : base + LANES, :]
        out_ref[base + HEAD : base + LANES, :] = (
            old * decay_rolled[seq : seq + 1, :HEAD] + change[HEAD:]
        )


def update_state(state_rows, removed, unit_rate, decay, key, value):
    seqs = removed.shape[0]
    steps = 8
    block = seqs // steps
    rows = pl.BlockSpec((block * LANES, HEAD), lambda i: (i, 0))
    small = pl.BlockSpec((block, LANES), lambda i: (i, 0))
    return pl.pallas_call(
        update_kernel,
        grid=(steps,),
        out_shape=jax.ShapeDtypeStruct(state_rows.shape, F32),
        in_specs=[rows] + [small] * 5,
        out_specs=rows,
        scratch_shapes=[VMEM((block * 8, LANES), F32), VMEM((block * 8, LANES), F32)],
        compiler_params=pltpu.CompilerParams(vmem_limit_bytes=8 << 20),
        cost_estimate=pl.CostEstimate(
            flops=2_000_000_000, bytes_accessed=8 << 20, transcendentals=0
        ),
        name="update_state",
    )(in_hbm(state_rows), removed, unit_rate, decay, key, value)


def dispatch_kernel(parts_ref, tokens_ref, pick_ref, resid_ref, out_ref):
    total = tokens_ref[...].astype(F32)
    mix = parts_ref[0].astype(F32)
    for z in range(1, parts_ref.shape[0]):
        mix = mix + parts_ref[z].astype(F32)
    resid = (total + mix).astype(BF16)
    resid_ref[...] = resid
    picked = jnp.dot(pick_ref[...], resid, preferred_element_type=F32).astype(BF16)
    for z in range(out_ref.shape[0]):
        out_ref[z] = picked


def dispatch_rows(parts, tokens, pick):
    return pl.pallas_call(
        dispatch_kernel,
        out_shape=(
            jax.ShapeDtypeStruct(tokens.shape, BF16),
            jax.ShapeDtypeStruct((parts.shape[0], pick.shape[0], LANES), BF16),
        ),
        compiler_params=pltpu.CompilerParams(vmem_limit_bytes=4 << 20),
        name="dispatch_rows",
    )(parts, tokens, pick)


ACROSS = (((1,), (1,)), ((), ()))


def core_columns(ref, core, first=0, count=None):
    blocks = z_order(ref.shape[1] // (2 * LANES))
    count = len(blocks) if count is None else count
    return jnp.concatenate(
        [
            ref[:, pl.ds(pl.multiple_of((2 * z + core) * LANES, LANES), LANES)]
            for z in blocks[first : first + count]
        ],
        axis=1,
    )


def half_products(rows_ref, gain_ref, gate_ref, up_ref, core, first=0):
    count = rows_ref.shape[0]
    gain = core_columns(gain_ref, core, first, count)
    squares = jnp.zeros(rows_ref.shape[1:], F32)
    parts = []
    for z in range(rows_ref.shape[0]):
        rows = rows_ref[z].astype(F32)
        squares = squares + rows * rows
        parts.append((rows * gain[:, z * LANES : (z + 1) * LANES]).astype(BF16))
    x = jnp.concatenate(parts, axis=1)
    gate = lax.dot_general(
        x, core_columns(gate_ref, core, first, count), ACROSS, preferred_element_type=F32
    )
    upward = lax.dot_general(
        x, core_columns(up_ref, core, first, count), ACROSS, preferred_element_type=F32
    )
    return squares, gate, upward


def own_half_kernel(
    rows_ref, gain_ref, gate_ref, up_ref, down_ref, squares_ref, gate_out, up_out
):
    core = lax.axis_index("tp_1")
    squares_ref[...], gate_out[...], up_out[...] = half_products(
        rows_ref, gain_ref, gate_ref, up_ref, core
    )


def other_first_kernel(
    rows_ref,
    gain_ref,
    gate_ref,
    up_ref,
    squares_part_ref,
    gate_part_ref,
    up_part_ref,
    squares_ref,
    gate_out,
    up_out,
):
    other = 1 - lax.axis_index("tp_1")
    squares, gate, upward = half_products(rows_ref, gain_ref, gate_ref, up_ref, other)
    squares_ref[...] = squares + squares_part_ref[...]
    gate_out[...] = gate + gate_part_ref[...]
    up_out[...] = upward + up_part_ref[...]


def other_half_kernel(
    rows_ref,
    gain_ref,
    gate_ref,
    up_ref,
    down_ref,
    squares_ref,
    gate_part_ref,
    up_part_ref,
    hidden_ref,
    send_ref,
):
    other = 1 - lax.axis_index("tp_1")
    squares, gate, upward = half_products(
        rows_ref, gain_ref, gate_ref, up_ref, other, send_ref.shape[0] - rows_ref.shape[0]
    )
    square_sum = jnp.sum(squares + squares_ref[...], axis=1, keepdims=True)
    scale = lax.rsqrt(square_sum / gate_ref.shape[1] + RMS_EPS)
    gate = (gate + gate_part_ref[...]) * scale
    upward = (upward + up_part_ref[...]) * scale
    hidden = (jax.nn.silu(gate) * upward).astype(BF16)
    hidden_ref[...] = hidden
    out = jnp.dot(hidden, core_columns(down_ref, other), preferred_element_type=F32)
    for z in range(send_ref.shape[0]):
        send_ref[z] = out[:, z * LANES : (z + 1) * LANES].astype(BF16)


def keep_kernel(hidden_ref, down_ref, keep_ref):
    core = lax.axis_index("tp_1")
    out = jnp.dot(hidden_ref[...], core_columns(down_ref, core), preferred_element_type=F32)
    for z in range(keep_ref.shape[0]):
        keep_ref[z] = out[:, z * LANES : (z + 1) * LANES]


def run_expert(own, gain, gate, up, down):
    rows = own.shape[1]
    vmem = pl.BlockSpec(memory_space=VMEM)
    part = jax.ShapeDtypeStruct((rows, gate.shape[0]), F32)

    def call(body, name, *operands, out_shape):
        return pl.pallas_call(
            body,
            out_shape=out_shape,
            in_specs=[vmem] * len(operands),
            out_specs=jax.tree.map(lambda _: vmem, out_shape),
            compiler_params=pltpu.CompilerParams(vmem_limit_bytes=10 << 20),
            name=name,
        )(*operands)

    middle = own.shape[0] // 2
    other_first, other_last = swap(own[:middle]), swap(own[middle:])
    sums = (jax.ShapeDtypeStruct((rows, LANES), F32), part, part)
    partial = call(own_half_kernel, "own_half", own, gain, gate, up, down, out_shape=sums)
    other_first, partial = lax.optimization_barrier((other_first, partial))
    partial = call(
        other_first_kernel, "other_first", other_first, gain, gate, up, *partial, out_shape=sums
    )
    other, partial = lax.optimization_barrier((other_last, partial))
    hidden, send = call(
        other_half_kernel,
        "other_half",
        other,
        gain,
        gate,
        up,
        down,
        *partial,
        out_shape=(
            jax.ShapeDtypeStruct((rows, gate.shape[0]), BF16),
            jax.ShapeDtypeStruct(own.shape, BF16),
        ),
    )
    received = swap(send)
    keep = call(
        keep_kernel, "keep_half", hidden, down, out_shape=jax.ShapeDtypeStruct(own.shape, F32)
    )
    return (keep + received.astype(F32)).astype(BF16)


def combine_kernel(share_ref, rows_ref, resid_ref, out_ref):
    rows = rows_ref[0].astype(F32)
    for z in range(1, rows_ref.shape[0]):
        rows = rows + rows_ref[z].astype(F32)
    moe = lax.dot_general(
        share_ref[...],
        rows,
        (((0,), (0,)), ((), ())),
        precision=HIGHEST,
        preferred_element_type=F32,
    )
    out_ref[...] = (resid_ref[...].astype(F32) + moe).astype(BF16)


def combine_rows(share, rows, resid):
    return pl.pallas_call(
        combine_kernel,
        out_shape=jax.ShapeDtypeStruct(resid.shape, BF16),
        compiler_params=pltpu.CompilerParams(vmem_limit_bytes=4 << 20),
        name="combine",
    )(share, rows, resid)


def swap(shard):
    return lax.ppermute(shard, "tp_1", [(0, 1), (1, 0)])


def exchange(shard, axis, order):
    return lax.all_to_all(
        shard, axis, split_axis=0, concat_axis=0, axis_index_groups=[order], tiled=True
    )


def exchange_rows(shard):
    ep_count, z_count = lax.axis_size("ep"), lax.axis_size("tp_0")
    order = [z * ep_count + e for z in z_order(z_count) for e in ep_order(ep_count)]
    chunks = shard.reshape(len(order), -1, 4, LANES)
    return exchange(chunks, ("tp_0", "ep"), order).reshape(shard.shape)


def local(
    tokens,
    state,
    routes,
    route_logits,
    mix_gain,
    w_recept,
    w_key,
    w_value,
    w_decay,
    w_rate,
    decay_base,
    rate_base,
    key_gain,
    group_gain,
    w_output,
    ffn_gain,
    w_gate,
    w_up,
    w_down,
):
    seq_rows = tokens.shape[0]
    z_count = lax.axis_size("tp_0")
    group_count = lax.axis_size("ep")
    slot_rows = max(2, 3 * routes.shape[1] * seq_rows // (2 * group_count))
    slot_count = group_count * slot_rows

    state_rows = state.reshape(-1, HEAD)
    vectors, recept, unit_rate, decay, key, value, own_tokens, pick, share = project_heads(
        tokens,
        (w_recept, w_key, w_value, w_decay, w_rate),
        mix_gain.reshape(1, -1),
        [v.reshape(1, -1) for v in (decay_base, rate_base, key_gain)],
        routes.T,
        route_logits.T,
        slot_count,
    )
    send, removed, mixed, w_output_near = mix(
        state_rows,
        vectors,
        recept,
        unit_rate,
        key,
        value,
        w_output,
        group_gain.reshape(1, -1),
        z_count,
    )
    keep = keep_out(mixed, w_output_near, z_count)
    pair_sum = (keep + swap(send).astype(F32)).astype(BF16)
    parts = exchange(pair_sum, "tp_0", z_order(z_count))
    new_state = update_state(state_rows, removed, unit_rate, decay, key, value)

    resid_own, outgoing = dispatch_rows(parts, own_tokens, pick)
    arrived = exchange_rows(outgoing)
    gain = ffn_gain.reshape(1, -1)
    pair_sum = run_expert(
        arrived,
        gain,
        jnp.swapaxes(w_gate[0], 0, 1),
        jnp.swapaxes(w_up[0], 0, 1),
        w_down[0],
    )
    output = combine_rows(share, exchange_rows(pair_sum), resid_own)
    return (output, new_state.reshape(state.shape))


def solution(mesh):
    torus = Mesh(mesh.devices.reshape(mesh.shape["ep"], 8, 2), ("ep", "tp_0", "tp_1"))
    return jax.shard_map(
        local,
        mesh=torus,
        in_specs=(
            P("ep", None),
            P("ep", TP, None, None),
            P("ep", None),
            P("ep", None),
            P(),
            P(None, TP),
            P(None, TP),
            P(None, TP),
            P(None, TP),
            P(None, TP),
            P(TP),
            P(TP),
            P(TP),
            P(TP),
            P(TP, None),
            P(),
            P("ep", None, TP),
            P("ep", None, TP),
            P("ep", TP, None),
        ),
        out_specs=(P("ep", TP), P("ep", TP, None, None)),
        check_vma=False,
    )
```

```python
import jax
import jax.numpy as jnp
from jax import lax
from jax.experimental import pallas as pl
from jax.experimental.pallas import tpu as pltpu
from jax.sharding import Mesh
from jax.sharding import PartitionSpec as P

TP = ("tp_0", "tp_1")

RMS_EPS = 1e-06
GROUP_EPS = 0.00064
UNIT_EPS = 6.4e-05
HIGHEST = lax.Precision.HIGHEST
F32 = jnp.float32
BF16 = jnp.bfloat16
VMEM = pltpu.VMEM
HEAD = 64
LANES = 128
FIRST_Z = 5
FIRST_EP = 10


def z_order(count):
    return [(FIRST_Z + 3 * step) % count for step in range(count)]


def ep_order(count):
    return [(FIRST_EP + step) % count for step in range(count)]


def in_hbm(array):
    return pltpu.with_memory_space_constraint(array, pltpu.HBM)


def head_sums(values):
    rows = lax.broadcasted_iota(jnp.int32, (LANES, LANES), 0) // HEAD
    cols = lax.broadcasted_iota(jnp.int32, (LANES, LANES), 1) // HEAD
    ones = (rows == cols).astype(F32)
    return jnp.dot(values, ones, precision=HIGHEST, preferred_element_type=F32)


def route_slots(routes, logits, pick_ref, share_ref):
    slots, seqs = pick_ref.shape
    experts = lax.axis_size("ep")
    first, second = routes[0:1, :], routes[1:2, :]
    expert = lax.broadcasted_iota(jnp.int32, (experts, seqs), 0)
    named = [(expert == choice).astype(F32) for choice in (first, second)]
    earlier = lax.broadcasted_iota(jnp.int32, (seqs, seqs), 0) < lax.broadcasted_iota(
        jnp.int32, (seqs, seqs), 1
    )
    counts = jnp.dot(
        (named[0] + named[1]).astype(BF16),
        earlier.astype(F32).astype(BF16),
        preferred_element_type=F32,
    )
    exps = jnp.exp(logits)
    total = exps[0:1, :] + exps[1:2, :]
    slot = lax.broadcasted_iota(jnp.int32, (slots, seqs), 0)
    picked = jnp.zeros((slots, seqs), F32)
    shares = jnp.zeros((slots, seqs), F32)
    for k, choice in enumerate((first, second)):
        placed = jnp.sum(named[k] * counts, axis=0, keepdims=True).astype(jnp.int32)
        chunk = lax.rem(choice + (experts - FIRST_EP), experts)
        here = slot == chunk * (slots // experts) + placed
        picked = jnp.where(here, 1.0, picked)
        shares = jnp.where(here, exps[k : k + 1, :] / total, shares)
    pick_ref[...] = picked.astype(BF16)
    share_ref[...] = shares


def project_kernel(
    tokens_hbm,
    w_recept_hbm,
    w_key_hbm,
    w_value_hbm,
    w_decay_hbm,
    w_rate_hbm,
    mix_gain_hbm,
    decay_base_hbm,
    rate_base_hbm,
    key_gain_hbm,
    routes_hbm,
    logits_hbm,
    vectors_ref,
    recept_ref,
    unit_rate_ref,
    decay_ref,
    key_ref,
    value_ref,
    own_ref,
    pick_ref,
    share_ref,
    tokens_ref,
    weights_ref,
    mix_gain_ref,
    decay_base_ref,
    rate_base_ref,
    key_gain_ref,
    routes_ref,
    logits_ref,
    sems,
    small_sems,
):
    seqs = tokens_ref.shape[0]
    copies = [pltpu.make_async_copy(tokens_hbm, tokens_ref, sems.at[0])]
    smalls = [
        pltpu.make_async_copy(source, target, small_sems.at[place])
        for place, (source, target) in enumerate(
            (
                (mix_gain_hbm, mix_gain_ref),
                (key_gain_hbm, key_gain_ref),
                (decay_base_hbm, decay_base_ref),
                (rate_base_hbm, rate_base_ref),
                (routes_hbm, routes_ref),
                (logits_hbm, logits_ref),
            )
        )
    ]
    sources = (w_key_hbm, w_value_hbm, w_recept_hbm, w_decay_hbm, w_rate_hbm)
    for place, source in enumerate(sources):
        target = weights_ref.at[:, pl.ds(place * LANES, LANES)]
        copies.append(pltpu.make_async_copy(source, target, sems.at[1 + place]))
    copies[0].start()
    for copy in smalls:
        copy.start()
    for copy in copies[1:]:
        copy.start()

    for copy in smalls:
        copy.wait()
    route_slots(routes_ref[...], logits_ref[...], pick_ref, share_ref)
    copies[0].wait()
    own_ref[...] = tokens_ref[:, pl.ds(pl.multiple_of(lax.axis_index(TP) * LANES, LANES), LANES)]
    values = tokens_ref[...].astype(F32)
    mean_square = jnp.mean(values * values, axis=1, keepdims=True)
    normed = (values * lax.rsqrt(mean_square + RMS_EPS) * mix_gain_ref[...]).astype(BF16)

    def project(first, count):
        for place in range(first, first + count):
            copies[1 + place].wait()
        weight = weights_ref[:, first * LANES : (first + count) * LANES]
        return jnp.dot(normed, weight, preferred_element_type=F32).astype(BF16).astype(F32)

    key_value = project(0, 2)
    keys_now = key_value[:, :LANES]
    key_ref[...] = keys_now
    value_ref[...] = key_value[:, LANES:]
    scaled = keys_now * key_gain_ref[...]
    unit_key = scaled * lax.rsqrt(head_sums(scaled * scaled) + UNIT_EPS)
    vectors_ref[...] = jnp.zeros_like(vectors_ref)
    vectors_ref[pl.ds(0, seqs, stride=8), :] = unit_key
    vectors_ref[pl.ds(2, seqs, stride=8), :] = pltpu.roll(unit_key, HEAD, 1)
    recept_decay = project(2, 2)
    recept = recept_decay[:, :LANES]
    recept_ref[...] = recept
    decay_pre = recept_decay[:, LANES:] + decay_base_ref[...]
    decay_now = jnp.exp(-jnp.exp(-jax.nn.softplus(-decay_pre) - 0.5))
    decay_ref[...] = decay_now
    decayed_recept = decay_now * recept
    vectors_ref[pl.ds(1, seqs, stride=8), :] = decayed_recept
    vectors_ref[pl.ds(3, seqs, stride=8), :] = pltpu.roll(decayed_recept, HEAD, 1)
    rate_pre = project(4, 1) + rate_base_ref[...]
    unit_rate_ref[...] = unit_key * jax.nn.sigmoid(rate_pre)


def project_heads(tokens, projections, mix_gain, vectors, routes, logits, slots):
    seqs, full_width = tokens.shape
    small = jax.ShapeDtypeStruct((seqs, LANES), F32)
    hbm = pl.BlockSpec(memory_space=pl.ANY)
    vmem = pl.BlockSpec(memory_space=VMEM)
    return pl.pallas_call(
        project_kernel,
        out_shape=(jax.ShapeDtypeStruct((seqs * 8, LANES), F32),)
        + (small,) * 5
        + (
            jax.ShapeDtypeStruct((seqs, LANES), BF16),
            jax.ShapeDtypeStruct((slots, seqs), BF16),
            jax.ShapeDtypeStruct((slots, seqs), F32),
        ),
        in_specs=[hbm] * 12,
        out_specs=(vmem,) * 9,
        scratch_shapes=[
            VMEM((seqs, full_width), BF16),
            VMEM((full_width, 5 * LANES), BF16),
            VMEM((1, full_width), F32),
            VMEM((1, LANES), F32),
            VMEM((1, LANES), F32),
            VMEM((1, LANES), F32),
            VMEM(routes.shape, jnp.int32),
            VMEM(logits.shape, F32),
            pltpu.SemaphoreType.DMA((6,)),
            pltpu.SemaphoreType.DMA((6,)),
        ],
        compiler_params=pltpu.CompilerParams(vmem_limit_bytes=12 << 20),
        cost_estimate=pl.CostEstimate(
            flops=3_000_000_000, bytes_accessed=6 << 20, transcendentals=0
        ),
        name="project_heads",
    )(*map(in_hbm, (tokens, *projections, mix_gain, *vectors, routes, logits)))


def mix_kernel(
    state_ref,
    vectors_ref,
    recept_ref,
    unit_rate_ref,
    key_ref,
    value_ref,
    w_output_hbm,
    group_gain_ref,
    send_ref,
    removed_ref,
    mixed_ref,
    w_output_ref,
    products_ref,
    sem,
):
    w_output_copy = pltpu.make_async_copy(w_output_hbm, w_output_ref, sem)
    w_output_copy.start()
    seqs = recept_ref.shape[0]
    group = 2
    for seq in range(0, seqs, group):
        left = vectors_ref[seq * 8 : (seq + group) * 8, :HEAD].astype(BF16)
        right = state_ref[seq * LANES : (seq + group) * LANES, :].astype(BF16)
        out = lax.dot_general(left, right, ACROSS, preferred_element_type=F32)
        for one in range(group):
            products_ref[(seq + one) * 8 : (seq + one + 1) * 8, :] = out[
                one * 8 : (one + 1) * 8, one * LANES : (one + 1) * LANES
            ]
    first_head = lax.broadcasted_iota(jnp.int32, (seqs, LANES), 1) < HEAD
    removed = jnp.where(
        first_head,
        products_ref[pl.ds(0, seqs, stride=8), :],
        products_ref[pl.ds(2, seqs, stride=8), :],
    )
    faded = jnp.where(
        first_head,
        products_ref[pl.ds(1, seqs, stride=8), :],
        products_ref[pl.ds(3, seqs, stride=8), :],
    )
    removed_ref[...] = removed
    recept = recept_ref[...]
    readout = (
        faded
        - removed * head_sums(unit_rate_ref[...] * recept)
        + value_ref[...] * head_sums(key_ref[...] * recept)
    )
    centred = readout - head_sums(readout) * (1.0 / HEAD)
    spread = head_sums(centred * centred) * (1.0 / HEAD)
    mixed = (centred * lax.rsqrt(spread + GROUP_EPS) * group_gain_ref[...]).astype(BF16)
    mixed_ref[...] = mixed
    w_output_copy.wait()
    out_columns(mixed, w_output_ref, send_ref, 1 - lax.axis_index("tp_1"))


def out_columns(mixed, w_output_ref, out_ref, core):
    for place, z in enumerate(z_order(out_ref.shape[0])):
        cols = pl.ds(pl.multiple_of((2 * z + core) * LANES, LANES), LANES)
        out_ref[place] = jnp.dot(
            mixed, w_output_ref[:, cols], preferred_element_type=F32
        ).astype(out_ref.dtype)


def mix(state_rows, vectors, recept, unit_rate, key, value, w_output, group_gain, z_count):
    seqs = recept.shape[0]
    vmem = pl.BlockSpec(memory_space=VMEM)
    return pl.pallas_call(
        mix_kernel,
        out_shape=(
            jax.ShapeDtypeStruct((z_count, seqs, LANES), BF16),
            jax.ShapeDtypeStruct((seqs, LANES), F32),
            jax.ShapeDtypeStruct((seqs, LANES), BF16),
            jax.ShapeDtypeStruct(w_output.shape, BF16),
        ),
        in_specs=[vmem] * 6 + [pl.BlockSpec(memory_space=pl.ANY), vmem],
        out_specs=(vmem,) * 4,
        scratch_shapes=[VMEM((seqs * 8, LANES), F32), pltpu.SemaphoreType.DMA(())],
        compiler_params=pltpu.CompilerParams(vmem_limit_bytes=12 << 20),
        name="mix",
    )(state_rows, vectors, recept, unit_rate, key, value, in_hbm(w_output), group_gain)


def keep_out_kernel(mixed_ref, w_output_ref, keep_ref):
    out_columns(mixed_ref[...], w_output_ref, keep_ref, lax.axis_index("tp_1"))


def keep_out(mixed, w_output, z_count):
    return pl.pallas_call(
        keep_out_kernel,
        out_shape=jax.ShapeDtypeStruct((z_count, *mixed.shape), F32),
        compiler_params=pltpu.CompilerParams(vmem_limit_bytes=2 << 20),
        name="keep_out",
    )(mixed, w_output)


def update_kernel(
    state_ref,
    removed_ref,
    unit_rate_ref,
    decay_ref,
    key_ref,
    value_ref,
    out_ref,
    left_ref,
    right_ref,
):
    block = removed_ref.shape[0]
    first_head = lax.broadcasted_iota(jnp.int32, (block, LANES), 1) < HEAD
    removed = -removed_ref[...]
    removed_high = removed.astype(BF16).astype(F32)
    removed_low = removed - removed_high
    unit_rate = unit_rate_ref[...]
    unit_high = unit_rate.astype(BF16).astype(F32)
    unit_low = unit_rate - unit_high
    key = key_ref[...]
    lefts = (removed_high, removed_low, removed_high, value_ref[...])
    rights = (unit_high, unit_high, unit_low, key)
    for place in range(4):
        left_ref[pl.ds(place, block, stride=8), :] = jnp.where(first_head, lefts[place], 0.0)
        left_ref[pl.ds(place + 4, block, stride=8), :] = jnp.where(first_head, 0.0, lefts[place])
        right_ref[pl.ds(place, block, stride=8), :] = rights[place]
        right_ref[pl.ds(place + 4, block, stride=8), :] = pltpu.roll(rights[place], HEAD, 1)
    decay = decay_ref[...]
    decay_rolled = pltpu.roll(decay, HEAD, 1)
    for seq in range(block):
        left = left_ref[seq * 8 : seq * 8 + 8, :].astype(BF16)
        right = right_ref[seq * 8 : seq * 8 + 8, :HEAD].astype(BF16)
        change = lax.dot_general(
            left, right, (((0,), (0,)), ((), ())), preferred_element_type=F32
        )
        base = seq * LANES
        old = state_ref[base : base + HEAD, :]
        out_ref[base : base + HEAD, :] = old * decay[seq : seq + 1, :HEAD] + change[:HEAD]
        old = state_ref[base + HEAD : base + LANES, :]
        out_ref[base + HEAD : base + LANES, :] = (
            old * decay_rolled[seq : seq + 1, :HEAD] + change[HEAD:]
        )


def update_state(state_rows, removed, unit_rate, decay, key, value):
    seqs = removed.shape[0]
    steps = 8
    block = seqs // steps
    rows = pl.BlockSpec((block * LANES, HEAD), lambda i: (i, 0))
    small = pl.BlockSpec((block, LANES), lambda i: (i, 0))
    return pl.pallas_call(
        update_kernel,
        grid=(steps,),
        out_shape=jax.ShapeDtypeStruct(state_rows.shape, F32),
        in_specs=[rows] + [small] * 5,
        out_specs=rows,
        scratch_shapes=[VMEM((block * 8, LANES), F32), VMEM((block * 8, LANES), F32)],
        compiler_params=pltpu.CompilerParams(vmem_limit_bytes=8 << 20),
        cost_estimate=pl.CostEstimate(
            flops=2_000_000_000, bytes_accessed=8 << 20, transcendentals=0
        ),
        name="update_state",
    )(in_hbm(state_rows), removed, unit_rate, decay, key, value)


def dispatch_kernel(parts_ref, tokens_ref, pick_ref, resid_ref, out_ref):
    total = tokens_ref[...].astype(F32)
    mix = parts_ref[0].astype(F32)
    for z in range(1, parts_ref.shape[0]):
        mix = mix + parts_ref[z].astype(F32)
    resid = (total + mix).astype(BF16)
    resid_ref[...] = resid
    picked = jnp.dot(pick_ref[...], resid, preferred_element_type=F32).astype(BF16)
    for z in range(out_ref.shape[0]):
        out_ref[z] = picked


def dispatch_rows(parts, tokens, pick):
    return pl.pallas_call(
        dispatch_kernel,
        out_shape=(
            jax.ShapeDtypeStruct(tokens.shape, BF16),
            jax.ShapeDtypeStruct((parts.shape[0], pick.shape[0], LANES), BF16),
        ),
        compiler_params=pltpu.CompilerParams(vmem_limit_bytes=4 << 20),
        name="dispatch_rows",
    )(parts, tokens, pick)


ACROSS = (((1,), (1,)), ((), ()))


def core_columns(ref, core, first=0, count=None):
    blocks = z_order(ref.shape[1] // (2 * LANES))
    count = len(blocks) if count is None else count
    return jnp.concatenate(
        [
            ref[:, pl.ds(pl.multiple_of((2 * z + core) * LANES, LANES), LANES)]
            for z in blocks[first : first + count]
        ],
        axis=1,
    )


def half_products(rows_ref, gain_ref, gate_ref, up_ref, core, first=0):
    count = rows_ref.shape[0]
    gain = core_columns(gain_ref, core, first, count)
    squares = jnp.zeros(rows_ref.shape[1:], F32)
    parts = []
    for z in range(rows_ref.shape[0]):
        rows = rows_ref[z].astype(F32)
        squares = squares + rows * rows
        parts.append((rows * gain[:, z * LANES : (z + 1) * LANES]).astype(BF16))
    x = jnp.concatenate(parts, axis=1)
    gate = lax.dot_general(
        x, core_columns(gate_ref, core, first, count), ACROSS, preferred_element_type=F32
    )
    upward = lax.dot_general(
        x, core_columns(up_ref, core, first, count), ACROSS, preferred_element_type=F32
    )
    return squares, gate, upward


def own_half_kernel(
    rows_ref, gain_ref, gate_ref, up_ref, down_ref, squares_ref, gate_out, up_out
):
    core = lax.axis_index("tp_1")
    squares_ref[...], gate_out[...], up_out[...] = half_products(
        rows_ref, gain_ref, gate_ref, up_ref, core
    )


def other_first_kernel(
    rows_ref,
    gain_ref,
    gate_ref,
    up_ref,
    squares_part_ref,
    gate_part_ref,
    up_part_ref,
    squares_ref,
    gate_out,
    up_out,
):
    other = 1 - lax.axis_index("tp_1")
    squares, gate, upward = half_products(rows_ref, gain_ref, gate_ref, up_ref, other)
    squares_ref[...] = squares + squares_part_ref[...]
    gate_out[...] = gate + gate_part_ref[...]
    up_out[...] = upward + up_part_ref[...]


def other_half_kernel(
    rows_ref,
    gain_ref,
    gate_ref,
    up_ref,
    down_ref,
    squares_ref,
    gate_part_ref,
    up_part_ref,
    hidden_ref,
    send_ref,
):
    other = 1 - lax.axis_index("tp_1")
    squares, gate, upward = half_products(
        rows_ref, gain_ref, gate_ref, up_ref, other, send_ref.shape[0] - rows_ref.shape[0]
    )
    square_sum = jnp.sum(squares + squares_ref[...], axis=1, keepdims=True)
    scale = lax.rsqrt(square_sum / gate_ref.shape[1] + RMS_EPS)
    gate = (gate + gate_part_ref[...]) * scale
    upward = (upward + up_part_ref[...]) * scale
    hidden = (jax.nn.silu(gate) * upward).astype(BF16)
    hidden_ref[...] = hidden
    out = jnp.dot(hidden, core_columns(down_ref, other), preferred_element_type=F32)
    for z in range(send_ref.shape[0]):
        send_ref[z] = out[:, z * LANES : (z + 1) * LANES].astype(BF16)


def keep_kernel(hidden_ref, down_ref, keep_ref):
    core = lax.axis_index("tp_1")
    out = jnp.dot(hidden_ref[...], core_columns(down_ref, core), preferred_element_type=F32)
    for z in range(keep_ref.shape[0]):
        keep_ref[z] = out[:, z * LANES : (z + 1) * LANES]


def run_expert(own, gain, gate, up, down):
    rows = own.shape[1]
    vmem = pl.BlockSpec(memory_space=VMEM)
    part = jax.ShapeDtypeStruct((rows, gate.shape[0]), F32)

    def call(body, name, *operands, out_shape):
        return pl.pallas_call(
            body,
            out_shape=out_shape,
            in_specs=[vmem] * len(operands),
            out_specs=jax.tree.map(lambda _: vmem, out_shape),
            compiler_params=pltpu.CompilerParams(vmem_limit_bytes=10 << 20),
            name=name,
        )(*operands)

    middle = own.shape[0] // 2
    other_first, other_last = swap(own[:middle]), swap(own[middle:])
    sums = (jax.ShapeDtypeStruct((rows, LANES), F32), part, part)
    partial = call(own_half_kernel, "own_half", own, gain, gate, up, down, out_shape=sums)
    other_first, partial = lax.optimization_barrier((other_first, partial))
    partial = call(
        other_first_kernel, "other_first", other_first, gain, gate, up, *partial, out_shape=sums
    )
    other, partial = lax.optimization_barrier((other_last, partial))
    hidden, send = call(
        other_half_kernel,
        "other_half",
        other,
        gain,
        gate,
        up,
        down,
        *partial,
        out_shape=(
            jax.ShapeDtypeStruct((rows, gate.shape[0]), BF16),
            jax.ShapeDtypeStruct(own.shape, BF16),
        ),
    )
    received = swap(send)
    keep = call(
        keep_kernel, "keep_half", hidden, down, out_shape=jax.ShapeDtypeStruct(own.shape, F32)
    )
    return (keep + received.astype(F32)).astype(BF16)


def combine_kernel(share_ref, rows_ref, resid_ref, out_ref):
    rows = rows_ref[0].astype(F32)
    for z in range(1, rows_ref.shape[0]):
        rows = rows + rows_ref[z].astype(F32)
    moe = lax.dot_general(
        share_ref[...],
        rows,
        (((0,), (0,)), ((), ())),
        precision=HIGHEST,
        preferred_element_type=F32,
    )
    out_ref[...] = (resid_ref[...].astype(F32) + moe).astype(BF16)


def combine_rows(share, rows, resid):
    return pl.pallas_call(
        combine_kernel,
        out_shape=jax.ShapeDtypeStruct(resid.shape, BF16),
        compiler_params=pltpu.CompilerParams(vmem_limit_bytes=4 << 20),
        name="combine",
    )(share, rows, resid)


def swap(shard):
    return lax.ppermute(shard, "tp_1", [(0, 1), (1, 0)])


def exchange(shard, axis, order):
    return lax.all_to_all(
        shard, axis, split_axis=0, concat_axis=0, axis_index_groups=[order], tiled=True
    )


def exchange_rows(shard):
    ep_count, z_count = lax.axis_size("ep"), lax.axis_size("tp_0")
    order = [z * ep_count + e for z in z_order(z_count) for e in ep_order(ep_count)]
    chunks = shard.reshape(len(order), -1, 4, LANES)
    return exchange(chunks, ("tp_0", "ep"), order).reshape(shard.shape)


def local(
    tokens,
    state,
    routes,
    route_logits,
    mix_gain,
    w_recept,
    w_key,
    w_value,
    w_decay,
    w_rate,
    decay_base,
    rate_base,
    key_gain,
    group_gain,
    w_output,
    ffn_gain,
    w_gate,
    w_up,
    w_down,
):
    seq_rows = tokens.shape[0]
    z_count = lax.axis_size("tp_0")
    group_count = lax.axis_size("ep")
    slot_rows = max(2, 3 * routes.shape[1] * seq_rows // (2 * group_count))
    slot_count = group_count * slot_rows

    state_rows = state.reshape(-1, HEAD)
    vectors, recept, unit_rate, decay, key, value, own_tokens, pick, share = project_heads(
        tokens,
        (w_recept, w_key, w_value, w_decay, w_rate),
        mix_gain.reshape(1, -1),
        [v.reshape(1, -1) for v in (decay_base, rate_base, key_gain)],
        routes.T,
        route_logits.T,
        slot_count,
    )
    send, removed, mixed, w_output_near = mix(
        state_rows,
        vectors,
        recept,
        unit_rate,
        key,
        value,
        w_output,
        group_gain.reshape(1, -1),
        z_count,
    )
    keep = keep_out(mixed, w_output_near, z_count)
    pair_sum = (keep + swap(send).astype(F32)).astype(BF16)
    parts = exchange(pair_sum, "tp_0", z_order(z_count))
    new_state = update_state(state_rows, removed, unit_rate, decay, key, value)

    resid_own, outgoing = dispatch_rows(parts, own_tokens, pick)
    arrived = exchange_rows(outgoing)
    gain = ffn_gain.reshape(1, -1)
    pair_sum = run_expert(
        arrived,
        gain,
        jnp.swapaxes(w_gate[0], 0, 1),
        jnp.swapaxes(w_up[0], 0, 1),
        w_down[0],
    )
    output = combine_rows(share, exchange_rows(pair_sum), resid_own)
    return (output, new_state.reshape(state.shape))


def solution(mesh):
    torus = Mesh(mesh.devices.reshape(mesh.shape["ep"], 8, 2), ("ep", "tp_0", "tp_1"))
    return jax.shard_map(
        local,
        mesh=torus,
        in_specs=(
            P("ep", None),
            P("ep", TP, None, None),
            P("ep", None),
            P("ep", None),
            P(),
            P(None, TP),
            P(None, TP),
            P(None, TP),
            P(None, TP),
            P(None, TP),
            P(TP),
            P(TP),
            P(TP),
            P(TP),
            P(TP, None),
            P(),
            P("ep", None, TP),
            P("ep", None, TP),
            P("ep", TP, None),
        ),
        out_specs=(P("ep", TP), P("ep", TP, None, None)),
        check_vma=False,
    )
```
